128 devices in a mesh: fs: 16 (over z, y), tp: 4 (over x), rep: 2 (over core).
Axes of the slice: x: 4, y: 4, z: 4, core: 2. Of those that a mesh axis runs over, the one named last changes fastest.
Arguments:
- gate_grads: float32 [2, 5632, 2048], P('rep', 'fs', 'tp'), may hold values from -16 to 16, as said below
- gate_velocity: float32 [5632, 2048], P(('fs', 'rep'), 'tp'), may hold values from -31 to 31, as said below
- gate_weight: float32 [5632, 2048], P(('fs', 'rep'), 'tp'), may hold values from -4 to 4
- up_grads: float32 [2, 5632, 2048], P('rep', 'fs', 'tp'), may hold values from -16 to 16, as said below
- up_velocity: float32 [5632, 2048], P(('fs', 'rep'), 'tp'), may hold values from -31 to 31, as said below
- up_weight: float32 [5632, 2048], P(('fs', 'rep'), 'tp'), may hold values from -4 to 4
- branch_grads: float32 [2, 2048, 1024], P('rep', 'fs', 'tp'), may hold values from -16 to 16, as said below
- branch_velocity: float32 [2048, 1024], P(('fs', 'rep'), 'tp'), may hold values from -31 to 31, as said below
- branch_weight: float32 [2048, 1024], P(('fs', 'rep'), 'tp'), may hold values from -4 to 4
Outputs:
- gate_momentum: float32 [5632, 2048], P(('fs', 'rep'), 'tp')
- gate_updated: float32 [5632, 2048], P(('fs', 'rep'), 'tp')
- up_momentum: float32 [5632, 2048], P(('fs', 'rep'), 'tp')
- up_updated: float32 [5632, 2048], P(('fs', 'rep'), 'tp')
- branch_momentum: float32 [2048, 1024], P(('fs', 'rep'), 'tp')
- branch_updated: float32 [2048, 1024], P(('fs', 'rep'), 'tp')
The draws below stay inside these ranges and needn't reach their ends.
Inputs may be any that keep to these rules, and one draw needn't show every extreme that they name: `gate_grads`: entries vary in scale over rows and over columns. `up_grads`: entries vary in scale over rows and over columns. `branch_grads`: entries vary in scale over rows and over columns. `gate_velocity`: entries vary in scale over rows and over columns. `up_velocity`: entries vary in scale over rows and over columns. `branch_velocity`: entries vary in scale over rows and over columns.
All inputs are finite; a program needn't handle non-finite values.
Results may differ from the reference program's by a relative error of at most 0.039.
Values may be sent and summed in bfloat16 or wider, within the bound.
A program may use at most 64 MiB of HBM per device.

```python
import math
import jax
import jax.numpy as jnp
from jax import lax

D = 2048
FF = 5632
BRANCH = 1024
ITERS = 3
REP = 2
N_FS = 16
N_REP = 2


def block_scaled(key, height, width):
    noise_key, row_key, col_key = jax.random.split(key, 3)
    noise = jnp.clip(jax.random.normal(noise_key, (height, width), jnp.float32), -4.0, 4.0)
    rise = math.log(4.0)
    row_factor = jnp.exp(jax.random.uniform(row_key, (8,), jnp.float32, -0.3, 0.3))
    col_factor = jnp.exp(jax.random.uniform(col_key, (4,), jnp.float32, -0.3, 0.3))
    row_ramp = jnp.exp(rise * (jnp.arange(height, dtype=jnp.float32) / (height - 1) - 1.0))
    col_ramp = jnp.exp(rise * (jnp.arange(width, dtype=jnp.float32) / (width - 1) - 1.0))
    row_scale = jnp.repeat(row_factor, height // 8) * row_ramp
    col_scale = jnp.repeat(col_factor, width // 4) * col_ramp
    return noise * row_scale[:, None] * col_scale[None, :]


def replicas(key, height, width):
    return jnp.stack([block_scaled(jax.random.fold_in(key, 11 + index), height, width) for index in range(REP)])


def draw_gate_grads(key, part):
    return replicas(key, FF, D)


def draw_up_grads(key, part):
    return replicas(jax.random.fold_in(key, 3), FF, D)


def draw_branch_grads(key, part):
    return replicas(jax.random.fold_in(key, 5), D, BRANCH)


def draw_gate_velocity(key, part):
    return 2.0 * block_scaled(jax.random.fold_in(key, 21), FF, D)


def draw_up_velocity(key, part):
    return 2.0 * block_scaled(jax.random.fold_in(key, 23), FF, D)


def draw_branch_velocity(key, part):
    return 2.0 * block_scaled(jax.random.fold_in(key, 25), D, BRANCH)


def steps_of(key, extent, cuts, smallest, high):
    def one(dim, parts):
        steps = jax.random.uniform(jax.random.fold_in(jax.random.fold_in(key, 6), dim), (parts,), jnp.float32, smallest / len(cuts), high / len(cuts))
        return jnp.repeat(jnp.exp(steps), extent[dim] // parts).reshape((-1,) + (1,) * (len(extent) - dim - 1))

    gain = one(*cuts[0])
    for cut in cuts[1:]:
        gain = gain * one(*cut)
    return gain


def normal_values(own_key, shape, scale, most, shards=(), kind=jnp.bfloat16):
    array = jax.random.normal(own_key, shape, jnp.float32) * scale
    if len(shards) > 0:
        array = steps_of(own_key, shape, shards, -0.22, 0.18) * array
    return jnp.clip(array, min=-most, max=most).astype(kind)


def setup_inputs(seed: int = 0) -> dict:
    keys = jax.random.split(jax.random.key(seed), 10)
    return {
        "gate_grads": draw_gate_grads(jax.random.fold_in(keys[9], 71), 0),
        "gate_velocity": draw_gate_velocity(jax.random.fold_in(keys[9], 71), 0),
        "gate_weight": normal_values(keys[2], (FF, D), 1.0, 4.0, ((0, 32), (1, 4)), jnp.float32),
        "up_grads": draw_up_grads(jax.random.fold_in(keys[9], 71), 0),
        "up_velocity": draw_up_velocity(jax.random.fold_in(keys[9], 71), 0),
        "up_weight": normal_values(keys[5], (FF, D), 1.0, 4.0, ((0, 32), (1, 4)), jnp.float32),
        "branch_grads": draw_branch_grads(jax.random.fold_in(keys[9], 71), 0),
        "branch_velocity": draw_branch_velocity(jax.random.fold_in(keys[9], 71), 0),
        "branch_weight": normal_values(keys[8], (D, BRANCH), 1.0, 4.0, ((0, 32), (1, 4)), jnp.float32),
    }


MOMENT = 0.95
COEF_ONE = 3.4445
COEF_THREE = -4.775
COEF_FIVE = 2.0315
SAFETY = 2.0
RATE = 0.5
SHRINK = 0.95

def block_gram(matrix):
    count = N_FS * N_REP
    height = matrix.shape[0] // count
    width = matrix.shape[1]
    stacked = matrix.reshape(count, height, width)

    def add_block(total, block):
        part = jnp.dot(block.T, block, preferred_element_type=jnp.float32)
        narrow = lax.optimization_barrier(part.astype(jnp.bfloat16))
        return (total + narrow.astype(jnp.float32), None)
    total, unused = lax.scan(add_block, jnp.zeros((width, width), jnp.float32), stacked)
    return total

def orthogonal(momentum):
    start = momentum.astype(jnp.bfloat16)
    first = jnp.sum(jnp.square(start.astype(jnp.float32)))
    raw = block_gram(start)
    second = jnp.sum(raw * raw)
    ratio = SAFETY * (second + 1.0) / (first + 1.0)
    scale = lax.rsqrt(ratio)
    gram = (raw / ratio).astype(jnp.bfloat16)
    ymat = (jnp.dot(start, gram, preferred_element_type=jnp.float32) * scale).astype(jnp.bfloat16)
    zmat = jnp.dot(ymat, gram, preferred_element_type=jnp.float32).astype(jnp.bfloat16)
    current = (COEF_ONE * scale * start.astype(jnp.float32) + COEF_THREE * ymat.astype(jnp.float32) + COEF_FIVE * zmat.astype(jnp.float32)).astype(jnp.bfloat16)
    for index in range(ITERS - 1):
        gram = block_gram(current).astype(jnp.bfloat16)
        ymat = jnp.dot(current, gram, preferred_element_type=jnp.float32).astype(jnp.bfloat16)
        zmat = jnp.dot(ymat, gram, preferred_element_type=jnp.float32).astype(jnp.bfloat16)
        current = (COEF_ONE * current.astype(jnp.float32) + COEF_THREE * ymat.astype(jnp.float32) + COEF_FIVE * zmat.astype(jnp.float32)).astype(jnp.bfloat16)
    return current

def one_matrix(grads, velocity, weight):
    momentum = MOMENT * velocity + lax.optimization_barrier(jnp.sum(grads, axis=0))
    final = orthogonal(momentum)
    updated = SHRINK * weight - RATE * math.sqrt(weight.shape[0]) * final.astype(jnp.float32)
    return (momentum, updated)

def reference(gate_grads, gate_velocity, gate_weight, up_grads, up_velocity, up_weight, branch_grads, branch_velocity, branch_weight):
    gate_momentum, gate_updated = one_matrix(gate_grads, gate_velocity, gate_weight)
    up_momentum, up_updated = one_matrix(up_grads, up_velocity, up_weight)
    branch_momentum, branch_updated = one_matrix(branch_grads, branch_velocity, branch_weight)
    return (gate_momentum, gate_updated, up_momentum, up_updated, branch_momentum, branch_updated)
```

```python
import math

import jax
import jax.numpy as jnp
from jax import lax
from jax.sharding import Mesh
from jax.sharding import PartitionSpec as P

D = 2048
FF = 5632
FS_REP = ("fs_0", "fs_1", "rep")
FS = ("fs_0", "fs_1")

MOMENT = 0.95
COEF_ONE = 3.4445
COEF_THREE = -4.775
COEF_FIVE = 2.0315
SAFETY = 2.0
RATE = 0.5
SHRINK = 0.95
BF = jnp.bfloat16


def dot(a, b):
    return jnp.dot(a, b, preferred_element_type=jnp.float32)


def sum_at_owner(value, axis, dim):
    devices = lax.axis_size(axis)
    before, after = (value.shape[:dim], value.shape[dim + 1 :])
    tiles = jnp.moveaxis(value.reshape(*before, devices, -1, *after), dim, 0)
    tiles = lax.all_to_all(tiles, axis, 0, 0, tiled=True)
    return jnp.sum(tiles.astype(jnp.float32), axis=0)


def chain(raw, start):
    raw = raw.astype(jnp.float32)
    ratio = SAFETY * (jnp.sum(raw * raw) + 1.0) / (jnp.trace(raw) + 1.0)
    scale = lax.rsqrt(ratio)
    g = (raw / ratio).astype(BF)
    x, factor = start, scale
    for index in range(3):
        s = dot(g, g)
        m = (COEF_THREE * g.astype(jnp.float32) + COEF_FIVE * s).astype(BF)
        if index == 2:
            return x, m
        t = (COEF_ONE * g.astype(jnp.float32) + dot(g, m)).astype(BF)
        x = (factor * (COEF_ONE * x.astype(jnp.float32) + dot(x, m))).astype(BF)
        g = (COEF_ONE * t.astype(jnp.float32) + dot(t, m)).astype(BF)
        factor = 1.0


def last(x, m, column, width):
    own = lax.dynamic_slice_in_dim(x, column * width, width, 1)
    cols = lax.dynamic_slice_in_dim(m, column * width, width, 1)
    return (COEF_ONE * own.astype(jnp.float32) + dot(x, cols)).astype(BF)


def local(
    gate_grads,
    gate_velocity,
    gate_weight,
    up_grads,
    up_velocity,
    up_weight,
    branch_grads,
    branch_velocity,
    branch_weight,
):
    both = jnp.concatenate((gate_grads.astype(BF), up_grads.astype(BF)), axis=0)
    total = sum_at_owner(both, "rep", 1)
    totals = (total[0], total[1], sum_at_owner(branch_grads.astype(BF), "rep", 1)[0])
    velocities = (gate_velocity, up_velocity, branch_velocity)
    moments = [MOMENT * velocity + part for velocity, part in zip(velocities, totals)]
    gate, up, branch = [moment.astype(BF) for moment in moments]
    rows = gate.shape[0]
    width = gate.shape[1]
    place = lax.axis_index("tp")
    odd = place % 2

    wide = lax.all_gather(jnp.concatenate((gate, up), axis=0), "tp", axis=1, tiled=True)
    gate_wide, up_wide = wide[:rows], wide[rows:]
    branch_wide = lax.all_gather(branch, "tp", axis=1, tiled=True)
    turn = (((0,), (0,)), ((), ()))
    parts = [
        lax.dot_general(whole, own, turn, preferred_element_type=jnp.float32).astype(BF)
        for whole, own in ((gate_wide, gate), (up_wide, up), (branch_wide, branch))
    ]
    share = sum_at_owner(jnp.concatenate(parts[:2], axis=1), FS_REP, 0).astype(BF)
    share_b = sum_at_owner(parts[2], FS_REP, 0).astype(BF)
    swapped = lax.all_gather(share, "tp", axis=0, tiled=False)
    mine = jnp.where(odd == 0, swapped[:, :, :width], swapped[:, :, width:])
    mine = jnp.moveaxis(mine, 0, 1).reshape(mine.shape[1], -1)
    raw = lax.all_gather(mine, FS_REP, axis=0, tiled=True)
    line_b = lax.all_gather(share_b, "tp", axis=1, tiled=True)
    raw_b = lax.all_gather(line_b, FS_REP, axis=0, tiled=True)
    start = jnp.where(odd == 0, gate_wide, up_wide)

    x, m = chain(raw, start)
    xb, mb = chain(raw_b, branch_wide)
    final_b = last(xb, mb, place, branch.shape[1])
    half = rows // 2
    own = last(x, m, place, width)
    ahead = last(x[:half], m, (place + 1) % 4, width)
    behind = last(x[half:], m, (place + 3) % 4, width)
    low = lax.ppermute(ahead, "tp", [(i, (i + 1) % 4) for i in range(4)])
    high = lax.ppermute(behind, "tp", [(i, (i + 3) % 4) for i in range(4)])
    other = jnp.concatenate((low, high), axis=0)
    finals = (jnp.where(odd == 0, own, other), jnp.where(odd == 0, other, own), final_b)
    weights = (gate_weight, up_weight, branch_weight)
    heights = (FF, FF, D)
    results = []
    for moment, weight, final, height in zip(moments, weights, finals, heights):
        results.append(moment)
        results.append(SHRINK * weight - RATE * math.sqrt(height) * final.astype(jnp.float32))
    return tuple(results)


def solution(mesh):
    torus = Mesh(
        mesh.devices.reshape(4, 4, mesh.shape["tp"], mesh.shape["rep"]),
        ("fs_0", "fs_1", "tp", "rep"),
    )
    grads, plain = P("rep", FS, "tp"), P(FS_REP, "tp")
    return jax.shard_map(
        local,
        mesh=torus,
        in_specs=(grads, plain, plain) * 3,
        out_specs=(plain,) * 6,
        check_vma=False,
    )
```

```python
import math

import jax
import jax.numpy as jnp
from jax import lax
from jax.experimental import pallas as pl
from jax.experimental.pallas import tpu as pltpu
from jax.sharding import Mesh
from jax.sharding import PartitionSpec as P

D = 2048
FF = 5632
FS_REP = ("fs_0", "fs_1", "rep")
FS = ("fs_0", "fs_1")

MOMENT = 0.95
COEF_ONE = 3.4445
COEF_THREE = -4.775
COEF_FIVE = 2.0315
SAFETY = 2.0
RATE = 0.5
SHRINK = 0.95
BF = jnp.bfloat16


def dot(a, b):
    return jnp.dot(a, b, preferred_element_type=jnp.float32)


def sum_at_owner(value, axis, dim):
    devices = lax.axis_size(axis)
    before, after = (value.shape[:dim], value.shape[dim + 1 :])
    tiles = jnp.moveaxis(value.reshape(*before, devices, -1, *after), dim, 0)
    tiles = lax.all_to_all(tiles, axis, 0, 0, tiled=True)
    return jnp.sum(tiles.astype(jnp.float32), axis=0)


N = 2048
HALF = 1024
CHUNK = 512
STEPS = N // CHUNK


def chunk_rows(r):
    return pl.ds(pl.multiple_of(r * CHUNK, CHUNK), CHUNK)


def iterate_kernel(
    raw, x_in, w_gate, w_up, gate_out, up_out, a, b, c, m, x0, x1, x2, final, trace, load_sem, send, recv, xsend, xrecv, fsend, frecv
):
    core = lax.axis_index("rep")
    place = lax.axis_index("tp")
    other = 1 - core
    kind = lax.rem(place, 2)
    ahead = lax.rem(place + 1, 4)
    behind = lax.rem(place + 3, 4)
    rows = x_in.shape[0]
    mine = pl.ds(pl.multiple_of(core * HALF, HALF), HALF)

    loads = [pltpu.make_async_copy(raw.at[pl.ds(i * CHUNK, CHUNK)], a.at[pl.ds(i * CHUNK, CHUNK)], load_sem.at[i]) for i in range(STEPS)]
    for copy in loads:
        copy.start()

    barrier = pltpu.get_barrier_semaphore()
    pl.semaphore_signal(barrier, inc=1, device_id={"rep": other}, device_id_type=pl.DeviceIdType.MESH)
    for near in (ahead, behind):
        for to in range(2):
            pl.semaphore_signal(barrier, inc=1, device_id={"tp": near, "rep": to}, device_id_type=pl.DeviceIdType.MESH)
    pl.semaphore_wait(barrier, 5)

    def remote(src, dst, ssem, rsem, to):
        return pltpu.make_async_remote_copy(
            src_ref=src, dst_ref=dst, send_sem=ssem, recv_sem=rsem, device_id=to, device_id_type=pl.DeviceIdType.MESH
        )

    partner = {"rep": other}

    def swap(buf, k, r, half):
        spot = buf.at[chunk_rows(r), pl.ds(pl.multiple_of(half * HALF, HALF), HALF)]
        return remote(spot, spot, send.at[k, r], recv.at[k, r], partner)

    def xswap(buf, k, half):
        spot = buf.at[:, pl.ds(pl.multiple_of(half * HALF, HALF), HALF)]
        return remote(spot, spot, xsend.at[k], xrecv.at[k], partner)

    own_rows = pl.ds(pl.multiple_of(core * rows, 16), rows)
    other_rows = pl.ds(pl.multiple_of(other * rows, 16), rows)
    x0[own_rows] = x_in[...]
    start_copy = remote(x0.at[own_rows], x0.at[own_rows], xsend.at[2], xrecv.at[2], partner)
    start_copy.start()

    for copy in loads:
        copy.wait()

    def squares(i, total):
        part = a[pl.ds(pl.multiple_of(i * 64, 64), 64), :].astype(jnp.float32)
        part = part * part
        return total + jnp.sum(part.reshape(8, 8, N), axis=0)

    second = jnp.sum(lax.fori_loop(0, N // 64, squares, jnp.zeros((8, N), jnp.float32)))
    same = lax.broadcasted_iota(jnp.int32, (128, 128), 0) == lax.broadcasted_iota(jnp.int32, (128, 128), 1)
    trace[...] = jnp.zeros((128, 128), jnp.float32)
    for i in range(N // 128):
        part = a[pl.ds(i * 128, 128), pl.ds(i * 128, 128)].astype(jnp.float32)
        trace[...] += jnp.where(same, part, 0.0)
    first = jnp.sum(trace[...])
    second = jnp.full((1, 1), second)
    first = jnp.full((1, 1), first)
    ratio = SAFETY * (second + 1.0) / (first + 1.0)
    alpha = 1.0 / ratio
    scale = lax.rsqrt(ratio)

    def square(left, k, low, high):
        def step(r, _):
            if k is not None:
                swap(left, k, r, core).wait_send()
                swap(left, k, r, other).wait_recv()
            s = dot(left[chunk_rows(r), :], left[:, mine])
            m[chunk_rows(r), :] = (low * left[chunk_rows(r), mine].astype(jnp.float32) + high * s).astype(BF)
            return 0

        lax.fori_loop(0, STEPS, step, 0)

    def times(left, k, out, k_out, factor):
        def step(r, _):
            if k is not None:
                swap(left, k, r, core).wait_send()
                swap(left, k, r, other).wait_recv()
            p = dot(left[chunk_rows(r), :], m[...])
            p = COEF_ONE * left[chunk_rows(r), mine].astype(jnp.float32) + p
            if factor is not None:
                p = factor * p
            out[chunk_rows(r), mine] = p.astype(BF)
            swap(out, k_out, r, core).start()
            return 0

        lax.fori_loop(0, STEPS, step, 0)

    square(a, None, COEF_THREE * alpha, COEF_FIVE * alpha * alpha)
    times(a, None, b, 0, alpha)
    start_copy.wait_send()
    remote(x0.at[other_rows], x0.at[other_rows], xsend.at[2], xrecv.at[2], partner).wait_recv()
    x1[:, mine] = (scale * (COEF_ONE * x0[:, mine].astype(jnp.float32) + dot(x0[...], m[...]))).astype(BF)
    xswap(x1, 0, core).start()
    times(b, 0, c, 1, None)
    square(c, 1, COEF_THREE, COEF_FIVE)
    times(c, None, b, 2, None)
    xswap(x1, 0, core).wait_send()
    xswap(x1, 0, other).wait_recv()
    x2[:, mine] = (COEF_ONE * x1[:, mine].astype(jnp.float32) + dot(x1[...], m[...])).astype(BF)
    xswap(x2, 1, core).start()
    times(b, 2, a, 3, None)
    square(a, 3, COEF_THREE, COEF_FIVE)
    xswap(x2, 1, core).wait_send()
    xswap(x2, 1, other).wait_recv()

    def last(where, block):
        cols = pl.ds(pl.multiple_of(block * 256, 256), 256)
        near = pl.ds(pl.multiple_of(core * HALF + block * 256, 256), 256)
        return (COEF_ONE * x2[where, near].astype(jnp.float32) + dot(x2[where, :], m[:, cols])).astype(BF)

    lower, upper = pl.ds(0, rows), pl.ds(rows, rows)
    final[2] = last(lower, ahead)
    to_ahead = remote(final.at[2], final.at[4 + core], fsend.at[0], frecv.at[core], {"tp": ahead, "rep": 0})
    to_ahead.start()
    final[3] = last(upper, behind)
    to_behind = remote(final.at[3], final.at[4 + core], fsend.at[1], frecv.at[core], {"tp": behind, "rep": 1})
    to_behind.start()
    final[6] = last(other_rows, place)
    to_partner = remote(final.at[6], final.at[core], fsend.at[2], frecv.at[2], partner)
    to_partner.start()
    final[core] = last(own_rows, place)
    to_ahead.wait_send()
    to_behind.wait_send()
    to_partner.wait_send()
    remote(final.at[6], final.at[other], fsend.at[2], frecv.at[2], partner).wait_recv()
    for i in range(2):
        remote(final.at[2], final.at[4 + i], fsend.at[0], frecv.at[i], partner).wait_recv()
    size = RATE * math.sqrt(FF)
    for i in range(2):
        cols = pl.ds(i * 256, 256)
        owned = final[i].astype(jnp.float32)
        fetched = final[4 + i].astype(jnp.float32)
        even = kind == 0
        gate_out[:, cols] = SHRINK * w_gate[:, cols] - size * jnp.where(even, owned, fetched)
        up_out[:, cols] = SHRINK * w_up[:, cols] - size * jnp.where(even, fetched, owned)


def iterate(raw, start, w_gate, w_up):
    rows, width = w_gate.shape
    whole = pl.BlockSpec(memory_space=pltpu.VMEM)
    dma = pltpu.SemaphoreType.DMA
    square = pltpu.VMEM((N, N), BF)
    wide = pltpu.VMEM((2 * rows, N), BF)
    return pl.pallas_call(
        iterate_kernel,
        out_shape=[jax.ShapeDtypeStruct((rows, width), jnp.float32)] * 2,
        in_specs=[pl.BlockSpec(memory_space=pl.ANY), whole, whole, whole],
        out_specs=[whole] * 2,
        scratch_shapes=[
            square,
            square,
            square,
            pltpu.VMEM((N, HALF), BF),
            wide,
            wide,
            wide,
            pltpu.VMEM((7, rows, 256), BF),
            pltpu.VMEM((128, 128), jnp.float32),
            dma((STEPS,)),
            dma((4, STEPS)),
            dma((4, STEPS)),
            dma((3,)),
            dma((3,)),
            dma((3,)),
            dma((3,)),
        ],
        compiler_params=pltpu.CompilerParams(collective_id=0, has_side_effects=True, vmem_limit_bytes=60 * 1024 * 1024),
    )(raw, start, w_gate, w_up)


def inner_order(value):
    rows = value.shape[0]
    return jnp.swapaxes(value.reshape(rows, 4, 2, 256), 1, 2).reshape(rows, N)


def chain(raw, start):
    raw = raw.astype(jnp.float32)
    ratio = SAFETY * (jnp.sum(raw * raw) + 1.0) / (jnp.trace(raw) + 1.0)
    scale = lax.rsqrt(ratio)
    g = (raw / ratio).astype(BF)
    x, factor = start, scale
    for index in range(3):
        s = dot(g, g)
        m = (COEF_THREE * g.astype(jnp.float32) + COEF_FIVE * s).astype(BF)
        if index == 2:
            return x, m
        t = (COEF_ONE * g.astype(jnp.float32) + dot(g, m)).astype(BF)
        x = (factor * (COEF_ONE * x.astype(jnp.float32) + dot(x, m))).astype(BF)
        g = (COEF_ONE * t.astype(jnp.float32) + dot(t, m)).astype(BF)
        factor = 1.0


def last(x, m, column, width):
    own = lax.dynamic_slice_in_dim(x, column * width, width, 1)
    cols = lax.dynamic_slice_in_dim(m, column * width, width, 1)
    return (COEF_ONE * own.astype(jnp.float32) + dot(x, cols)).astype(BF)


def local(
    gate_grads,
    gate_velocity,
    gate_weight,
    up_grads,
    up_velocity,
    up_weight,
    branch_grads,
    branch_velocity,
    branch_weight,
):
    both = jnp.concatenate((gate_grads.astype(BF), up_grads.astype(BF)), axis=0)
    total = sum_at_owner(both, "rep", 1)
    totals = (total[0], total[1], sum_at_owner(branch_grads.astype(BF), "rep", 1)[0])
    velocities = (gate_velocity, up_velocity, branch_velocity)
    moments = [MOMENT * velocity + part for velocity, part in zip(velocities, totals)]
    gate, up, branch = [moment.astype(BF) for moment in moments]
    rows = gate.shape[0]
    width = gate.shape[1]
    place = lax.axis_index("tp")
    odd = place % 2

    wide = lax.all_gather(jnp.concatenate((gate, up), axis=0), "tp", axis=1, tiled=True)
    gate_wide, up_wide = wide[:rows], wide[rows:]
    branch_wide = lax.all_gather(branch, "tp", axis=1, tiled=True)
    turn = (((0,), (0,)), ((), ()))
    parts = [
        lax.dot_general(whole, own, turn, preferred_element_type=jnp.float32).astype(BF)
        for whole, own in ((gate_wide, gate), (up_wide, up), (branch_wide, branch))
    ]
    share = sum_at_owner(jnp.concatenate(parts[:2], axis=1), FS_REP, 0).astype(BF)
    share_b = sum_at_owner(parts[2], FS_REP, 0).astype(BF)
    swapped = lax.all_gather(share, "tp", axis=0, tiled=False)
    mine = jnp.where(odd == 0, swapped[:, :, :width], swapped[:, :, width:])
    mine = jnp.moveaxis(mine, 0, 1).reshape(mine.shape[1], -1)
    raw = lax.all_gather(mine, FS_REP, axis=0, tiled=True)
    line_b = lax.all_gather(share_b, "tp", axis=1, tiled=True)
    raw_b = lax.all_gather(line_b, FS_REP, axis=0, tiled=True)
    start = jnp.where(odd == 0, gate_wide, up_wide)

    raw = inner_order(inner_order(raw).T)
    gate_new, up_new = iterate(raw, inner_order(start), gate_weight, up_weight)
    xb, mb = chain(raw_b, branch_wide)
    final_b = last(xb, mb, place, branch.shape[1])
    branch_new = SHRINK * branch_weight - RATE * math.sqrt(D) * final_b.astype(jnp.float32)
    return moments[0], gate_new, moments[1], up_new, moments[2], branch_new


def solution(mesh):
    torus = Mesh(
        mesh.devices.reshape(4, 4, mesh.shape["tp"], mesh.shape["rep"]),
        ("fs_0", "fs_1", "tp", "rep"),
    )
    grads, plain = P("rep", FS, "tp"), P(FS_REP, "tp")
    return jax.shard_map(
        local,
        mesh=torus,
        in_specs=(grads, plain, plain) * 3,
        out_specs=(plain,) * 6,
        check_vma=False,
    )
```

```python
import functools
import math

import jax
import jax.numpy as jnp
from jax import lax
from jax.experimental import pallas as pl
from jax.experimental.pallas import tpu as pltpu
from jax.sharding import Mesh
from jax.sharding import PartitionSpec as P

D = 2048
FF = 5632
FS_REP = ("fs_0", "fs_1", "rep")
FS = ("fs_0", "fs_1")

MOMENT = 0.95
COEF_ONE = 3.4445
COEF_THREE = -4.775
COEF_FIVE = 2.0315
SAFETY = 2.0
RATE = 0.5
SHRINK = 0.95
BF = jnp.bfloat16


def dot(a, b):
    return jnp.dot(a, b, preferred_element_type=jnp.float32)


N = 2048
HALF = 1024
CHUNK = 512
STEPS = N // CHUNK
NB = 1024
COPIES = 160
MESH = pl.DeviceIdType.MESH


def at(index, size):
    return pl.ds(index * size if isinstance(index, int) else pl.multiple_of(index * size, size), size)


def spot(offset, size, unit):
    return pl.ds(pl.multiple_of(offset, unit), size)


def turned(a, b):
    return lax.dot_general(a, b, (((0,), (0,)), ((), ())), preferred_element_type=jnp.float32)


def kernel(
    gate_g, up_g, branch_g, gate_v, up_v, branch_v, gate_w, up_w, branch_w,
    gate_m, gate_out, up_m, up_out, branch_m, branch_out,
    a, b, c, m, xs, xb, x1, x2, final,
    give, take, give_b, take_b,
    part, near, kept, near2, piece, panels,
    part_b, near_b, kept_b, near2_b, gram_b, m_b, t_b, g_b,
    sems, recvs, send, recv,
):
    core = lax.axis_index("rep")
    place = lax.axis_index("tp")
    iy = lax.axis_index("fs_1")
    iz = lax.axis_index("fs_0")
    other = 1 - core
    kind = lax.rem(place, 2)
    ahead = lax.rem(place + 1, 4)
    behind = lax.rem(place + 3, 4)
    across = lax.rem(place + 2, 4)
    rows = gate_v.shape[0]
    rows_b = branch_v.shape[0]
    mine = at(core, HALF)
    partner = {"rep": other}
    used = []

    def turn(axis, index, step):
        return {axis: lax.rem(index + step, 4)}

    def remote(src, dst, to):
        k = len(used)
        copy = pltpu.make_async_remote_copy(
            src_ref=src, dst_ref=dst, send_sem=sems.at[k], recv_sem=recvs.at[k], device_id=to, device_id_type=MESH
        )
        used.append(copy)
        return copy

    def send_to(ref, to):
        copy = remote(ref, ref, to)
        copy.start()
        return copy

    barrier = pltpu.get_barrier_semaphore()
    peers = [partner, {"tp": across}]
    peers += [{"tp": x, "rep": r} for x in (ahead, behind) for r in range(2)]
    peers += [turn(axis, index, step) for axis, index in (("fs_1", iy), ("fs_0", iz)) for step in (1, 2, 3)]
    for to in peers:
        pl.semaphore_signal(barrier, inc=1, device_id=to, device_id_type=MESH)

    own_rows, other_rows = at(core, rows), at(other, rows)
    give[0] = gate_g[0, other_rows, :].astype(BF)
    give[1] = up_g[0, other_rows, :].astype(BF)
    give_b[...] = branch_g[0, at(other, rows_b), :].astype(BF)
    pl.semaphore_wait(barrier, len(peers))
    first_copies = [remote(give_b, take_b, partner), remote(give, take, partner)]
    for copy in first_copies:
        copy.start()
    same = lax.broadcasted_iota(jnp.int32, (128, 128), 0) == lax.broadcasted_iota(jnp.int32, (128, 128), 1)

    def columns(ref, lines, height, width):
        def block(x, part):
            return ref.at[at(core, height), spot(part * 4 * width + x * width, width, width)]

        state = {}

        def start():
            state["right"] = [send_to(block(place, p), {"tp": ahead}) for p in range(2)]
            state["left"] = [send_to(block(place, p), {"tp": behind}) for p in range(2)]
            state["own"] = [send_to(block(place, p), partner) for p in range(2)]

        def second():
            state["right"][0].wait_recv()
            far = [send_to(block(behind, 0), {"tp": ahead})]
            state["left"][1].wait_recv()
            far.append(send_to(block(ahead, 1), {"tp": behind}))
            state["far"] = far
            state["own"].append(send_to(block(behind, 0), partner))
            state["own"].append(send_to(block(ahead, 1), partner))
            state["right"][1].wait_recv()
            state["own"].append(send_to(block(behind, 1), partner))
            state["left"][0].wait_recv()
            state["own"].append(send_to(block(ahead, 0), partner))

        def finish():
            for p in range(2):
                state["far"][p].wait_recv()
                state["own"].append(send_to(block(across, p), partner))
            for copy in state["own"]:
                copy.wait_recv()

        return start, second, finish

    gate_x, up_x = xs.at[0], xs.at[1]
    lines = [columns(xb, None, rows_b, 128), columns(gate_x, None, rows, 256), columns(up_x, None, rows, 256)]
    first_copies[0].wait_recv()
    moment = MOMENT * branch_v[...] + (branch_g[0, at(core, rows_b), :] + take_b[...].astype(jnp.float32))
    branch_m[...] = moment
    for p in range(2):
        xb[at(core, rows_b), spot(p * 512 + place * 128, 128, 128)] = moment[:, p * 128 : p * 128 + 128].astype(BF)
    lines[0][0]()
    first_copies[1].wait_recv()
    for i, (grads, velocity, out) in enumerate(((gate_g, gate_v, gate_m), (up_g, up_v, up_m))):
        moment = MOMENT * velocity[...] + (grads[0, own_rows, :] + take[i].astype(jnp.float32))
        out[...] = moment
        for p in range(2):
            xs[i, own_rows, spot(p * HALF + place * 256, 256, 256)] = moment[:, p * 256 : p * 256 + 256].astype(BF)
        lines[1 + i][0]()

    axes = ((("fs_1", iy), ("fs_0", iz)), (("fs_0", iz), ("fs_1", iy)))

    def exchange(source, landing, axis, index):
        copies = []
        for step in (2, 1, 3):
            to = lax.rem(index + step, 4)
            copies.append(remote(source(to), landing.at[step - 1], {axis: to}))
            copies[-1].start()
        return copies

    def total(own, landing, copies):
        for copy in copies:
            copy.wait_recv()
        value = own.astype(jnp.float32)
        for k in range(3):
            value = value + landing[k].astype(jnp.float32)
        return value.astype(BF)

    def scatter_one(source, landings):
        return [
            exchange(functools.partial(source, p), landings[p], *axes[p][0]) for p in range(2)
        ]

    def source_of(i):
        return lambda p, t: part.at[i, at(t, 64), at(p, 640)]

    def source_b(p, t):
        return part_b.at[spot(p * 64 + t * 16, 16, 16), :]

    lines[0][1]()
    lines[0][2]()
    part_b[...] = turned(xb[:, spot(core * 512 + place * 128, 128, 128)], xb[...]).astype(BF)
    one_b = scatter_one(source_b, [near_b.at[p] for p in range(2)])
    lines[1][1]()
    lines[2][1]()

    def panel(i):
        lines[1 + i][2]()
        own = xs[i, :, spot(core * HALF + place * 256, 256, 256)]
        for d in range(5):
            block = lax.rem(core * 4 + place + d, 8)
            part[i, :, at(d, 256)] = turned(own, xs[i, :, at(block, 256)]).astype(BF)
        return scatter_one(source_of(i), [near.at[i, p] for p in range(2)])

    ones = [panel(0)]
    two_b = []
    for p in range(2):
        kept_b[p] = total(part_b[spot(p * 64 + axes[p][0][1] * 16, 16, 16), :], near_b.at[p], one_b[p])
        two_b.append(exchange(lambda t, p=p: kept_b.at[p, :, at(t, 256)], near2_b.at[p], *axes[p][1]))
    ones.append(panel(1))

    def gram_rows(p, i1):
        return spot(p * 64 + i1 * 16, 16, 16)

    group = at(core, 4)
    swaps_b = []
    for p in range(2):
        i1, i2 = axes[p][0][1], axes[p][1][1]
        gram_b[core * 4 + place, gram_rows(p, i1), at(i2, 256)] = total(
            kept_b[p, :, at(i2, 256)], near2_b.at[p], two_b[p]
        )
        ref = gram_b.at[core * 4 + place, gram_rows(p, i1), at(i2, 256)]
        swaps_b.append([send_to(ref, {"tp": x}) for x in (across, ahead, behind)])
    twos = []
    for i in range(2):
        pair = []
        for p in range(2):
            index = axes[p][0][1]
            kept[i, p] = total(part[i, at(index, 64), at(p, 640)], near.at[i, p], ones[i][p])
            pair.append(exchange(lambda t, i=i, p=p: kept.at[i, p, at(t, 16), :], near2.at[i, p], *axes[p][1]))
        twos.append(pair)

    class Ring:
        def __init__(self, axis, index, block, cut):
            self.next, self.prev = turn(axis, index, 1), turn(axis, index, 3)
            self.index, self.block, self.cut = index, block, cut

        def start(self):
            ref = self.block(self.index)
            self.right = send_to(ref, self.next)
            self.left = send_to(ref, self.prev)

        def second(self):
            self.right.wait_recv()
            self.far = [send_to(self.cut(lax.rem(self.index + 3, 4), 0), self.next)]
            self.left.wait_recv()
            self.far.append(send_to(self.cut(lax.rem(self.index + 1, 4), 1), self.prev))

        def finish(self):
            for copy in self.far:
                copy.wait_recv()

    def rings(phase, block, cut):
        return [
            Ring(*axes[p][phase], functools.partial(block, p), functools.partial(cut, p)) for p in range(2)
        ]

    def b_small(p, j):
        return gram_b.at[group, gram_rows(p, axes[p][0][1]), at(j, 256)]

    def b_small_cut(p, j, h):
        return gram_b.at[at(core * 2 + h, 2), gram_rows(p, axes[p][0][1]), at(j, 256)]

    def b_large(p, j):
        return gram_b.at[group, gram_rows(p, j), :]

    def b_large_cut(p, j, h):
        return gram_b.at[at(core * 2 + h, 2), gram_rows(p, j), :]

    def g_rows(p, j):
        return spot(axes[p][0][1] * 64 + j * 16, 16, 16)

    def g_small(p, j):
        return panels.at[core, :, g_rows(p, j), at(p, 640)]

    def g_small_cut(p, j, h):
        return panels.at[core, at(h, 2), g_rows(p, j), at(p, 640)]

    def g_large(p, j):
        return panels.at[core, :, at(j, 64), at(p, 640)]

    def g_large_cut(p, j, h):
        return panels.at[core, at(h, 2), at(j, 64), at(p, 640)]

    small_b, large_b = rings(1, b_small, b_small_cut), rings(0, b_large, b_large_cut)
    small, large = rings(1, g_small, g_small_cut), rings(0, g_large, g_large_cut)
    for p in range(2):
        for copy in swaps_b[p]:
            copy.wait_recv()
        small_b[p].start()
    swaps = []
    for p in range(2):
        i2 = axes[p][1][1]
        for i in range(2):
            piece[i, p] = total(kept[i, p, at(i2, 16), :], near2.at[i, p], twos[i][p])
        target = panels.at[core, place, g_rows(p, i2), at(p, 640)]
        panels[core, place, g_rows(p, i2), at(p, 640)] = piece[kind, p]
        swaps.append(send_to(target, {"tp": across}))
        for x in (ahead, behind):
            copy = remote(piece.at[1 - kind, p], target, {"tp": x})
            copy.start()
            swaps.append(copy)
    for ring in small_b:
        ring.second()
    for copy in swaps:
        copy.wait_recv()
    for ring in small:
        ring.start()
    for ring in small_b:
        ring.finish()
    for ring in large_b:
        ring.start()
    for ring in small:
        ring.second()
    forward_b, forward = [], []
    for p, ring in enumerate(large_b):
        ring.second()
        forward_b += [send_to(b_large(p, lax.rem(ring.index + k, 4)), partner) for k in (0, 3, 1)]
    for ring in small:
        ring.finish()
    for ring in large:
        ring.start()
    for p, ring in enumerate(large_b):
        ring.finish()
        forward_b.append(send_to(b_large(p, lax.rem(ring.index + 2, 4)), partner))
    for copy in forward_b:
        copy.wait_recv()

    def coefficients(squares, diagonal):
        second = jnp.full((1, 1), squares)
        first = jnp.full((1, 1), diagonal)
        ratio = SAFETY * (second + 1.0) / (first + 1.0)
        return 1.0 / ratio, lax.rsqrt(ratio)

    def squares_b(i, sums):
        value = gram_b[i].astype(jnp.float32)
        diagonal = gram_b[i, :, at(i, 128)].astype(jnp.float32)
        return (
            sums[0] + jnp.sum((value * value).reshape(16, 8, NB), axis=0),
            sums[1] + jnp.where(same, diagonal, 0.0),
        )

    sums = lax.fori_loop(0, 8, squares_b, (jnp.zeros((8, NB), jnp.float32), jnp.zeros((128, 128), jnp.float32)))
    alpha_b, scale_b = coefficients(jnp.sum(sums[0]), jnp.sum(sums[1]))

    def square_b(left, low, high):
        def step(r, _):
            where = at(r, 512)
            m_b[where, :] = (low * left[where, :].astype(jnp.float32) + high * dot(left[where, :], left[...])).astype(BF)
            return 0

        lax.fori_loop(0, 2, step, 0)

    def times_b(left, out, factor):
        def step(r, _):
            where = at(r, 512)
            value = factor * (COEF_ONE * left[where, :].astype(jnp.float32) + dot(left[where, :], m_b[...]))
            out[where, :] = value.astype(BF)
            return 0

        lax.fori_loop(0, 2, step, 0)

    def rows_of(left, factor):
        return (factor * (COEF_ONE * left.astype(jnp.float32) + dot(left, m_b[...]))).astype(BF)

    for i in range(8):
        g_b[at(i, 128), :] = gram_b[i]
    square_b(g_b, COEF_THREE * alpha_b, COEF_FIVE * alpha_b * alpha_b)
    times_b(g_b, t_b, alpha_b)
    line = rows_of(xb[at(core, rows_b), :], scale_b)
    times_b(t_b, g_b, 1.0)
    square_b(g_b, COEF_THREE, COEF_FIVE)
    for p, ring in enumerate(large):
        ring.second()
        forward += [send_to(g_large(p, lax.rem(ring.index + k, 4)), partner) for k in (0, 3, 1)]
    times_b(g_b, t_b, 1.0)
    line = rows_of(line, 1.0)
    times_b(t_b, g_b, 1.0)
    for p, ring in enumerate(large):
        ring.finish()
        forward.append(send_to(g_large(p, lax.rem(ring.index + 2, 4)), partner))
    square_b(g_b, COEF_THREE, COEF_FIVE)
    t_b[0:rows_b, :] = line
    for p in range(2):
        cols = spot(p * 512 + place * 128, 128, 128)
        last_b = COEF_ONE * t_b[0:rows_b, cols].astype(jnp.float32) + dot(line, m_b[:, cols])
        branch_out[:, at(p, 128)] = SHRINK * branch_w[:, at(p, 128)] - RATE * math.sqrt(D) * last_b.astype(BF).astype(
            jnp.float32
        )
    for copy in forward:
        copy.wait_recv()

    def assemble(r, sums):
        value = panels[lax.div(r, 4), lax.rem(r, 4)]
        squares, diagonal = sums
        for d in range(5):
            block = value[:, d * 256 : d * 256 + 256]
            column = at(lax.rem(r + d, 8), 256)
            a[at(r, 256), column] = block
            if 0 < d < 4:
                a[column, at(r, 256)] = block.T
            wide = block.astype(jnp.float32)
            weight = 2.0 if 0 < d < 4 else 1.0
            squares = squares + weight * jnp.sum((wide * wide).reshape(32, 8, 256), axis=0)
        for k in range(2):
            corner = value[k * 128 : k * 128 + 128, k * 128 : k * 128 + 128].astype(jnp.float32)
            diagonal = diagonal + jnp.where(same, corner, 0.0)
        return squares, diagonal

    sums = lax.fori_loop(0, 8, assemble, (jnp.zeros((8, 256), jnp.float32), jnp.zeros((128, 128), jnp.float32)))
    alpha, scale = coefficients(jnp.sum(sums[0]), jnp.sum(sums[1]))

    x0 = xs.at[kind]

    def swap(buf, k, r, half):
        ref = buf.at[at(r, CHUNK), at(half, HALF)]
        return pltpu.make_async_remote_copy(
            src_ref=ref, dst_ref=ref, send_sem=send.at[k, r], recv_sem=recv.at[k, r], device_id=partner, device_id_type=MESH
        )

    def square(left, k, low, high):
        def step(r, _):
            if k is not None:
                swap(left, k, r, core).wait_send()
                swap(left, k, r, other).wait_recv()
            s = dot(left[at(r, CHUNK), :], left[:, mine])
            m[at(r, CHUNK), :] = (low * left[at(r, CHUNK), mine].astype(jnp.float32) + high * s).astype(BF)
            return 0

        lax.fori_loop(0, STEPS, step, 0)

    def times(left, k, out, k_out, factor):
        def step(r, _):
            if k is not None:
                swap(left, k, r, core).wait_send()
                swap(left, k, r, other).wait_recv()
            p = dot(left[at(r, CHUNK), :], m[...])
            p = COEF_ONE * left[at(r, CHUNK), mine].astype(jnp.float32) + p
            if factor is not None:
                p = factor * p
            out[at(r, CHUNK), mine] = p.astype(BF)
            swap(out, k_out, r, core).start()
            return 0

        lax.fori_loop(0, STEPS, step, 0)

    square(a, None, COEF_THREE * alpha, COEF_FIVE * alpha * alpha)
    times(a, None, b, 0, alpha)
    x1[:, mine] = (scale * (COEF_ONE * x0[:, mine].astype(jnp.float32) + dot(x0[...], m[...]))).astype(BF)
    turn_one = send_to(x1.at[:, mine], partner)
    times(b, 0, c, 1, None)
    square(c, 1, COEF_THREE, COEF_FIVE)
    times(c, None, b, 2, None)
    turn_one.wait_recv()
    x2[:, mine] = (COEF_ONE * x1[:, mine].astype(jnp.float32) + dot(x1[...], m[...])).astype(BF)
    turn_two = send_to(x2.at[:, mine], partner)
    times(b, 2, a, 3, None)
    square(a, 3, COEF_THREE, COEF_FIVE)
    turn_two.wait_recv()

    def last(where, block):
        cols = at(block, 256)
        close = spot(core * HALF + block * 256, 256, 256)
        return (COEF_ONE * x2[where, close].astype(jnp.float32) + dot(x2[where, :], m[:, cols])).astype(BF)

    final[2] = last(pl.ds(0, rows), ahead)
    to_ahead = pltpu.make_async_remote_copy(
        src_ref=final.at[2], dst_ref=final.at[4 + core], send_sem=sems.at[COPIES], recv_sem=recvs.at[COPIES + core],
        device_id={"tp": ahead, "rep": 0}, device_id_type=MESH,
    )
    to_ahead.start()
    final[3] = last(pl.ds(rows, rows), behind)
    to_behind = pltpu.make_async_remote_copy(
        src_ref=final.at[3], dst_ref=final.at[4 + core], send_sem=sems.at[COPIES + 1], recv_sem=recvs.at[COPIES + core],
        device_id={"tp": behind, "rep": 1}, device_id_type=MESH,
    )
    to_behind.start()
    final[6] = last(other_rows, place)
    to_partner = remote(final.at[6], final.at[core], partner)
    to_partner.start()
    final[core] = last(own_rows, place)
    to_partner.wait_recv()
    for i in range(2):
        pltpu.make_async_remote_copy(
            src_ref=final.at[2], dst_ref=final.at[4 + i], send_sem=sems.at[COPIES], recv_sem=recvs.at[COPIES + i],
            device_id=partner, device_id_type=MESH,
        ).wait_recv()
    size = RATE * math.sqrt(FF)
    for i in range(2):
        cols = pl.ds(i * 256, 256)
        owned = final[i].astype(jnp.float32)
        fetched = final[4 + i].astype(jnp.float32)
        even = kind == 0
        gate_out[:, cols] = SHRINK * gate_w[:, cols] - size * jnp.where(even, owned, fetched)
        up_out[:, cols] = SHRINK * up_w[:, cols] - size * jnp.where(even, fetched, owned)
    to_ahead.wait_send()
    to_behind.wait_send()
    for copy in used:
        copy.wait_send()


def local(*args):
    velocities = (args[1], args[4], args[7])
    rows, width = velocities[0].shape
    rows_b, width_b = velocities[2].shape
    whole = pl.BlockSpec(memory_space=pltpu.VMEM)
    dma = pltpu.SemaphoreType.DMA

    def buf(*shape):
        return pltpu.VMEM(shape, BF)

    outs = []
    for velocity in velocities:
        outs += [jax.ShapeDtypeStruct(velocity.shape, jnp.float32)] * 2
    return pl.pallas_call(
        kernel,
        out_shape=outs,
        in_specs=[whole] * 9,
        out_specs=[whole] * 6,
        scratch_shapes=[
            buf(N, N), buf(N, N), buf(N, N), buf(N, HALF),
            buf(2, 2 * rows, N), buf(2 * rows_b, NB), buf(2 * rows, N), buf(2 * rows, N), buf(7, rows, 256),
            buf(2, rows, width), buf(2, rows, width), buf(rows_b, width_b), buf(rows_b, width_b),
            buf(2, 256, 1280), buf(2, 2, 3, 64, 640), buf(2, 2, 64, 640), buf(2, 2, 3, 16, 640), buf(2, 2, 16, 640),
            buf(2, 4, 256, 1280),
            buf(128, NB), buf(2, 3, 16, NB), buf(2, 16, NB), buf(2, 3, 16, 256), buf(8, 128, NB),
            buf(NB, NB), buf(NB, NB), buf(NB, NB),
            dma((COPIES + 2,)), dma((COPIES + 2,)), dma((4, STEPS)), dma((4, STEPS)),
        ],
        compiler_params=pltpu.CompilerParams(collective_id=0, has_side_effects=True, vmem_limit_bytes=63 * 1024 * 1024),
    )(args[0], args[3], args[6], args[1], args[4], args[7], args[2], args[5], args[8])


def solution(mesh):
    torus = Mesh(
        mesh.devices.reshape(4, 4, mesh.shape["tp"], mesh.shape["rep"]),
        ("fs_0", "fs_1", "tp", "rep"),
    )
    grads, plain = P("rep", FS, "tp"), P(FS_REP, "tp")
    return jax.shard_map(
        local,
        mesh=torus,
        in_specs=(grads, plain, plain) * 3,
        out_specs=(plain,) * 6,
        check_vma=False,
    )
```

```python
import functools
import math

import jax
import jax.numpy as jnp
from jax import lax
from jax.experimental import pallas as pl
from jax.experimental.pallas import tpu as pltpu
from jax.sharding import Mesh
from jax.sharding import PartitionSpec as P

D = 2048
FF = 5632
FS_REP = ("fs_0", "fs_1", "rep")
FS = ("fs_0", "fs_1")

MOMENT = 0.95
COEF_ONE = 3.4445
COEF_THREE = -4.775
COEF_FIVE = 2.0315
SAFETY = 2.0
RATE = 0.5
SHRINK = 0.95
BF = jnp.bfloat16


def dot(a, b):
    return jnp.dot(a, b, preferred_element_type=jnp.float32)


N = 2048
HALF = 1024
CHUNK = 512
STEPS = N // CHUNK
NB = 1024
COPIES = 160
MESH = pl.DeviceIdType.MESH


def at(index, size):
    return pl.ds(index * size if isinstance(index, int) else pl.multiple_of(index * size, size), size)


def spot(offset, size, unit):
    return pl.ds(pl.multiple_of(offset, unit), size)


def turned(a, b):
    return lax.dot_general(a, b, (((0,), (0,)), ((), ())), preferred_element_type=jnp.float32)


def kernel(
    gate_g, up_g, branch_g, gate_v, up_v, branch_v,
    gate_m, up_m, branch_m, gate_out, up_out, branch_out,
    grads, grads_b, speed, speed_b, results, results_b, in_sem, out_sem,
    a, b, c, m, xs, xb, x1, x2, final,
    give, take, give_b, take_b,
    part, near, kept, near2, piece, panels,
    part_b, near_b, kept_b, near2_b, gram_b, m_b, t_b, g_b,
    sems, recvs, send, recv,
):
    core = lax.axis_index("rep")
    place = lax.axis_index("tp")
    iy = lax.axis_index("fs_1")
    iz = lax.axis_index("fs_0")
    other = 1 - core
    kind = lax.rem(place, 2)
    ahead = lax.rem(place + 1, 4)
    behind = lax.rem(place + 3, 4)
    across = lax.rem(place + 2, 4)
    rows = gate_v.shape[0]
    rows_b = branch_v.shape[0]
    loads = []

    def load(source, target):
        copy = pltpu.make_async_copy(source, target, in_sem.at[len(loads)])
        copy.start()
        loads.append(copy)

    load(branch_g.at[0, at(other, rows_b)], grads_b.at[1])
    load(gate_g.at[0, at(other, rows)], grads.at[0, 1])
    load(up_g.at[0, at(other, rows)], grads.at[1, 1])
    load(branch_g.at[0, at(core, rows_b)], grads_b.at[0])
    load(branch_v, speed_b)
    load(gate_g.at[0, at(core, rows)], grads.at[0, 0])
    load(gate_v, speed.at[0])
    load(up_g.at[0, at(core, rows)], grads.at[1, 0])
    load(up_v, speed.at[1])
    mine = at(core, HALF)
    partner = {"rep": other}
    used = []

    def turn(axis, index, step):
        return {axis: lax.rem(index + step, 4)}

    def remote(src, dst, to):
        k = len(used)
        copy = pltpu.make_async_remote_copy(
            src_ref=src, dst_ref=dst, send_sem=sems.at[k], recv_sem=recvs.at[k], device_id=to, device_id_type=MESH
        )
        used.append(copy)
        return copy

    def send_to(ref, to):
        copy = remote(ref, ref, to)
        copy.start()
        return copy

    barrier = pltpu.get_barrier_semaphore()
    peers = [partner, {"tp": across}]
    peers += [{"tp": x, "rep": r} for x in (ahead, behind) for r in range(2)]
    peers += [turn(axis, index, step) for axis, index in (("fs_1", iy), ("fs_0", iz)) for step in (1, 2, 3)]
    for to in peers:
        pl.semaphore_signal(barrier, inc=1, device_id=to, device_id_type=MESH)

    own_rows, other_rows = at(core, rows), at(other, rows)
    loads[0].wait()
    give_b[...] = grads_b[1].astype(BF)
    for i in range(2):
        loads[1 + i].wait()
        give[i] = grads[i, 1].astype(BF)
    pl.semaphore_wait(barrier, len(peers))
    first_copies = [remote(give_b, take_b, partner)]
    first_copies += [remote(give.at[i], take.at[i], partner) for i in range(2)]
    for copy in first_copies:
        copy.start()
    same = lax.broadcasted_iota(jnp.int32, (128, 128), 0) == lax.broadcasted_iota(jnp.int32, (128, 128), 1)

    def columns(ref, lines, height, width):
        def block(x, part):
            return ref.at[at(core, height), spot(part * 4 * width + x * width, width, width)]

        state = {}

        def start():
            state["right"] = [send_to(block(place, p), {"tp": ahead}) for p in range(2)]
            state["left"] = [send_to(block(place, p), {"tp": behind}) for p in range(2)]
            state["own"] = [send_to(block(place, p), partner) for p in range(2)]

        def second():
            state["right"][0].wait_recv()
            far = [send_to(block(behind, 0), {"tp": ahead})]
            state["left"][1].wait_recv()
            far.append(send_to(block(ahead, 1), {"tp": behind}))
            state["far"] = far
            state["own"].append(send_to(block(behind, 0), partner))
            state["own"].append(send_to(block(ahead, 1), partner))
            state["right"][1].wait_recv()
            state["own"].append(send_to(block(behind, 1), partner))
            state["left"][0].wait_recv()
            state["own"].append(send_to(block(ahead, 0), partner))

        def finish():
            for p in range(2):
                state["far"][p].wait_recv()
                state["own"].append(send_to(block(across, p), partner))
            for copy in state["own"]:
                copy.wait_recv()

        return start, second, finish

    gate_x, up_x = xs.at[0], xs.at[1]
    lines = [columns(xb, None, rows_b, 128), columns(gate_x, None, rows, 256), columns(up_x, None, rows, 256)]
    first_copies[0].wait_recv()
    loads[3].wait()
    loads[4].wait()
    moment = MOMENT * speed_b[...] + (grads_b[0] + take_b[...].astype(jnp.float32))
    speed_b[...] = moment
    for p in range(2):
        xb[at(core, rows_b), spot(p * 512 + place * 128, 128, 128)] = moment[:, p * 128 : p * 128 + 128].astype(BF)
    lines[0][0]()
    for i in range(2):
        first_copies[1 + i].wait_recv()
        loads[5 + 2 * i].wait()
        loads[6 + 2 * i].wait()
        moment = MOMENT * speed[i] + (grads[i, 0] + take[i].astype(jnp.float32))
        speed[i] = moment
        for p in range(2):
            xs[i, own_rows, spot(p * HALF + place * 256, 256, 256)] = moment[:, p * 256 : p * 256 + 256].astype(BF)
        lines[1 + i][0]()
    stores = []

    def store(source, target):
        copy = pltpu.make_async_copy(source, target, out_sem.at[len(stores)])
        copy.start()
        stores.append(copy)

    axes = ((("fs_1", iy), ("fs_0", iz)), (("fs_0", iz), ("fs_1", iy)))

    def exchange(source, landing, axis, index):
        copies = []
        for step in (2, 1, 3):
            to = lax.rem(index + step, 4)
            copies.append(remote(source(to), landing.at[step - 1], {axis: to}))
            copies[-1].start()
        return copies

    def total(own, landing, copies):
        for copy in copies:
            copy.wait_recv()
        value = own.astype(jnp.float32)
        for k in range(3):
            value = value + landing[k].astype(jnp.float32)
        return value.astype(BF)

    def scatter_one(source, landings):
        return [
            exchange(functools.partial(source, p), landings[p], *axes[p][0]) for p in range(2)
        ]

    def source_of(i):
        return lambda p, t: part.at[i, at(t, 64), at(p, 640)]

    def source_b(p, t):
        return part_b.at[spot(p * 64 + t * 16, 16, 16), :]

    def panel(i):
        lines[1 + i][2]()
        own = xs[i, :, spot(core * HALF + place * 256, 256, 256)]
        for d in range(5):
            block = lax.rem(core * 4 + place + d, 8)
            part[i, :, at(d, 256)] = turned(own, xs[i, :, at(block, 256)]).astype(BF)
        return scatter_one(source_of(i), [near.at[i, p] for p in range(2)])

    def gram_rows(p, i1):
        return spot(p * 64 + i1 * 16, 16, 16)

    group = at(core, 4)

    class Ring:
        def __init__(self, axis, index, block, cut):
            self.next, self.prev = turn(axis, index, 1), turn(axis, index, 3)
            self.index, self.block, self.cut = index, block, cut

        def start(self):
            ref = self.block(self.index)
            self.right = send_to(ref, self.next)
            self.left = send_to(ref, self.prev)

        def second(self):
            self.right.wait_recv()
            self.far = [send_to(self.cut(lax.rem(self.index + 3, 4), 0), self.next)]
            self.left.wait_recv()
            self.far.append(send_to(self.cut(lax.rem(self.index + 1, 4), 1), self.prev))

        def finish(self):
            for copy in self.far:
                copy.wait_recv()

    def rings(phase, block, cut):
        return [
            Ring(*axes[p][phase], functools.partial(block, p), functools.partial(cut, p)) for p in range(2)
        ]

    def b_small(p, j):
        return gram_b.at[group, gram_rows(p, axes[p][0][1]), at(j, 256)]

    def b_small_cut(p, j, h):
        return gram_b.at[at(core * 2 + h, 2), gram_rows(p, axes[p][0][1]), at(j, 256)]

    def b_large(p, j):
        return gram_b.at[group, gram_rows(p, j), :]

    def b_large_cut(p, j, h):
        return gram_b.at[at(core * 2 + h, 2), gram_rows(p, j), :]

    def g_rows(p, j):
        return spot(axes[p][0][1] * 64 + j * 16, 16, 16)

    def g_small(p, j):
        return panels.at[core, :, g_rows(p, j), at(p, 640)]

    def g_small_cut(p, j, h):
        return panels.at[core, at(h, 2), g_rows(p, j), at(p, 640)]

    def g_large(p, j):
        return panels.at[core, :, at(j, 64), at(p, 640)]

    def g_large_cut(p, j, h):
        return panels.at[core, at(h, 2), at(j, 64), at(p, 640)]

    small_b, large_b = rings(1, b_small, b_small_cut), rings(0, b_large, b_large_cut)
    small, large = rings(1, g_small, g_small_cut), rings(0, g_large, g_large_cut)
    lines[0][1]()
    lines[0][2]()
    part_b[...] = turned(xb[:, spot(core * 512 + place * 128, 128, 128)], xb[...]).astype(BF)
    one_b = scatter_one(source_b, [near_b.at[p] for p in range(2)])
    lines[1][1]()
    two_b = []
    for p in range(2):
        kept_b[p] = total(part_b[spot(p * 64 + axes[p][0][1] * 16, 16, 16), :], near_b.at[p], one_b[p])
        two_b.append(exchange(lambda t, p=p: kept_b.at[p, :, at(t, 256)], near2_b.at[p], *axes[p][1]))
    lines[2][1]()
    swaps_b = []
    for p in range(2):
        i1, i2 = axes[p][0][1], axes[p][1][1]
        gram_b[core * 4 + place, gram_rows(p, i1), at(i2, 256)] = total(
            kept_b[p, :, at(i2, 256)], near2_b.at[p], two_b[p]
        )
        ref = gram_b.at[core * 4 + place, gram_rows(p, i1), at(i2, 256)]
        swaps_b.append([send_to(ref, {"tp": x}) for x in (across, ahead, behind)])
    for source, target in ((speed_b, branch_m), (speed.at[0], gate_m), (speed.at[1], up_m)):
        store(source, target)
    ones = [panel(0), panel(1)]

    def scatter_two(i):
        pair = []
        for p in range(2):
            index = axes[p][0][1]
            kept[i, p] = total(part[i, at(index, 64), at(p, 640)], near.at[i, p], ones[i][p])
            pair.append(exchange(lambda t, p=p: kept.at[i, p, at(t, 16), :], near2.at[i, p], *axes[p][1]))
        return pair

    twos = [scatter_two(0)]
    for p in range(2):
        for copy in swaps_b[p]:
            copy.wait_recv()
        small_b[p].start()
    twos.append(scatter_two(1))
    for ring in small_b:
        ring.second()
    swaps = []
    for p in range(2):
        i2 = axes[p][1][1]
        for i in range(2):
            piece[i, p] = total(kept[i, p, at(i2, 16), :], near2.at[i, p], twos[i][p])
        target = panels.at[core, place, g_rows(p, i2), at(p, 640)]
        panels[core, place, g_rows(p, i2), at(p, 640)] = piece[kind, p]
        swaps.append(send_to(target, {"tp": across}))
        for x in (ahead, behind):
            copy = remote(piece.at[1 - kind, p], target, {"tp": x})
            copy.start()
            swaps.append(copy)
    for ring in small_b:
        ring.finish()
    for ring in large_b:
        ring.start()
    for copy in swaps:
        copy.wait_recv()
    for ring in small:
        ring.start()
    forward_b, forward = [], []
    for p, ring in enumerate(large_b):
        ring.second()
        forward_b += [send_to(b_large(p, lax.rem(ring.index + k, 4)), partner) for k in (0, 3, 1)]
    for ring in small:
        ring.second()
    for p, ring in enumerate(large_b):
        ring.finish()
        forward_b.append(send_to(b_large(p, lax.rem(ring.index + 2, 4)), partner))
    for ring in small:
        ring.finish()
    for ring in large:
        ring.start()
    for copy in forward_b:
        copy.wait_recv()

    def coefficients(squares, diagonal):
        second = jnp.full((1, 1), squares)
        first = jnp.full((1, 1), diagonal)
        ratio = SAFETY * (second + 1.0) / (first + 1.0)
        return 1.0 / ratio, lax.rsqrt(ratio)

    def squares_b(i, sums):
        value = gram_b[i].astype(jnp.float32)
        diagonal = gram_b[i, :, at(i, 128)].astype(jnp.float32)
        return (
            sums[0] + jnp.sum((value * value).reshape(16, 8, NB), axis=0),
            sums[1] + jnp.where(same, diagonal, 0.0),
        )

    sums = lax.fori_loop(0, 8, squares_b, (jnp.zeros((8, NB), jnp.float32), jnp.zeros((128, 128), jnp.float32)))
    alpha_b, scale_b = coefficients(jnp.sum(sums[0]), jnp.sum(sums[1]))

    def square_b(left, low, high):
        def step(r, _):
            where = at(r, 512)
            m_b[where, :] = (low * left[where, :].astype(jnp.float32) + high * dot(left[where, :], left[...])).astype(BF)
            return 0

        lax.fori_loop(0, 2, step, 0)

    def times_b(left, out, factor):
        def step(r, _):
            where = at(r, 512)
            value = factor * (COEF_ONE * left[where, :].astype(jnp.float32) + dot(left[where, :], m_b[...]))
            out[where, :] = value.astype(BF)
            return 0

        lax.fori_loop(0, 2, step, 0)

    def rows_of(left, factor):
        return (factor * (COEF_ONE * left.astype(jnp.float32) + dot(left, m_b[...]))).astype(BF)

    for i in range(8):
        g_b[at(i, 128), :] = gram_b[i]
    square_b(g_b, COEF_THREE * alpha_b, COEF_FIVE * alpha_b * alpha_b)
    times_b(g_b, t_b, alpha_b)
    line = rows_of(xb[at(core, rows_b), :], scale_b)
    times_b(t_b, g_b, 1.0)
    square_b(g_b, COEF_THREE, COEF_FIVE)
    for p, ring in enumerate(large):
        ring.second()
        forward += [send_to(g_large(p, lax.rem(ring.index + k, 4)), partner) for k in (0, 3, 1)]
    times_b(g_b, t_b, 1.0)
    line = rows_of(line, 1.0)
    times_b(t_b, g_b, 1.0)
    for p, ring in enumerate(large):
        ring.finish()
        forward.append(send_to(g_large(p, lax.rem(ring.index + 2, 4)), partner))
    square_b(g_b, COEF_THREE, COEF_FIVE)
    t_b[0:rows_b, :] = line
    for p in range(2):
        cols = spot(p * 512 + place * 128, 128, 128)
        last_b = COEF_ONE * t_b[0:rows_b, cols].astype(jnp.float32) + dot(line, m_b[:, cols])
        results_b[:, at(p, 128)] = last_b.astype(BF)
    store(results_b, branch_out)
    for copy in forward:
        copy.wait_recv()

    def assemble(r, sums):
        value = panels[lax.div(r, 4), lax.rem(r, 4)]
        squares, diagonal = sums
        for d in range(5):
            block = value[:, d * 256 : d * 256 + 256]
            column = at(lax.rem(r + d, 8), 256)
            a[at(r, 256), column] = block
            if 0 < d < 4:
                a[column, at(r, 256)] = block.T
            wide = block.astype(jnp.float32)
            weight = 2.0 if 0 < d < 4 else 1.0
            squares = squares + weight * jnp.sum((wide * wide).reshape(32, 8, 256), axis=0)
        for k in range(2):
            corner = value[k * 128 : k * 128 + 128, k * 128 : k * 128 + 128].astype(jnp.float32)
            diagonal = diagonal + jnp.where(same, corner, 0.0)
        return squares, diagonal

    sums = lax.fori_loop(0, 8, assemble, (jnp.zeros((8, 256), jnp.float32), jnp.zeros((128, 128), jnp.float32)))
    alpha, scale = coefficients(jnp.sum(sums[0]), jnp.sum(sums[1]))

    x0 = xs.at[kind]

    def swap(buf, k, r, half):
        ref = buf.at[at(r, CHUNK), at(half, HALF)]
        return pltpu.make_async_remote_copy(
            src_ref=ref, dst_ref=ref, send_sem=send.at[k, r], recv_sem=recv.at[k, r], device_id=partner, device_id_type=MESH
        )

    def square(left, k, low, high):
        def step(r, _):
            if k is not None:
                swap(left, k, r, core).wait_send()
                swap(left, k, r, other).wait_recv()
            s = dot(left[at(r, CHUNK), :], left[:, mine])
            m[at(r, CHUNK), :] = (low * left[at(r, CHUNK), mine].astype(jnp.float32) + high * s).astype(BF)
            return 0

        lax.fori_loop(0, STEPS, step, 0)

    def times(left, k, out, k_out, factor):
        def step(r, _):
            if k is not None:
                swap(left, k, r, core).wait_send()
                swap(left, k, r, other).wait_recv()
            p = dot(left[at(r, CHUNK), :], m[...])
            p = COEF_ONE * left[at(r, CHUNK), mine].astype(jnp.float32) + p
            if factor is not None:
                p = factor * p
            out[at(r, CHUNK), mine] = p.astype(BF)
            swap(out, k_out, r, core).start()
            return 0

        lax.fori_loop(0, STEPS, step, 0)

    square(a, None, COEF_THREE * alpha, COEF_FIVE * alpha * alpha)
    times(a, None, b, 0, alpha)
    x1[:, mine] = (scale * (COEF_ONE * x0[:, mine].astype(jnp.float32) + dot(x0[...], m[...]))).astype(BF)
    turn_one = send_to(x1.at[:, mine], partner)
    times(b, 0, c, 1, None)
    square(c, 1, COEF_THREE, COEF_FIVE)
    times(c, None, b, 2, None)
    turn_one.wait_recv()
    x2[:, mine] = (COEF_ONE * x1[:, mine].astype(jnp.float32) + dot(x1[...], m[...])).astype(BF)
    turn_two = send_to(x2.at[:, mine], partner)
    times(b, 2, a, 3, None)
    square(a, 3, COEF_THREE, COEF_FIVE)
    turn_two.wait_recv()

    def last(where, block):
        cols = at(block, 256)
        close = spot(core * HALF + block * 256, 256, 256)
        return (COEF_ONE * x2[where, close].astype(jnp.float32) + dot(x2[where, :], m[:, cols])).astype(BF)

    final[2] = last(pl.ds(0, rows), ahead)
    to_ahead = pltpu.make_async_remote_copy(
        src_ref=final.at[2], dst_ref=final.at[4 + core], send_sem=sems.at[COPIES], recv_sem=recvs.at[COPIES + core],
        device_id={"tp": ahead, "rep": 0}, device_id_type=MESH,
    )
    to_ahead.start()
    final[3] = last(pl.ds(rows, rows), behind)
    to_behind = pltpu.make_async_remote_copy(
        src_ref=final.at[3], dst_ref=final.at[4 + core], send_sem=sems.at[COPIES + 1], recv_sem=recvs.at[COPIES + core],
        device_id={"tp": behind, "rep": 1}, device_id_type=MESH,
    )
    to_behind.start()
    final[6] = last(other_rows, place)
    to_partner = remote(final.at[6], final.at[core], partner)
    to_partner.start()
    final[core] = last(own_rows, place)
    to_partner.wait_recv()
    for i in range(2):
        pltpu.make_async_remote_copy(
            src_ref=final.at[2], dst_ref=final.at[4 + i], send_sem=sems.at[COPIES], recv_sem=recvs.at[COPIES + i],
            device_id=partner, device_id_type=MESH,
        ).wait_recv()
    for i in range(2):
        cols = pl.ds(i * 256, 256)
        results[kind, :, cols] = final[i]
        results[1 - kind, :, cols] = final[4 + i]
    store(results.at[0], gate_out)
    store(results.at[1], up_out)
    to_ahead.wait_send()
    to_behind.wait_send()
    for copy in used:
        copy.wait_send()
    for copy in stores:
        copy.wait()


def finish_kernel(*refs):
    ins, outs, stage, fresh, in_sem, out_sem = refs[:9], refs[9:15], refs[15:24], refs[24:27], refs[27], refs[28]
    loads = [pltpu.make_async_copy(ins[i], stage[i], in_sem.at[i]) for i in range(9)]
    for i in (3, 6, 4, 7, 5, 8, 0, 1, 2):
        loads[i].start()
    stores = []

    def store(source, target):
        copy = pltpu.make_async_copy(source, target, out_sem.at[len(stores)])
        copy.start()
        stores.append(copy)

    for i, height in enumerate((FF, FF, D)):
        loads[3 + i].wait()
        loads[6 + i].wait()
        fresh[i][...] = SHRINK * stage[6 + i][...] - RATE * math.sqrt(height) * stage[3 + i][...].astype(jnp.float32)
        store(fresh[i], outs[2 * i + 1])
    for i in range(3):
        loads[i].wait()
        store(stage[i], outs[2 * i])
    for copy in stores:
        copy.wait()


def local(*args):
    velocities = (args[1], args[4], args[7])
    shapes = [velocity.shape for velocity in velocities]
    (rows, width), (rows_b, width_b) = shapes[0], shapes[2]
    anywhere = pl.BlockSpec(memory_space=pl.ANY)
    dma = pltpu.SemaphoreType.DMA

    def buf(*shape):
        return pltpu.VMEM(shape, BF)

    def full(*shape):
        return pltpu.VMEM(shape, jnp.float32)

    outs = [jax.ShapeDtypeStruct(shape, kind) for kind in (jnp.float32, BF) for shape in shapes]
    middle = pl.pallas_call(
        kernel,
        out_shape=outs,
        in_specs=[anywhere] * 6,
        out_specs=[anywhere] * 6,
        scratch_shapes=[
            full(2, 2, rows, width), full(2, rows_b, width_b), full(2, rows, width), full(rows_b, width_b),
            buf(2, rows, width), buf(rows_b, width_b), dma((9,)), dma((6,)),
            buf(N, N), buf(N, N), buf(N, N), buf(N, HALF),
            buf(2, 2 * rows, N), buf(2 * rows_b, NB), buf(2 * rows, N), buf(2 * rows, N), buf(7, rows, 256),
            buf(2, rows, width), buf(2, rows, width), buf(rows_b, width_b), buf(rows_b, width_b),
            buf(2, 256, 1280), buf(2, 2, 3, 64, 640), buf(2, 2, 64, 640), buf(2, 2, 3, 16, 640), buf(2, 2, 16, 640),
            buf(2, 4, 256, 1280),
            buf(128, NB), buf(2, 3, 16, NB), buf(2, 16, NB), buf(2, 3, 16, 256), buf(8, 128, NB),
            buf(NB, NB), buf(NB, NB), buf(NB, NB),
            dma((COPIES + 2,)), dma((COPIES + 2,)), dma((4, STEPS)), dma((4, STEPS)),
        ],
        compiler_params=pltpu.CompilerParams(collective_id=0, has_side_effects=True, vmem_limit_bytes=62 * 1024 * 1024),
    )(args[0], args[3], args[6], args[1], args[4], args[7])
    results = [jax.ShapeDtypeStruct(shape, jnp.float32) for shape in shapes for _ in range(2)]
    stage = [full(*shape) for shape in shapes] + [buf(*shape) for shape in shapes] + [full(*shape) for shape in shapes] * 2
    return pl.pallas_call(
        finish_kernel,
        out_shape=results,
        in_specs=[anywhere] * 9,
        out_specs=[anywhere] * 6,
        scratch_shapes=stage + [dma((9,)), dma((6,))],
    )(*middle, args[2], args[5], args[8])


def solution(mesh):
    torus = Mesh(
        mesh.devices.reshape(4, 4, mesh.shape["tp"], mesh.shape["rep"]),
        ("fs_0", "fs_1", "tp", "rep"),
    )
    grads, plain = P("rep", FS, "tp"), P(FS_REP, "tp")
    return jax.shard_map(
        local,
        mesh=torus,
        in_specs=(grads, plain, plain) * 3,
        out_specs=(plain,) * 6,
        check_vma=False,
    )
```

```python
import functools
import math

import jax
import jax.numpy as jnp
from jax import lax
from jax.experimental import pallas as pl
from jax.experimental.pallas import tpu as pltpu
from jax.sharding import Mesh
from jax.sharding import PartitionSpec as P

D = 2048
FF = 5632
FS_REP = ("fs_0", "fs_1", "rep")
FS = ("fs_0", "fs_1")

MOMENT = 0.95
COEF_ONE = 3.4445
COEF_THREE = -4.775
COEF_FIVE = 2.0315
SAFETY = 2.0
RATE = 0.5
SHRINK = 0.95
BF = jnp.bfloat16


def dot(a, b):
    return jnp.dot(a, b, preferred_element_type=jnp.float32)


N = 2048
HALF = 1024
BLOCK = 512
NB = 1024
COPIES = 160
MESH = pl.DeviceIdType.MESH


def at(index, size):
    return pl.ds(index * size if isinstance(index, int) else pl.multiple_of(index * size, size), size)


def spot(offset, size, unit):
    return pl.ds(pl.multiple_of(offset, unit), size)


def turned(a, b):
    return lax.dot_general(a, b, (((0,), (0,)), ((), ())), preferred_element_type=jnp.float32)


def kernel(
    gate_g, up_g, branch_g, gate_v, up_v, branch_v,
    gate_m, up_m, branch_m, gate_out, up_out, branch_out,
    grads, grads_b, speed, speed_b, results, results_b, in_sem, out_sem,
    a, b, c, m, xs, xb, x1, x2, final,
    give, take, give_b, take_b,
    part, near, kept, near2, piece, panels,
    part_b, near_b, kept_b, near2_b, gram_b, m_b, t_b, g_b,
    stage, sems, recvs, send, recv,
):
    core = lax.axis_index("rep")
    place = lax.axis_index("tp")
    iy = lax.axis_index("fs_1")
    iz = lax.axis_index("fs_0")
    other = 1 - core
    kind = lax.rem(place, 2)
    ahead = lax.rem(place + 1, 4)
    behind = lax.rem(place + 3, 4)
    across = lax.rem(place + 2, 4)
    rows = gate_v.shape[0]
    rows_b = branch_v.shape[0]
    loads = []

    def load(source, target):
        copy = pltpu.make_async_copy(source, target, in_sem.at[len(loads)])
        copy.start()
        loads.append(copy)

    load(branch_g.at[0, at(other, rows_b)], grads_b.at[1])
    load(gate_g.at[0, at(other, rows)], grads.at[0, 1])
    load(up_g.at[0, at(other, rows)], grads.at[1, 1])
    load(branch_g.at[0, at(core, rows_b)], grads_b.at[0])
    load(branch_v, speed_b)
    load(gate_g.at[0, at(core, rows)], grads.at[0, 0])
    load(gate_v, speed.at[0])
    load(up_g.at[0, at(core, rows)], grads.at[1, 0])
    load(up_v, speed.at[1])
    mine = at(core, HALF)
    partner = {"rep": other}
    used = []

    def turn(axis, index, step):
        return {axis: lax.rem(index + step, 4)}

    def remote(src, dst, to):
        k = len(used)
        copy = pltpu.make_async_remote_copy(
            src_ref=src, dst_ref=dst, send_sem=sems.at[k], recv_sem=recvs.at[k], device_id=to, device_id_type=MESH
        )
        used.append(copy)
        return copy

    def send_to(ref, to):
        copy = remote(ref, ref, to)
        copy.start()
        return copy

    barrier = pltpu.get_barrier_semaphore()
    peers = [partner, {"tp": across}]
    peers += [{"tp": x, "rep": r} for x in (ahead, behind) for r in range(2)]
    peers += [turn(axis, index, step) for axis, index in (("fs_1", iy), ("fs_0", iz)) for step in (1, 2, 3)]
    for to in peers:
        pl.semaphore_signal(barrier, inc=1, device_id=to, device_id_type=MESH)

    own_rows, other_rows = at(core, rows), at(other, rows)
    loads[0].wait()
    give_b[...] = grads_b[1].astype(BF)
    for i in range(2):
        loads[1 + i].wait()
        give[i] = grads[i, 1].astype(BF)
    pl.semaphore_wait(barrier, len(peers))
    first_copies = [remote(give_b, take_b, partner)]
    first_copies += [remote(give.at[i], take.at[i], partner) for i in range(2)]
    for copy in first_copies:
        copy.start()
    same = lax.broadcasted_iota(jnp.int32, (128, 128), 0) == lax.broadcasted_iota(jnp.int32, (128, 128), 1)

    def columns(ref, lines, height, width):
        def block(x, part):
            return ref.at[at(core, height), spot(part * 4 * width + x * width, width, width)]

        state = {}

        def start():
            state["right"] = [send_to(block(place, p), {"tp": ahead}) for p in range(2)]
            state["left"] = [send_to(block(place, p), {"tp": behind}) for p in range(2)]
            state["own"] = [send_to(block(place, p), partner) for p in range(2)]

        def second():
            state["right"][0].wait_recv()
            far = [send_to(block(behind, 0), {"tp": ahead})]
            state["left"][1].wait_recv()
            far.append(send_to(block(ahead, 1), {"tp": behind}))
            state["far"] = far
            state["own"].append(send_to(block(behind, 0), partner))
            state["own"].append(send_to(block(ahead, 1), partner))
            state["right"][1].wait_recv()
            state["own"].append(send_to(block(behind, 1), partner))
            state["left"][0].wait_recv()
            state["own"].append(send_to(block(ahead, 0), partner))

        def finish():
            for p in range(2):
                state["far"][p].wait_recv()
                state["own"].append(send_to(block(across, p), partner))
            for copy in state["own"]:
                copy.wait_recv()

        return start, second, finish

    gate_x, up_x = xs.at[0], xs.at[1]
    lines = [columns(xb, None, rows_b, 128), columns(gate_x, None, rows, 256), columns(up_x, None, rows, 256)]
    first_copies[0].wait_recv()
    loads[3].wait()
    loads[4].wait()
    moment = MOMENT * speed_b[...] + (grads_b[0] + take_b[...].astype(jnp.float32))
    speed_b[...] = moment
    for p in range(2):
        xb[at(core, rows_b), spot(p * 512 + place * 128, 128, 128)] = moment[:, p * 128 : p * 128 + 128].astype(BF)
    lines[0][0]()
    for i in range(2):
        first_copies[1 + i].wait_recv()
        loads[5 + 2 * i].wait()
        loads[6 + 2 * i].wait()
        moment = MOMENT * speed[i] + (grads[i, 0] + take[i].astype(jnp.float32))
        speed[i] = moment
        for p in range(2):
            xs[i, own_rows, spot(p * HALF + place * 256, 256, 256)] = moment[:, p * 256 : p * 256 + 256].astype(BF)
        lines[1 + i][0]()
    stores = []

    def store(source, target):
        copy = pltpu.make_async_copy(source, target, out_sem.at[len(stores)])
        copy.start()
        stores.append(copy)

    axes = ((("fs_1", iy), ("fs_0", iz)), (("fs_0", iz), ("fs_1", iy)))

    def exchange(source, landing, axis, index):
        copies = []
        for step in (2, 1, 3):
            to = lax.rem(index + step, 4)
            copies.append(remote(source(to), landing.at[step - 1], {axis: to}))
            copies[-1].start()
        return copies

    def total(own, landing, copies):
        for copy in copies:
            copy.wait_recv()
        value = own.astype(jnp.float32)
        for k in range(3):
            value = value + landing[k].astype(jnp.float32)
        return value.astype(BF)

    def scatter_one(source, landings):
        return [
            exchange(functools.partial(source, p), landings[p], *axes[p][0]) for p in range(2)
        ]

    def source_of(i):
        return lambda p, t: part.at[i, at(t, 64), at(p, 640)]

    def source_b(p, t):
        return part_b.at[spot(p * 64 + t * 16, 16, 16), :]

    def panel(i):
        lines[1 + i][2]()
        own = xs[i, :, spot(core * HALF + place * 256, 256, 256)]
        for d in range(5):
            block = lax.rem(core * 4 + place + d, 8)
            part[i, :, at(d, 256)] = turned(own, xs[i, :, at(block, 256)]).astype(BF)
        return scatter_one(source_of(i), [near.at[i, p] for p in range(2)])

    def gram_rows(p, i1):
        return spot(p * 64 + i1 * 16, 16, 16)

    group = at(core, 4)

    class Ring:
        def __init__(self, axis, index, block, cut):
            self.next, self.prev = turn(axis, index, 1), turn(axis, index, 3)
            self.index, self.block, self.cut = index, block, cut

        def start(self):
            ref = self.block(self.index)
            self.right = send_to(ref, self.next)
            self.left = send_to(ref, self.prev)

        def second(self):
            self.right.wait_recv()
            self.far = [send_to(self.cut(lax.rem(self.index + 3, 4), 0), self.next)]
            self.left.wait_recv()
            self.far.append(send_to(self.cut(lax.rem(self.index + 1, 4), 1), self.prev))

        def finish(self):
            for copy in self.far:
                copy.wait_recv()

    def rings(phase, block, cut):
        return [
            Ring(*axes[p][phase], functools.partial(block, p), functools.partial(cut, p)) for p in range(2)
        ]

    def b_small(p, j):
        return gram_b.at[group, gram_rows(p, axes[p][0][1]), at(j, 256)]

    def b_small_cut(p, j, h):
        return gram_b.at[at(core * 2 + h, 2), gram_rows(p, axes[p][0][1]), at(j, 256)]

    def b_large(p, j):
        return gram_b.at[group, gram_rows(p, j), :]

    def b_large_cut(p, j, h):
        return gram_b.at[at(core * 2 + h, 2), gram_rows(p, j), :]

    def g_rows(p, j):
        return spot(axes[p][0][1] * 64 + j * 16, 16, 16)

    def g_small(p, j):
        return panels.at[core, :, g_rows(p, j), at(p, 640)]

    def g_small_cut(p, j, h):
        return panels.at[core, at(h, 2), g_rows(p, j), at(p, 640)]

    def g_large(p, j):
        return panels.at[core, :, at(j, 64), at(p, 640)]

    def g_large_cut(p, j, h):
        return panels.at[core, at(h, 2), at(j, 64), at(p, 640)]

    small_b, large_b = rings(1, b_small, b_small_cut), rings(0, b_large, b_large_cut)
    small, large = rings(1, g_small, g_small_cut), rings(0, g_large, g_large_cut)
    lines[0][1]()
    lines[0][2]()
    part_b[...] = turned(xb[:, spot(core * 512 + place * 128, 128, 128)], xb[...]).astype(BF)
    one_b = scatter_one(source_b, [near_b.at[p] for p in range(2)])
    lines[1][1]()
    two_b = []
    for p in range(2):
        kept_b[p] = total(part_b[spot(p * 64 + axes[p][0][1] * 16, 16, 16), :], near_b.at[p], one_b[p])
        two_b.append(exchange(lambda t, p=p: kept_b.at[p, :, at(t, 256)], near2_b.at[p], *axes[p][1]))
    lines[2][1]()
    swaps_b = []
    for p in range(2):
        i1, i2 = axes[p][0][1], axes[p][1][1]
        gram_b[core * 4 + place, gram_rows(p, i1), at(i2, 256)] = total(
            kept_b[p, :, at(i2, 256)], near2_b.at[p], two_b[p]
        )
        ref = gram_b.at[core * 4 + place, gram_rows(p, i1), at(i2, 256)]
        swaps_b.append([send_to(ref, {"tp": x}) for x in (across, ahead, behind)])
    for source, target in ((speed_b, branch_m), (speed.at[0], gate_m), (speed.at[1], up_m)):
        store(source, target)
    ones = [panel(0), panel(1)]

    def scatter_two(i):
        pair = []
        for p in range(2):
            index = axes[p][0][1]
            kept[i, p] = total(part[i, at(index, 64), at(p, 640)], near.at[i, p], ones[i][p])
            pair.append(exchange(lambda t, p=p: kept.at[i, p, at(t, 16), :], near2.at[i, p], *axes[p][1]))
        return pair

    twos = [scatter_two(0)]
    for p in range(2):
        for copy in swaps_b[p]:
            copy.wait_recv()
        small_b[p].start()
    twos.append(scatter_two(1))
    for ring in small_b:
        ring.second()
    swaps = []
    for p in range(2):
        i2 = axes[p][1][1]
        for i in range(2):
            piece[i, p] = total(kept[i, p, at(i2, 16), :], near2.at[i, p], twos[i][p])
        target = panels.at[core, place, g_rows(p, i2), at(p, 640)]
        panels[core, place, g_rows(p, i2), at(p, 640)] = piece[kind, p]
        swaps.append(send_to(target, {"tp": across}))
        for x in (ahead, behind):
            copy = remote(piece.at[1 - kind, p], target, {"tp": x})
            copy.start()
            swaps.append(copy)
    for ring in small_b:
        ring.finish()
    for ring in large_b:
        ring.start()
    for copy in swaps:
        copy.wait_recv()
    for ring in small:
        ring.start()
    forward_b, forward = [], []
    for p, ring in enumerate(large_b):
        ring.second()
        forward_b += [send_to(b_large(p, lax.rem(ring.index + k, 4)), partner) for k in (0, 3, 1)]
    for ring in small:
        ring.second()
    for p, ring in enumerate(large_b):
        ring.finish()
        forward_b.append(send_to(b_large(p, lax.rem(ring.index + 2, 4)), partner))
    for ring in small:
        ring.finish()
    for ring in large:
        ring.start()
    for copy in forward_b:
        copy.wait_recv()

    def coefficients(squares, diagonal):
        second = jnp.full((1, 1), squares)
        first = jnp.full((1, 1), diagonal)
        ratio = SAFETY * (second + 1.0) / (first + 1.0)
        return 1.0 / ratio, lax.rsqrt(ratio)

    def squares_b(i, sums):
        value = gram_b[i].astype(jnp.float32)
        diagonal = gram_b[i, :, at(i, 128)].astype(jnp.float32)
        return (
            sums[0] + jnp.sum((value * value).reshape(16, 8, NB), axis=0),
            sums[1] + jnp.where(same, diagonal, 0.0),
        )

    sums = lax.fori_loop(0, 8, squares_b, (jnp.zeros((8, NB), jnp.float32), jnp.zeros((128, 128), jnp.float32)))
    alpha_b, scale_b = coefficients(jnp.sum(sums[0]), jnp.sum(sums[1]))

    def square_b(left, low, high):
        def step(r, _):
            where = at(r, 512)
            m_b[where, :] = (low * left[where, :].astype(jnp.float32) + high * dot(left[where, :], left[...])).astype(BF)
            return 0

        lax.fori_loop(0, 2, step, 0)

    def times_b(left, out, factor):
        def step(r, _):
            where = at(r, 512)
            value = factor * (COEF_ONE * left[where, :].astype(jnp.float32) + dot(left[where, :], m_b[...]))
            out[where, :] = value.astype(BF)
            return 0

        lax.fori_loop(0, 2, step, 0)

    def rows_of(left, factor):
        return (factor * (COEF_ONE * left.astype(jnp.float32) + dot(left, m_b[...]))).astype(BF)

    for i in range(8):
        g_b[at(i, 128), :] = gram_b[i]
    square_b(g_b, COEF_THREE * alpha_b, COEF_FIVE * alpha_b * alpha_b)
    times_b(g_b, t_b, alpha_b)
    line = rows_of(xb[at(core, rows_b), :], scale_b)
    times_b(t_b, g_b, 1.0)
    square_b(g_b, COEF_THREE, COEF_FIVE)
    for p, ring in enumerate(large):
        ring.second()
        forward += [send_to(g_large(p, lax.rem(ring.index + k, 4)), partner) for k in (0, 3, 1)]
    times_b(g_b, t_b, 1.0)
    line = rows_of(line, 1.0)
    times_b(t_b, g_b, 1.0)
    for p, ring in enumerate(large):
        ring.finish()
        forward.append(send_to(g_large(p, lax.rem(ring.index + 2, 4)), partner))
    square_b(g_b, COEF_THREE, COEF_FIVE)
    t_b[0:rows_b, :] = line
    for p in range(2):
        cols = spot(p * 512 + place * 128, 128, 128)
        last_b = COEF_ONE * t_b[0:rows_b, cols].astype(jnp.float32) + dot(line, m_b[:, cols])
        results_b[:, at(p, 128)] = last_b.astype(BF)
    store(results_b, branch_out)
    for copy in forward:
        copy.wait_recv()

    def assemble(r, sums):
        value = panels[lax.div(r, 4), lax.rem(r, 4)]
        squares, diagonal = sums
        for d in range(5):
            block = value[:, d * 256 : d * 256 + 256]
            column = at(lax.rem(r + d, 8), 256)
            a[at(r, 256), column] = block
            if 0 < d < 4:
                a[column, at(r, 256)] = block.T
            wide = block.astype(jnp.float32)
            weight = 2.0 if 0 < d < 4 else 1.0
            squares = squares + weight * jnp.sum((wide * wide).reshape(32, 8, 256), axis=0)
        for k in range(2):
            corner = value[k * 128 : k * 128 + 128, k * 128 : k * 128 + 128].astype(jnp.float32)
            diagonal = diagonal + jnp.where(same, corner, 0.0)
        return squares, diagonal

    sums = lax.fori_loop(0, 8, assemble, (jnp.zeros((8, 256), jnp.float32), jnp.zeros((128, 128), jnp.float32)))
    alpha, scale = coefficients(jnp.sum(sums[0]), jnp.sum(sums[1]))

    x0 = xs.at[kind]

    def h(q):
        return at(2 * core + q, BLOCK)

    def o(q):
        return at(2 * other + q, BLOCK)

    def flip(q):
        return lax.rem(q + core, 2)

    def flop(q):
        return lax.rem(q + other, 2)

    def pair(ref, target, k, q):
        return pltpu.make_async_remote_copy(
            src_ref=ref, dst_ref=target, send_sem=send.at[k, q], recv_sem=recv.at[k, q], device_id=partner, device_id_type=MESH
        )

    def cross_out(buf, k, q):
        ref = buf.at[o(q), h(flip(q))]
        return pair(ref, ref, k, q)

    def cross_in(buf, k, q):
        ref = buf.at[h(q), o(flop(q))]
        return pair(ref, ref, k, q)

    def square_out(buf, k, q, side):
        first = at(2 * side, BLOCK)
        second = at(2 * side + 1, BLOCK)
        ref = (buf.at[first, at(side, HALF)], buf.at[second, first], buf.at[second, second])[q]
        return pair(ref, ref, k, 2 + q)

    def stage_out(k, q):
        return pair(m.at[o(q), at(flip(q), BLOCK)], stage.at[q], 4 + k, q)

    def product(left, k, right, emit, after_head, after_cross, after_all):
        if k is not None:
            def receive(q, _):
                cross_out(left, k, q).wait_send()
                cross_in(left, k, q).wait_recv()
                left[o(flop(q)), h(q)] = left[h(q), o(flop(q))].T
                return 0

            lax.fori_loop(0, 2, receive, 0)

        def head(q, _):
            emit(h(q), 0, dot(left[h(q), :], right(0)))
            return 0

        lax.fori_loop(0, 2, head, 0)
        after_head()
        if k is not None:
            for q in range(3):
                square_out(left, k, q, core).wait_send()
                square_out(left, k, q, other).wait_recv()

        def cross(q, _):
            j = flip(q)
            emit(o(q), j, dot(left[o(q), :], right(j)))
            after_cross(q)
            return 0

        lax.fori_loop(0, 2, cross, 0)
        emit(h(1), 1, dot(left[h(1), :], right(1)))
        after_all()

    def square(left, k, k_out, low, high):
        def emit(where, j, value):
            value = low * left[where, h(j)].astype(jnp.float32) + high * value
            m[where, at(j, BLOCK)] = value.astype(BF)

        def after_head():
            m[h(0), at(1, BLOCK)] = m[h(1), at(0, BLOCK)].T

        def after_cross(q):
            stage_out(k_out, q).start()

        def right(j):
            return left[:, h(j)]

        product(left, k, right, emit, after_head, after_cross, lambda: None)

        def receive(q, _):
            copy = stage_out(k_out, q)
            copy.wait_send()
            copy.wait_recv()
            m[o(flop(q)), at(q, BLOCK)] = stage[q].T
            return 0

        lax.fori_loop(0, 2, receive, 0)

    def times(left, k, out, k_out, factor):
        def emit(where, j, value):
            value = COEF_ONE * left[where, h(j)].astype(jnp.float32) + value
            if factor is not None:
                value = factor * value
            out[where, h(j)] = value.astype(BF)

        def after_head():
            out[h(0), h(1)] = out[h(1), h(0)].T
            square_out(out, k_out, 0, core).start()
            square_out(out, k_out, 1, core).start()

        def after_cross(q):
            cross_out(out, k_out, q).start()
            out[h(flip(q)), o(q)] = out[o(q), h(flip(q))].T

        def after_all():
            square_out(out, k_out, 2, core).start()

        def right(j):
            return m[:, at(j, BLOCK)]

        product(left, k, right, emit, after_head, after_cross, after_all)

    square(a, None, 0, COEF_THREE * alpha, COEF_FIVE * alpha * alpha)
    times(a, None, b, 0, alpha)
    x1[:, mine] = (scale * (COEF_ONE * x0[:, mine].astype(jnp.float32) + dot(x0[...], m[...]))).astype(BF)
    turn_one = send_to(x1.at[:, mine], partner)
    times(b, 0, c, 1, None)
    square(c, 1, 1, COEF_THREE, COEF_FIVE)
    times(c, None, b, 2, None)
    turn_one.wait_recv()
    x2[:, mine] = (COEF_ONE * x1[:, mine].astype(jnp.float32) + dot(x1[...], m[...])).astype(BF)
    turn_two = send_to(x2.at[:, mine], partner)
    times(b, 2, a, 3, None)
    square(a, 3, 2, COEF_THREE, COEF_FIVE)
    turn_two.wait_recv()

    def last(where, block):
        cols = at(block, 256)
        close = spot(core * HALF + block * 256, 256, 256)
        return (COEF_ONE * x2[where, close].astype(jnp.float32) + dot(x2[where, :], m[:, cols])).astype(BF)

    final[2] = last(pl.ds(0, rows), ahead)
    to_ahead = pltpu.make_async_remote_copy(
        src_ref=final.at[2], dst_ref=final.at[4 + core], send_sem=sems.at[COPIES], recv_sem=recvs.at[COPIES + core],
        device_id={"tp": ahead, "rep": 0}, device_id_type=MESH,
    )
    to_ahead.start()
    final[3] = last(pl.ds(rows, rows), behind)
    to_behind = pltpu.make_async_remote_copy(
        src_ref=final.at[3], dst_ref=final.at[4 + core], send_sem=sems.at[COPIES + 1], recv_sem=recvs.at[COPIES + core],
        device_id={"tp": behind, "rep": 1}, device_id_type=MESH,
    )
    to_behind.start()
    final[6] = last(other_rows, place)
    to_partner = remote(final.at[6], final.at[core], partner)
    to_partner.start()
    final[core] = last(own_rows, place)
    to_partner.wait_recv()
    for i in range(2):
        pltpu.make_async_remote_copy(
            src_ref=final.at[2], dst_ref=final.at[4 + i], send_sem=sems.at[COPIES], recv_sem=recvs.at[COPIES + i],
            device_id=partner, device_id_type=MESH,
        ).wait_recv()
    for i in range(2):
        cols = pl.ds(i * 256, 256)
        results[kind, :, cols] = final[i]
        results[1 - kind, :, cols] = final[4 + i]
    store(results.at[0], gate_out)
    store(results.at[1], up_out)
    to_ahead.wait_send()
    to_behind.wait_send()
    for copy in used:
        copy.wait_send()
    for copy in stores:
        copy.wait()


def finish_kernel(*refs):
    ins, outs, stage, fresh, in_sem, out_sem = refs[:9], refs[9:15], refs[15:24], refs[24:27], refs[27], refs[28]
    loads = [pltpu.make_async_copy(ins[i], stage[i], in_sem.at[i]) for i in range(9)]
    for i in (3, 6, 4, 7, 5, 8, 0, 1, 2):
        loads[i].start()
    stores = []

    def store(source, target):
        copy = pltpu.make_async_copy(source, target, out_sem.at[len(stores)])
        copy.start()
        stores.append(copy)

    for i, height in enumerate((FF, FF, D)):
        loads[3 + i].wait()
        loads[6 + i].wait()
        fresh[i][...] = SHRINK * stage[6 + i][...] - RATE * math.sqrt(height) * stage[3 + i][...].astype(jnp.float32)
        store(fresh[i], outs[2 * i + 1])
    for i in range(3):
        loads[i].wait()
        store(stage[i], outs[2 * i])
    for copy in stores:
        copy.wait()


def local(*args):
    velocities = (args[1], args[4], args[7])
    shapes = [velocity.shape for velocity in velocities]
    (rows, width), (rows_b, width_b) = shapes[0], shapes[2]
    anywhere = pl.BlockSpec(memory_space=pl.ANY)
    dma = pltpu.SemaphoreType.DMA

    def buf(*shape):
        return pltpu.VMEM(shape, BF)

    def full(*shape):
        return pltpu.VMEM(shape, jnp.float32)

    outs = [jax.ShapeDtypeStruct(shape, kind) for kind in (jnp.float32, BF) for shape in shapes]
    middle = pl.pallas_call(
        kernel,
        out_shape=outs,
        in_specs=[anywhere] * 6,
        out_specs=[anywhere] * 6,
        scratch_shapes=[
            full(2, 2, rows, width), full(2, rows_b, width_b), full(2, rows, width), full(rows_b, width_b),
            buf(2, rows, width), buf(rows_b, width_b), dma((9,)), dma((6,)),
            buf(N, N), buf(N, N), buf(N, N), buf(N, HALF),
            buf(2, 2 * rows, N), buf(2 * rows_b, NB), buf(2 * rows, N), buf(2 * rows, N), buf(7, rows, 256),
            buf(2, rows, width), buf(2, rows, width), buf(rows_b, width_b), buf(rows_b, width_b),
            buf(2, 256, 1280), buf(2, 2, 3, 64, 640), buf(2, 2, 64, 640), buf(2, 2, 3, 16, 640), buf(2, 2, 16, 640),
            buf(2, 4, 256, 1280),
            buf(128, NB), buf(2, 3, 16, NB), buf(2, 16, NB), buf(2, 3, 16, 256), buf(8, 128, NB),
            buf(NB, NB), buf(NB, NB), buf(NB, NB),
            buf(2, BLOCK, BLOCK),
            dma((COPIES + 2,)), dma((COPIES + 2,)), dma((7, 5)), dma((7, 5)),
        ],
        compiler_params=pltpu.CompilerParams(collective_id=0, has_side_effects=True, vmem_limit_bytes=62 * 1024 * 1024),
    )(args[0], args[3], args[6], args[1], args[4], args[7])
    results = [jax.ShapeDtypeStruct(shape, jnp.float32) for shape in shapes for _ in range(2)]
    stage = [full(*shape) for shape in shapes] + [buf(*shape) for shape in shapes] + [full(*shape) for shape in shapes] * 2
    return pl.pallas_call(
        finish_kernel,
        out_shape=results,
        in_specs=[anywhere] * 9,
        out_specs=[anywhere] * 6,
        scratch_shapes=stage + [dma((9,)), dma((6,))],
    )(*middle, args[2], args[5], args[8])


def solution(mesh):
    torus = Mesh(
        mesh.devices.reshape(4, 4, mesh.shape["tp"], mesh.shape["rep"]),
        ("fs_0", "fs_1", "tp", "rep"),
    )
    grads, plain = P("rep", FS, "tp"), P(FS_REP, "tp")
    return jax.shard_map(
        local,
        mesh=torus,
        in_specs=(grads, plain, plain) * 3,
        out_specs=(plain,) * 6,
        check_vma=False,
    )
```

```python
import functools
import math

import jax
import jax.numpy as jnp
from jax import lax
from jax.experimental import pallas as pl
from jax.experimental.pallas import tpu as pltpu
from jax.sharding import Mesh
from jax.sharding import PartitionSpec as P

D = 2048
FF = 5632
FS_REP = ("fs_0", "fs_1", "rep")
FS = ("fs_0", "fs_1")

MOMENT = 0.95
COEF_ONE = 3.4445
COEF_THREE = -4.775
COEF_FIVE = 2.0315
SAFETY = 2.0
RATE = 0.5
SHRINK = 0.95
BF = jnp.bfloat16


def dot(a, b):
    return jnp.dot(a, b, preferred_element_type=jnp.float32)


N = 2048
HALF = 1024
BLOCK = 512
NB = 1024
COPIES = 160
MESH = pl.DeviceIdType.MESH


def at(index, size):
    return pl.ds(index * size if isinstance(index, int) else pl.multiple_of(index * size, size), size)


def spot(offset, size, unit):
    return pl.ds(pl.multiple_of(offset, unit), size)


def turned(a, b):
    return lax.dot_general(a, b, (((0,), (0,)), ((), ())), preferred_element_type=jnp.float32)


def kernel(
    gate_g, up_g, branch_g, gate_v, up_v, branch_v,
    gate_m, up_m, branch_m, gate_out, up_out, branch_out,
    grads, grads_b, speed, speed_b, results, results_b, in_sem, out_sem,
    a, b, c, m, x0, xb, x1, x2, final, starts, relay,
    give, take, give_b, take_b,
    part, near, kept, near2, panels,
    part_b, near_b, kept_b, near2_b, gram_b, m_b, t_b, g_b,
    stage, sems, recvs, send, recv,
):
    core = lax.axis_index("rep")
    place = lax.axis_index("tp")
    iy = lax.axis_index("fs_1")
    iz = lax.axis_index("fs_0")
    other = 1 - core
    kind = lax.rem(place, 2)
    ahead = lax.rem(place + 1, 4)
    behind = lax.rem(place + 3, 4)
    across = lax.rem(place + 2, 4)
    rows = gate_v.shape[0]
    rows_b = branch_v.shape[0]
    loads = []

    def load(source, target):
        copy = pltpu.make_async_copy(source, target, in_sem.at[len(loads)])
        copy.start()
        loads.append(copy)

    load(branch_g.at[0, at(other, rows_b)], grads_b.at[1])
    load(gate_g.at[0, at(other, rows)], grads.at[0, 1])
    load(up_g.at[0, at(other, rows)], grads.at[1, 1])
    load(branch_g.at[0, at(core, rows_b)], grads_b.at[0])
    load(branch_v, speed_b)
    load(gate_g.at[0, at(core, rows)], grads.at[0, 0])
    load(gate_v, speed.at[0])
    load(up_g.at[0, at(core, rows)], grads.at[1, 0])
    load(up_v, speed.at[1])
    mine = at(core, HALF)
    partner = {"rep": other}
    used = []

    def turn(axis, index, step):
        return {axis: lax.rem(index + step, 4)}

    def remote(src, dst, to):
        k = len(used)
        copy = pltpu.make_async_remote_copy(
            src_ref=src, dst_ref=dst, send_sem=sems.at[k], recv_sem=recvs.at[k], device_id=to, device_id_type=MESH
        )
        used.append(copy)
        return copy

    def send_to(ref, to):
        copy = remote(ref, ref, to)
        copy.start()
        return copy

    barrier = pltpu.get_barrier_semaphore()
    peers = [partner, {"tp": across}]
    peers += [{"tp": x, "rep": r} for x in (ahead, behind) for r in range(2)]
    peers += [turn(axis, index, step) for axis, index in (("fs_1", iy), ("fs_0", iz)) for step in (1, 2, 3)]
    for to in peers:
        pl.semaphore_signal(barrier, inc=1, device_id=to, device_id_type=MESH)

    own_rows, other_rows = at(core, rows), at(other, rows)
    loads[0].wait()
    give_b[...] = grads_b[1].astype(BF)
    for i in range(2):
        loads[1 + i].wait()
        give[i] = grads[i, 1].astype(BF)
    pl.semaphore_wait(barrier, len(peers))
    first_copies = [remote(give_b, take_b, partner)]
    first_copies += [remote(give.at[i], take.at[i], partner) for i in range(2)]
    for copy in first_copies:
        copy.start()
    same = lax.broadcasted_iota(jnp.int32, (128, 128), 0) == lax.broadcasted_iota(jnp.int32, (128, 128), 1)

    def columns(ref, lines, height, width):
        def block(x, part):
            return ref.at[at(core, height), spot(part * 4 * width + x * width, width, width)]

        state = {}

        def start():
            state["right"] = [send_to(block(place, p), {"tp": ahead}) for p in range(2)]
            state["left"] = [send_to(block(place, p), {"tp": behind}) for p in range(2)]
            state["own"] = [send_to(block(place, p), partner) for p in range(2)]

        def second():
            state["right"][0].wait_recv()
            far = [send_to(block(behind, 0), {"tp": ahead})]
            state["left"][1].wait_recv()
            far.append(send_to(block(ahead, 1), {"tp": behind}))
            state["far"] = far
            state["own"].append(send_to(block(behind, 0), partner))
            state["own"].append(send_to(block(ahead, 1), partner))
            state["right"][1].wait_recv()
            state["own"].append(send_to(block(behind, 1), partner))
            state["left"][0].wait_recv()
            state["own"].append(send_to(block(ahead, 0), partner))

        def finish():
            for p in range(2):
                state["far"][p].wait_recv()
                state["own"].append(send_to(block(across, p), partner))
            for copy in state["own"]:
                copy.wait_recv()

        return start, second, finish

    lines = [columns(xb, None, rows_b, 128)]
    line = {}

    def block_of(x, p):
        return x0.at[own_rows, spot(p * HALF + x * 256, 256, 256)]

    def line_start():
        line["relay"] = [
            remote(starts.at[kind, p], relay.at[p], {"tp": to}) for p, to in ((0, ahead), (1, behind))
        ]
        line["out"] = [
            [remote(starts.at[1 - kind, p], block_of(place, p), {"tp": to}) for p in range(2)] for to in (ahead, behind)
        ]
        for copy in line["relay"] + line["out"][0] + line["out"][1]:
            copy.start()
        line["own"] = [send_to(block_of(place, p), partner) for p in range(2)]

    def line_second():
        line["far"] = []
        for p, (source, to) in enumerate(((behind, ahead), (ahead, behind))):
            line["relay"][p].wait_recv()
            copy = remote(relay.at[p], block_of(source, p), {"tp": to})
            copy.start()
            line["far"].append(copy)

    def line_third():
        for side, source in ((0, behind), (1, ahead)):
            for p in range(2):
                line["out"][side][p].wait_recv()
                line["own"].append(send_to(block_of(source, p), partner))

    def line_finish():
        for p in range(2):
            line["far"][p].wait_recv()
            line["own"].append(send_to(block_of(across, p), partner))
        for copy in line["own"]:
            copy.wait_recv()

    first_copies[0].wait_recv()
    loads[3].wait()
    loads[4].wait()
    moment = MOMENT * speed_b[...] + (grads_b[0] + take_b[...].astype(jnp.float32))
    speed_b[...] = moment
    for p in range(2):
        xb[at(core, rows_b), spot(p * 512 + place * 128, 128, 128)] = moment[:, p * 128 : p * 128 + 128].astype(BF)
    lines[0][0]()
    for i in range(2):
        first_copies[1 + i].wait_recv()
        loads[5 + 2 * i].wait()
        loads[6 + 2 * i].wait()
        moment = MOMENT * speed[i] + (grads[i, 0] + take[i].astype(jnp.float32))
        speed[i] = moment
        for p in range(2):
            starts[i, p] = moment[:, p * 256 : p * 256 + 256].astype(BF)
    for p in range(2):
        x0[own_rows, spot(p * HALF + place * 256, 256, 256)] = starts[kind, p]
    line_start()
    stores = []

    def store(source, target):
        copy = pltpu.make_async_copy(source, target, out_sem.at[len(stores)])
        copy.start()
        stores.append(copy)

    axes = ((("fs_1", iy), ("fs_0", iz)), (("fs_0", iz), ("fs_1", iy)))

    def exchange(source, landing, axis, index):
        copies = []
        for step in (2, 1, 3):
            to = lax.rem(index + step, 4)
            copies.append(remote(source(to), landing.at[step - 1], {axis: to}))
            copies[-1].start()
        return copies

    def total(own, landing, copies):
        for copy in copies:
            copy.wait_recv()
        value = own.astype(jnp.float32)
        for k in range(3):
            value = value + landing[k].astype(jnp.float32)
        return value.astype(BF)

    def scatter_one(source, landings):
        return [
            exchange(functools.partial(source, p), landings[p], *axes[p][0]) for p in range(2)
        ]

    def source_of(i):
        return lambda p, t: part.at[i, at(t, 64), at(p, 640)]

    def source_b(p, t):
        return part_b.at[spot(p * 64 + t * 16, 16, 16), :]

    upper = lax.div(place, 2)

    def panel(i):
        first = core * 4 + 2 * upper + i
        own = x0[:, at(first, 256)]
        for d in range(5):
            part[i, :, at(d, 256)] = turned(own, x0[:, at(lax.rem(first + d, 8), 256)]).astype(BF)
        return scatter_one(source_of(i), [near.at[i, p] for p in range(2)])

    def gram_rows(p, i1):
        return spot(p * 64 + i1 * 16, 16, 16)

    group = at(core, 4)

    class Ring:
        def __init__(self, axis, index, block, cut):
            self.next, self.prev = turn(axis, index, 1), turn(axis, index, 3)
            self.index, self.block, self.cut = index, block, cut

        def start(self):
            ref = self.block(self.index)
            self.right = send_to(ref, self.next)
            self.left = send_to(ref, self.prev)

        def second(self):
            self.right.wait_recv()
            self.far = [send_to(self.cut(lax.rem(self.index + 3, 4), 0), self.next)]
            self.left.wait_recv()
            self.far.append(send_to(self.cut(lax.rem(self.index + 1, 4), 1), self.prev))

        def finish(self):
            for copy in self.far:
                copy.wait_recv()

    def rings(phase, block, cut):
        return [
            Ring(*axes[p][phase], functools.partial(block, p), functools.partial(cut, p)) for p in range(2)
        ]

    def b_small(p, j):
        return gram_b.at[group, gram_rows(p, axes[p][0][1]), at(j, 256)]

    def b_small_cut(p, j, h):
        return gram_b.at[at(core * 2 + h, 2), gram_rows(p, axes[p][0][1]), at(j, 256)]

    def b_large(p, j):
        return gram_b.at[group, gram_rows(p, j), :]

    def b_large_cut(p, j, h):
        return gram_b.at[at(core * 2 + h, 2), gram_rows(p, j), :]

    def g_rows(p, j):
        return spot(axes[p][0][1] * 64 + j * 16, 16, 16)

    def g_small(p, j):
        return panels.at[core, :, g_rows(p, j), at(p, 640)]

    def g_small_cut(p, j, h):
        return panels.at[core, at(h, 2), g_rows(p, j), at(p, 640)]

    def g_large(p, j):
        return panels.at[core, :, at(j, 64), at(p, 640)]

    def g_large_cut(p, j, h):
        return panels.at[core, at(h, 2), at(j, 64), at(p, 640)]

    small_b, large_b = rings(1, b_small, b_small_cut), rings(0, b_large, b_large_cut)
    small, large = rings(1, g_small, g_small_cut), rings(0, g_large, g_large_cut)
    lines[0][1]()
    lines[0][2]()
    part_b[...] = turned(xb[:, spot(core * 512 + place * 128, 128, 128)], xb[...]).astype(BF)
    one_b = scatter_one(source_b, [near_b.at[p] for p in range(2)])
    line_second()
    two_b = []
    for p in range(2):
        kept_b[p] = total(part_b[spot(p * 64 + axes[p][0][1] * 16, 16, 16), :], near_b.at[p], one_b[p])
        two_b.append(exchange(lambda t, p=p: kept_b.at[p, :, at(t, 256)], near2_b.at[p], *axes[p][1]))
    line_third()
    swaps_b = []
    for p in range(2):
        i1, i2 = axes[p][0][1], axes[p][1][1]
        gram_b[core * 4 + place, gram_rows(p, i1), at(i2, 256)] = total(
            kept_b[p, :, at(i2, 256)], near2_b.at[p], two_b[p]
        )
        ref = gram_b.at[core * 4 + place, gram_rows(p, i1), at(i2, 256)]
        swaps_b.append([send_to(ref, {"tp": x}) for x in (across, ahead, behind)])
    for source, target in ((speed_b, branch_m), (speed.at[0], gate_m), (speed.at[1], up_m)):
        store(source, target)
    line_finish()
    ones = [panel(0), panel(1)]

    def scatter_two(i):
        pair = []
        for p in range(2):
            index = axes[p][0][1]
            kept[i, p] = total(part[i, at(index, 64), at(p, 640)], near.at[i, p], ones[i][p])
            pair.append(exchange(lambda t, p=p: kept.at[i, p, at(t, 16), :], near2.at[i, p], *axes[p][1]))
        return pair

    twos = [scatter_two(0)]
    for p in range(2):
        for copy in swaps_b[p]:
            copy.wait_recv()
        small_b[p].start()
    twos.append(scatter_two(1))
    for ring in small_b:
        ring.second()
    swaps = []
    for p in range(2):
        i2 = axes[p][1][1]
        for i in range(2):
            panels[core, 2 * upper + i, g_rows(p, i2), at(p, 640)] = total(
                kept[i, p, at(i2, 16), :], near2.at[i, p], twos[i][p]
            )
        swaps.append(send_to(panels.at[core, at(upper, 2), g_rows(p, i2), at(p, 640)], {"tp": across}))
    for ring in small_b:
        ring.finish()
    for ring in large_b:
        ring.start()
    for copy in swaps:
        copy.wait_recv()
    for ring in small:
        ring.start()
    forward_b, forward = [], []
    for p, ring in enumerate(large_b):
        ring.second()
        forward_b += [send_to(b_large(p, lax.rem(ring.index + k, 4)), partner) for k in (0, 3, 1)]
    for ring in small:
        ring.second()
    for p, ring in enumerate(large_b):
        ring.finish()
        forward_b.append(send_to(b_large(p, lax.rem(ring.index + 2, 4)), partner))
    for ring in small:
        ring.finish()
    for ring in large:
        ring.start()
    for copy in forward_b:
        copy.wait_recv()

    def coefficients(squares, diagonal):
        second = jnp.full((1, 1), squares)
        first = jnp.full((1, 1), diagonal)
        ratio = SAFETY * (second + 1.0) / (first + 1.0)
        return 1.0 / ratio, lax.rsqrt(ratio)

    def squares_b(i, sums):
        value = gram_b[i].astype(jnp.float32)
        diagonal = gram_b[i, :, at(i, 128)].astype(jnp.float32)
        return (
            sums[0] + jnp.sum((value * value).reshape(16, 8, NB), axis=0),
            sums[1] + jnp.where(same, diagonal, 0.0),
        )

    sums = lax.fori_loop(0, 8, squares_b, (jnp.zeros((8, NB), jnp.float32), jnp.zeros((128, 128), jnp.float32)))
    alpha_b, scale_b = coefficients(jnp.sum(sums[0]), jnp.sum(sums[1]))

    top, low_half = pl.ds(0, 512), pl.ds(512, 512)

    def mirrored_b(left, right, out, emit):
        out[top, top] = emit(left[top, top], dot(left[top, :], right[:, top])).astype(BF)
        out[low_half, :] = emit(left[low_half, :], dot(left[low_half, :], right[...])).astype(BF)
        out[top, low_half] = out[low_half, top].T

    def square_b(left, low, high):
        mirrored_b(left, left, m_b, lambda own, value: low * own.astype(jnp.float32) + high * value)

    def times_b(left, out, factor):
        mirrored_b(left, m_b, out, lambda own, value: factor * (COEF_ONE * own.astype(jnp.float32) + value))

    def rows_of(left, factor):
        return (factor * (COEF_ONE * left.astype(jnp.float32) + dot(left, m_b[...]))).astype(BF)

    for i in range(8):
        g_b[at(i, 128), :] = gram_b[i]
    square_b(g_b, COEF_THREE * alpha_b, COEF_FIVE * alpha_b * alpha_b)
    times_b(g_b, t_b, alpha_b)
    line_b = rows_of(xb[at(core, rows_b), :], scale_b)
    times_b(t_b, g_b, 1.0)
    square_b(g_b, COEF_THREE, COEF_FIVE)
    for p, ring in enumerate(large):
        ring.second()
        forward += [send_to(g_large(p, lax.rem(ring.index + k, 4)), partner) for k in (0, 3, 1)]
    times_b(g_b, t_b, 1.0)
    line_b = rows_of(line_b, 1.0)
    times_b(t_b, g_b, 1.0)
    for p, ring in enumerate(large):
        ring.finish()
        forward.append(send_to(g_large(p, lax.rem(ring.index + 2, 4)), partner))
    square_b(g_b, COEF_THREE, COEF_FIVE)
    t_b[0:rows_b, :] = line_b
    for p in range(2):
        cols = spot(p * 512 + place * 128, 128, 128)
        last_b = COEF_ONE * t_b[0:rows_b, cols].astype(jnp.float32) + dot(line_b, m_b[:, cols])
        results_b[:, at(p, 128)] = last_b.astype(BF)
    store(results_b, branch_out)
    for copy in forward:
        copy.wait_recv()

    def assemble(r, sums):
        value = panels[lax.div(r, 4), lax.rem(r, 4)]
        squares, diagonal = sums
        for d in range(5):
            block = value[:, d * 256 : d * 256 + 256]
            column = at(lax.rem(r + d, 8), 256)
            a[at(r, 256), column] = block
            if 0 < d < 4:
                a[column, at(r, 256)] = block.T
            wide = block.astype(jnp.float32)
            weight = 2.0 if 0 < d < 4 else 1.0
            squares = squares + weight * jnp.sum((wide * wide).reshape(32, 8, 256), axis=0)
        for k in range(2):
            corner = value[k * 128 : k * 128 + 128, k * 128 : k * 128 + 128].astype(jnp.float32)
            diagonal = diagonal + jnp.where(same, corner, 0.0)
        return squares, diagonal

    sums = lax.fori_loop(0, 8, assemble, (jnp.zeros((8, 256), jnp.float32), jnp.zeros((128, 128), jnp.float32)))
    alpha, scale = coefficients(jnp.sum(sums[0]), jnp.sum(sums[1]))


    def h(q):
        return at(2 * core + q, BLOCK)

    def o(q):
        return at(2 * other + q, BLOCK)

    def flip(q):
        return lax.rem(q + core, 2)

    def flop(q):
        return lax.rem(q + other, 2)

    def pair(ref, target, k, q):
        return pltpu.make_async_remote_copy(
            src_ref=ref, dst_ref=target, send_sem=send.at[k, q], recv_sem=recv.at[k, q], device_id=partner, device_id_type=MESH
        )

    def cross_out(buf, k, q):
        ref = buf.at[o(q), h(flip(q))]
        return pair(ref, ref, k, q)

    def cross_in(buf, k, q):
        ref = buf.at[h(q), o(flop(q))]
        return pair(ref, ref, k, q)

    def square_out(buf, k, q, side):
        first = at(2 * side, BLOCK)
        second = at(2 * side + 1, BLOCK)
        ref = (buf.at[first, at(side, HALF)], buf.at[second, first], buf.at[second, second])[q]
        return pair(ref, ref, k, 2 + q)

    def stage_out(k, q):
        return pair(m.at[o(q), at(flip(q), BLOCK)], stage.at[q], 4 + k, q)

    def receive_cross(left, k):
        def step(q, _):
            cross_out(left, k, q).wait_send()
            cross_in(left, k, q).wait_recv()
            left[o(flop(q)), h(q)] = left[h(q), o(flop(q))].T
            return 0

        lax.fori_loop(0, 2, step, 0)

    def receive_square(left, k):
        for q in range(3):
            square_out(left, k, q, core).wait_send()
            square_out(left, k, q, other).wait_recv()

    def product(left, k, right, emit, after_head, after_cross, after_all):
        if k is not None:
            receive_cross(left, k)

        def head(q, _):
            emit(h(q), 0, dot(left[h(q), :], right(0)))
            return 0

        lax.fori_loop(0, 2, head, 0)
        after_head()
        if k is not None:
            receive_square(left, k)

        def cross(q, _):
            j = flip(q)
            emit(o(q), j, dot(left[o(q), :], right(j)))
            after_cross(q)
            return 0

        lax.fori_loop(0, 2, cross, 0)
        emit(h(1), 1, dot(left[h(1), :], right(1)))
        after_all()

    def square(left, k, k_out, low, high):
        def emit(where, j, value):
            value = low * left[where, h(j)].astype(jnp.float32) + high * value
            m[where, at(j, BLOCK)] = value.astype(BF)

        def after_head():
            m[h(0), at(1, BLOCK)] = m[h(1), at(0, BLOCK)].T

        def after_cross(q):
            stage_out(k_out, q).start()

        def right(j):
            return left[:, h(j)]

        product(left, k, right, emit, after_head, after_cross, lambda: None)

        def receive(q, _):
            copy = stage_out(k_out, q)
            copy.wait_send()
            copy.wait_recv()
            m[o(flop(q)), at(q, BLOCK)] = stage[q].T
            return 0

        lax.fori_loop(0, 2, receive, 0)

    def times(left, k, out, k_out, factor):
        def emit(where, j, value):
            value = COEF_ONE * left[where, h(j)].astype(jnp.float32) + value
            if factor is not None:
                value = factor * value
            out[where, h(j)] = value.astype(BF)

        def after_head():
            out[h(0), h(1)] = out[h(1), h(0)].T
            square_out(out, k_out, 0, core).start()
            square_out(out, k_out, 1, core).start()

        def after_cross(q):
            cross_out(out, k_out, q).start()
            out[h(flip(q)), o(q)] = out[o(q), h(flip(q))].T

        def after_all():
            square_out(out, k_out, 2, core).start()

        def right(j):
            return m[:, at(j, BLOCK)]

        product(left, k, right, emit, after_head, after_cross, after_all)

    square(a, None, 0, COEF_THREE * alpha, COEF_FIVE * alpha * alpha)
    times(a, None, b, 0, alpha)
    x1[:, mine] = (scale * (COEF_ONE * x0[:, mine].astype(jnp.float32) + dot(x0[...], m[...]))).astype(BF)
    turn_one = send_to(x1.at[:, mine], partner)
    times(b, 0, c, 1, None)
    square(c, 1, 1, COEF_THREE, COEF_FIVE)
    times(c, None, b, 2, None)
    turn_one.wait_recv()
    x2[:, mine] = (COEF_ONE * x1[:, mine].astype(jnp.float32) + dot(x1[...], m[...])).astype(BF)
    turn_two = send_to(x2.at[:, mine], partner)
    times(b, 2, a, 3, None)

    def some(block, low, high):
        close = spot(core * HALF + block * 256, 256, 256)

        def step(r, _):
            where = at(lax.rem(2 * core + r, 4), BLOCK)
            value = COEF_THREE * a[where, close].astype(jnp.float32) + COEF_FIVE * dot(a[where, :], a[:, close])
            m[where, at(block, 256)] = value.astype(BF)
            return 0

        lax.fori_loop(low, high, step, 0)

    def last(where, block):
        cols = at(block, 256)
        close = spot(core * HALF + block * 256, 256, 256)
        return (COEF_ONE * x2[where, close].astype(jnp.float32) + dot(x2[where, :], m[:, cols])).astype(BF)

    receive_cross(a, 3)
    some(ahead, 0, 2)
    receive_square(a, 3)
    some(ahead, 2, 4)
    turn_two.wait_recv()
    final[2] = last(pl.ds(0, rows), ahead)
    to_ahead = pltpu.make_async_remote_copy(
        src_ref=final.at[2], dst_ref=final.at[4 + core], send_sem=sems.at[COPIES], recv_sem=recvs.at[COPIES + core],
        device_id={"tp": ahead, "rep": 0}, device_id_type=MESH,
    )
    to_ahead.start()
    some(behind, 0, 4)
    final[3] = last(pl.ds(rows, rows), behind)
    to_behind = pltpu.make_async_remote_copy(
        src_ref=final.at[3], dst_ref=final.at[4 + core], send_sem=sems.at[COPIES + 1], recv_sem=recvs.at[COPIES + core],
        device_id={"tp": behind, "rep": 1}, device_id_type=MESH,
    )
    to_behind.start()
    some(place, 0, 4)
    final[6] = last(other_rows, place)
    to_partner = remote(final.at[6], final.at[core], partner)
    to_partner.start()
    final[core] = last(own_rows, place)
    to_partner.wait_recv()
    for i in range(2):
        pltpu.make_async_remote_copy(
            src_ref=final.at[2], dst_ref=final.at[4 + i], send_sem=sems.at[COPIES], recv_sem=recvs.at[COPIES + i],
            device_id=partner, device_id_type=MESH,
        ).wait_recv()
    for i in range(2):
        cols = pl.ds(i * 256, 256)
        results[kind, :, cols] = final[i]
        results[1 - kind, :, cols] = final[4 + i]
    store(results.at[0], gate_out)
    store(results.at[1], up_out)
    to_ahead.wait_send()
    to_behind.wait_send()
    for copy in used:
        copy.wait_send()
    for copy in stores:
        copy.wait()


def finish_kernel(*refs):
    ins, outs, stage, fresh, in_sem, out_sem = refs[:9], refs[9:15], refs[15:24], refs[24:27], refs[27], refs[28]
    loads = [pltpu.make_async_copy(ins[i], stage[i], in_sem.at[i]) for i in range(9)]
    for i in (3, 6, 4, 7, 5, 8, 0, 1, 2):
        loads[i].start()
    stores = []

    def store(source, target):
        copy = pltpu.make_async_copy(source, target, out_sem.at[len(stores)])
        copy.start()
        stores.append(copy)

    for i, height in enumerate((FF, FF, D)):
        loads[3 + i].wait()
        loads[6 + i].wait()
        fresh[i][...] = SHRINK * stage[6 + i][...] - RATE * math.sqrt(height) * stage[3 + i][...].astype(jnp.float32)
        store(fresh[i], outs[2 * i + 1])
    for i in range(3):
        loads[i].wait()
        store(stage[i], outs[2 * i])
    for copy in stores:
        copy.wait()


def local(*args):
    velocities = (args[1], args[4], args[7])
    shapes = [velocity.shape for velocity in velocities]
    (rows, width), (rows_b, width_b) = shapes[0], shapes[2]
    anywhere = pl.BlockSpec(memory_space=pl.ANY)
    dma = pltpu.SemaphoreType.DMA

    def buf(*shape):
        return pltpu.VMEM(shape, BF)

    def full(*shape):
        return pltpu.VMEM(shape, jnp.float32)

    outs = [jax.ShapeDtypeStruct(shape, kind) for kind in (jnp.float32, BF) for shape in shapes]
    middle = pl.pallas_call(
        kernel,
        out_shape=outs,
        in_specs=[anywhere] * 6,
        out_specs=[anywhere] * 6,
        scratch_shapes=[
            full(2, 2, rows, width), full(2, rows_b, width_b), full(2, rows, width), full(rows_b, width_b),
            buf(2, rows, width), buf(rows_b, width_b), dma((9,)), dma((6,)),
            buf(N, N), buf(N, N), buf(N, N), buf(N, HALF),
            buf(2 * rows, N), buf(2 * rows_b, NB), buf(2 * rows, N), buf(2 * rows, N), buf(7, rows, 256),
            buf(2, 2, rows, 256), buf(2, rows, 256),
            buf(2, rows, width), buf(2, rows, width), buf(rows_b, width_b), buf(rows_b, width_b),
            buf(2, 256, 1280), buf(2, 2, 3, 64, 640), buf(2, 2, 64, 640), buf(2, 2, 3, 16, 640),
            buf(2, 4, 256, 1280),
            buf(128, NB), buf(2, 3, 16, NB), buf(2, 16, NB), buf(2, 3, 16, 256), buf(8, 128, NB),
            buf(NB, NB), buf(NB, NB), buf(NB, NB),
            buf(2, BLOCK, BLOCK),
            dma((COPIES + 2,)), dma((COPIES + 2,)), dma((7, 5)), dma((7, 5)),
        ],
        compiler_params=pltpu.CompilerParams(collective_id=0, has_side_effects=True, vmem_limit_bytes=62 * 1024 * 1024),
    )(args[0], args[3], args[6], args[1], args[4], args[7])
    results = [jax.ShapeDtypeStruct(shape, jnp.float32) for shape in shapes for _ in range(2)]
    stage = [full(*shape) for shape in shapes] + [buf(*shape) for shape in shapes] + [full(*shape) for shape in shapes] * 2
    return pl.pallas_call(
        finish_kernel,
        out_shape=results,
        in_specs=[anywhere] * 9,
        out_specs=[anywhere] * 6,
        scratch_shapes=stage + [dma((9,)), dma((6,))],
    )(*middle, args[2], args[5], args[8])


def solution(mesh):
    torus = Mesh(
        mesh.devices.reshape(4, 4, mesh.shape["tp"], mesh.shape["rep"]),
        ("fs_0", "fs_1", "tp", "rep"),
    )
    grads, plain = P("rep", FS, "tp"), P(FS_REP, "tp")
    return jax.shard_map(
        local,
        mesh=torus,
        in_specs=(grads, plain, plain) * 3,
        out_specs=(plain,) * 6,
        check_vma=False,
    )
```

```python
import functools
import math

import jax
import jax.numpy as jnp
from jax import lax
from jax.experimental import pallas as pl
from jax.experimental.pallas import tpu as pltpu
from jax.sharding import Mesh
from jax.sharding import PartitionSpec as P

D = 2048
FF = 5632
FS_REP = ("fs_0", "fs_1", "rep")
FS = ("fs_0", "fs_1")

MOMENT = 0.95
COEF_ONE = 3.4445
COEF_THREE = -4.775
COEF_FIVE = 2.0315
SAFETY = 2.0
RATE = 0.5
SHRINK = 0.95
BF = jnp.bfloat16


def dot(a, b):
    return jnp.dot(a, b, preferred_element_type=jnp.float32)


N = 2048
HALF = 1024
BLOCK = 512
NB = 1024
COPIES = 160
MESH = pl.DeviceIdType.MESH


def at(index, size):
    return pl.ds(index * size if isinstance(index, int) else pl.multiple_of(index * size, size), size)


def spot(offset, size, unit):
    return pl.ds(pl.multiple_of(offset, unit), size)


def turned(a, b):
    return lax.dot_general(a, b, (((0,), (0,)), ((), ())), preferred_element_type=jnp.float32)


def kernel(
    gate_g, up_g, branch_g, gate_v, up_v, branch_v,
    gate_m, up_m, branch_m, gate_out, up_out, branch_out,
    grads, grads_b, speed, speed_b, results, results_b, in_sem, out_sem,
    a, b, c, m, x0, xb, x1, x2, final, starts, relay,
    give, take, give_b, take_b,
    part, near, kept, near2, panels,
    part_b, near_b, kept_b, near2_b, gram_b, m_b, t_b, g_b,
    stage, sems, recvs, send, recv,
):
    core = lax.axis_index("rep")
    place = lax.axis_index("tp")
    iy = lax.axis_index("fs_1")
    iz = lax.axis_index("fs_0")
    other = 1 - core
    kind = lax.rem(place, 2)
    ahead = lax.rem(place + 1, 4)
    behind = lax.rem(place + 3, 4)
    across = lax.rem(place + 2, 4)
    rows = gate_v.shape[0]
    rows_b = branch_v.shape[0]
    loads = []

    def load(source, target):
        copy = pltpu.make_async_copy(source, target, in_sem.at[len(loads)])
        copy.start()
        loads.append(copy)

    load(branch_g.at[0, at(other, rows_b)], grads_b.at[1])
    load(gate_g.at[0, at(other, rows)], grads.at[0, 1])
    load(up_g.at[0, at(other, rows)], grads.at[1, 1])
    load(branch_g.at[0, at(core, rows_b)], grads_b.at[0])
    load(branch_v, speed_b)
    load(gate_g.at[0, at(core, rows)], grads.at[0, 0])
    load(gate_v, speed.at[0])
    load(up_g.at[0, at(core, rows)], grads.at[1, 0])
    load(up_v, speed.at[1])
    mine = at(core, HALF)
    partner = {"rep": other}
    used = []

    def turn(axis, index, step):
        return {axis: lax.rem(index + step, 4)}

    def remote(src, dst, to):
        k = len(used)
        copy = pltpu.make_async_remote_copy(
            src_ref=src, dst_ref=dst, send_sem=sems.at[k], recv_sem=recvs.at[k], device_id=to, device_id_type=MESH
        )
        used.append(copy)
        return copy

    def send_to(ref, to):
        copy = remote(ref, ref, to)
        copy.start()
        return copy

    barrier = pltpu.get_barrier_semaphore()
    peers = [partner, {"tp": across}]
    peers += [{"tp": x, "rep": r} for x in (ahead, behind) for r in range(2)]
    peers += [turn(axis, index, step) for axis, index in (("fs_1", iy), ("fs_0", iz)) for step in (1, 2, 3)]
    for to in peers:
        pl.semaphore_signal(barrier, inc=1, device_id=to, device_id_type=MESH)

    own_rows, other_rows = at(core, rows), at(other, rows)
    loads[0].wait()
    give_b[...] = grads_b[1].astype(BF)
    for i in range(2):
        loads[1 + i].wait()
        give[i] = grads[i, 1].astype(BF)
    pl.semaphore_wait(barrier, len(peers))
    first_copies = [remote(give_b, take_b, partner)]
    first_copies += [remote(give.at[i], take.at[i], partner) for i in range(2)]
    for copy in first_copies:
        copy.start()
    same = lax.broadcasted_iota(jnp.int32, (128, 128), 0) == lax.broadcasted_iota(jnp.int32, (128, 128), 1)

    def columns(ref, lines, height, width):
        def block(x, part):
            return ref.at[at(core, height), spot(part * 4 * width + x * width, width, width)]

        state = {}

        def start():
            state["right"] = [send_to(block(place, p), {"tp": ahead}) for p in range(2)]
            state["left"] = [send_to(block(place, p), {"tp": behind}) for p in range(2)]
            state["own"] = [send_to(block(place, p), partner) for p in range(2)]

        def second():
            state["right"][0].wait_recv()
            far = [send_to(block(behind, 0), {"tp": ahead})]
            state["left"][1].wait_recv()
            far.append(send_to(block(ahead, 1), {"tp": behind}))
            state["far"] = far
            state["own"].append(send_to(block(behind, 0), partner))
            state["own"].append(send_to(block(ahead, 1), partner))
            state["right"][1].wait_recv()
            state["own"].append(send_to(block(behind, 1), partner))
            state["left"][0].wait_recv()
            state["own"].append(send_to(block(ahead, 0), partner))

        def finish():
            for p in range(2):
                state["far"][p].wait_recv()
                state["own"].append(send_to(block(across, p), partner))
            for copy in state["own"]:
                copy.wait_recv()

        return start, second, finish

    lines = [columns(xb, None, rows_b, 128)]
    line = {}

    def block_of(x, p):
        return x0.at[own_rows, spot(p * HALF + x * 256, 256, 256)]

    def line_start():
        line["relay"] = [
            remote(starts.at[kind, p], relay.at[p], {"tp": to}) for p, to in ((0, ahead), (1, behind))
        ]
        line["out"] = [
            [remote(starts.at[1 - kind, p], block_of(place, p), {"tp": to}) for p in range(2)] for to in (ahead, behind)
        ]
        for copy in line["relay"] + line["out"][0] + line["out"][1]:
            copy.start()
        line["own"] = [send_to(block_of(place, p), partner) for p in range(2)]

    def line_second():
        line["far"] = []
        for p, (source, to) in enumerate(((behind, ahead), (ahead, behind))):
            line["relay"][p].wait_recv()
            copy = remote(relay.at[p], block_of(source, p), {"tp": to})
            copy.start()
            line["far"].append(copy)

    def line_third():
        for side, source in ((0, behind), (1, ahead)):
            for p in range(2):
                line["out"][side][p].wait_recv()
                line["own"].append(send_to(block_of(source, p), partner))

    def line_finish():
        for p in range(2):
            line["far"][p].wait_recv()
            line["own"].append(send_to(block_of(across, p), partner))
        for copy in line["own"]:
            copy.wait_recv()

    first_copies[0].wait_recv()
    loads[3].wait()
    loads[4].wait()
    moment = MOMENT * speed_b[...] + (grads_b[0] + take_b[...].astype(jnp.float32))
    speed_b[...] = moment
    for p in range(2):
        xb[at(core, rows_b), spot(p * 512 + place * 128, 128, 128)] = moment[:, p * 128 : p * 128 + 128].astype(BF)
    lines[0][0]()
    for i in range(2):
        first_copies[1 + i].wait_recv()
        loads[5 + 2 * i].wait()
        loads[6 + 2 * i].wait()
        moment = MOMENT * speed[i] + (grads[i, 0] + take[i].astype(jnp.float32))
        speed[i] = moment
        for p in range(2):
            starts[i, p] = moment[:, p * 256 : p * 256 + 256].astype(BF)
    for p in range(2):
        x0[own_rows, spot(p * HALF + place * 256, 256, 256)] = starts[kind, p]
    line_start()
    stores = []

    def store(source, target):
        copy = pltpu.make_async_copy(source, target, out_sem.at[len(stores)])
        copy.start()
        stores.append(copy)

    axes = ((("fs_1", iy), ("fs_0", iz)), (("fs_0", iz), ("fs_1", iy)))

    def exchange(source, landing, axis, index):
        copies = []
        for step in (2, 1, 3):
            to = lax.rem(index + step, 4)
            copies.append(remote(source(to), landing.at[step - 1], {axis: to}))
            copies[-1].start()
        return copies

    def total(own, landing, copies):
        for copy in copies:
            copy.wait_recv()
        value = own.astype(jnp.float32)
        for k in range(3):
            value = value + landing[k].astype(jnp.float32)
        return value.astype(BF)

    def scatter_one(source, landings):
        return [
            exchange(functools.partial(source, p), landings[p], *axes[p][0]) for p in range(2)
        ]

    def source_of(i):
        return lambda p, t: part.at[i, at(t, 64), at(p, 640)]

    def source_b(p, t):
        return part_b.at[spot(p * 64 + t * 16, 16, 16), :]

    upper = lax.div(place, 2)

    def panel(i):
        first = core * 4 + 2 * upper + i
        own = x0[:, at(first, 256)]
        for d in range(5):
            part[i, :, at(d, 256)] = turned(own, x0[:, at(lax.rem(first + d, 8), 256)]).astype(BF)
        return scatter_one(source_of(i), [near.at[i, p] for p in range(2)])

    def gram_rows(p, i1):
        return spot(p * 64 + i1 * 16, 16, 16)

    group = at(core, 4)

    class Ring:
        def __init__(self, axis, index, block, cut):
            self.next, self.prev = turn(axis, index, 1), turn(axis, index, 3)
            self.index, self.block, self.cut = index, block, cut

        def start(self):
            ref = self.block(self.index)
            self.right = send_to(ref, self.next)
            self.left = send_to(ref, self.prev)

        def second(self):
            self.right.wait_recv()
            self.far = [send_to(self.cut(lax.rem(self.index + 3, 4), 0), self.next)]
            self.left.wait_recv()
            self.far.append(send_to(self.cut(lax.rem(self.index + 1, 4), 1), self.prev))

        def finish(self):
            for copy in self.far:
                copy.wait_recv()

    def rings(phase, block, cut):
        return [
            Ring(*axes[p][phase], functools.partial(block, p), functools.partial(cut, p)) for p in range(2)
        ]

    def b_small(p, j):
        return gram_b.at[group, gram_rows(p, axes[p][0][1]), at(j, 256)]

    def b_small_cut(p, j, h):
        return gram_b.at[at(core * 2 + h, 2), gram_rows(p, axes[p][0][1]), at(j, 256)]

    def b_large(p, j):
        return gram_b.at[group, gram_rows(p, j), :]

    def b_large_cut(p, j, h):
        return gram_b.at[at(core * 2 + h, 2), gram_rows(p, j), :]

    def g_rows(p, j):
        return spot(axes[p][0][1] * 64 + j * 16, 16, 16)

    def g_small(p, j):
        return panels.at[core, :, g_rows(p, j), at(p, 640)]

    def g_small_cut(p, j, h):
        return panels.at[core, at(h, 2), g_rows(p, j), at(p, 640)]

    def g_large(p, j):
        return panels.at[core, :, at(j, 64), at(p, 640)]

    def g_large_cut(p, j, h):
        return panels.at[core, at(h, 2), at(j, 64), at(p, 640)]

    small_b, large_b = rings(1, b_small, b_small_cut), rings(0, b_large, b_large_cut)
    small, large = rings(1, g_small, g_small_cut), rings(0, g_large, g_large_cut)
    lines[0][1]()
    line_second()
    lines[0][2]()
    part_b[...] = turned(xb[:, spot(core * 512 + place * 128, 128, 128)], xb[...]).astype(BF)
    one_b = scatter_one(source_b, [near_b.at[p] for p in range(2)])
    line_third()
    for source, target in ((speed_b, branch_m), (speed.at[0], gate_m), (speed.at[1], up_m)):
        store(source, target)
    line_finish()
    ones = [panel(0), panel(1)]
    two_b = []
    for p in range(2):
        kept_b[p] = total(part_b[spot(p * 64 + axes[p][0][1] * 16, 16, 16), :], near_b.at[p], one_b[p])
        two_b.append(exchange(lambda t, p=p: kept_b.at[p, :, at(t, 256)], near2_b.at[p], *axes[p][1]))
    swaps_b = []
    for p in range(2):
        i1, i2 = axes[p][0][1], axes[p][1][1]
        gram_b[core * 4 + place, gram_rows(p, i1), at(i2, 256)] = total(
            kept_b[p, :, at(i2, 256)], near2_b.at[p], two_b[p]
        )
        ref = gram_b.at[core * 4 + place, gram_rows(p, i1), at(i2, 256)]
        swaps_b.append([send_to(ref, {"tp": x}) for x in (across, ahead, behind)])

    def scatter_two(i):
        pair = []
        for p in range(2):
            index = axes[p][0][1]
            kept[i, p] = total(part[i, at(index, 64), at(p, 640)], near.at[i, p], ones[i][p])
            pair.append(exchange(lambda t, p=p: kept.at[i, p, at(t, 16), :], near2.at[i, p], *axes[p][1]))
        return pair

    twos = [scatter_two(0)]
    for p in range(2):
        for copy in swaps_b[p]:
            copy.wait_recv()
        small_b[p].start()
    twos.append(scatter_two(1))
    for ring in small_b:
        ring.second()
    swaps = []
    for p in range(2):
        i2 = axes[p][1][1]
        for i in range(2):
            panels[core, 2 * upper + i, g_rows(p, i2), at(p, 640)] = total(
                kept[i, p, at(i2, 16), :], near2.at[i, p], twos[i][p]
            )
        swaps.append(send_to(panels.at[core, at(upper, 2), g_rows(p, i2), at(p, 640)], {"tp": across}))
    for ring in small_b:
        ring.finish()
    for ring in large_b:
        ring.start()
    for copy in swaps:
        copy.wait_recv()
    for ring in small:
        ring.start()
    forward_b, forward = [], []
    for p, ring in enumerate(large_b):
        ring.second()
        forward_b += [send_to(b_large(p, lax.rem(ring.index + k, 4)), partner) for k in (0, 3, 1)]
    for ring in small:
        ring.second()
    for p, ring in enumerate(large_b):
        ring.finish()
        forward_b.append(send_to(b_large(p, lax.rem(ring.index + 2, 4)), partner))
    for ring in small:
        ring.finish()
    for ring in large:
        ring.start()
    for copy in forward_b:
        copy.wait_recv()

    def coefficients(squares, diagonal):
        second = jnp.full((1, 1), squares)
        first = jnp.full((1, 1), diagonal)
        ratio = SAFETY * (second + 1.0) / (first + 1.0)
        return 1.0 / ratio, lax.rsqrt(ratio)

    def squares_b(i, sums):
        value = gram_b[i].astype(jnp.float32)
        diagonal = gram_b[i, :, at(i, 128)].astype(jnp.float32)
        return (
            sums[0] + jnp.sum((value * value).reshape(16, 8, NB), axis=0),
            sums[1] + jnp.where(same, diagonal, 0.0),
        )

    sums = lax.fori_loop(0, 8, squares_b, (jnp.zeros((8, NB), jnp.float32), jnp.zeros((128, 128), jnp.float32)))
    alpha_b, scale_b = coefficients(jnp.sum(sums[0]), jnp.sum(sums[1]))

    top, low_half = pl.ds(0, 512), pl.ds(512, 512)

    def mirrored_b(left, right, out, emit):
        out[top, top] = emit(left[top, top], dot(left[top, :], right[:, top])).astype(BF)
        out[low_half, :] = emit(left[low_half, :], dot(left[low_half, :], right[...])).astype(BF)
        out[top, low_half] = out[low_half, top].T

    def square_b(left, low, high):
        mirrored_b(left, left, m_b, lambda own, value: low * own.astype(jnp.float32) + high * value)

    def times_b(left, out, factor):
        mirrored_b(left, m_b, out, lambda own, value: factor * (COEF_ONE * own.astype(jnp.float32) + value))

    def rows_of(left, factor):
        return (factor * (COEF_ONE * left.astype(jnp.float32) + dot(left, m_b[...]))).astype(BF)

    for i in range(8):
        g_b[at(i, 128), :] = gram_b[i]
    square_b(g_b, COEF_THREE * alpha_b, COEF_FIVE * alpha_b * alpha_b)
    times_b(g_b, t_b, alpha_b)
    line_b = rows_of(xb[at(core, rows_b), :], scale_b)
    times_b(t_b, g_b, 1.0)
    square_b(g_b, COEF_THREE, COEF_FIVE)
    for p, ring in enumerate(large):
        ring.second()
        forward += [send_to(g_large(p, lax.rem(ring.index + k, 4)), partner) for k in (0, 3, 1)]
    times_b(g_b, t_b, 1.0)
    line_b = rows_of(line_b, 1.0)
    times_b(t_b, g_b, 1.0)
    for p, ring in enumerate(large):
        ring.finish()
        forward.append(send_to(g_large(p, lax.rem(ring.index + 2, 4)), partner))
    square_b(g_b, COEF_THREE, COEF_FIVE)
    t_b[0:rows_b, :] = line_b
    for p in range(2):
        cols = spot(p * 512 + place * 128, 128, 128)
        last_b = COEF_ONE * t_b[0:rows_b, cols].astype(jnp.float32) + dot(line_b, m_b[:, cols])
        results_b[:, at(p, 128)] = last_b.astype(BF)
    store(results_b, branch_out)
    for copy in forward:
        copy.wait_recv()

    def assemble(r, sums):
        value = panels[lax.div(r, 4), lax.rem(r, 4)]
        squares, diagonal = sums
        for d in range(5):
            block = value[:, d * 256 : d * 256 + 256]
            column = at(lax.rem(r + d, 8), 256)
            a[at(r, 256), column] = block
            if 0 < d < 4:
                a[column, at(r, 256)] = block.T
            wide = block.astype(jnp.float32)
            weight = 2.0 if 0 < d < 4 else 1.0
            squares = squares + weight * jnp.sum((wide * wide).reshape(32, 8, 256), axis=0)
        for k in range(2):
            corner = value[k * 128 : k * 128 + 128, k * 128 : k * 128 + 128].astype(jnp.float32)
            diagonal = diagonal + jnp.where(same, corner, 0.0)
        return squares, diagonal

    sums = lax.fori_loop(0, 8, assemble, (jnp.zeros((8, 256), jnp.float32), jnp.zeros((128, 128), jnp.float32)))
    alpha, scale = coefficients(jnp.sum(sums[0]), jnp.sum(sums[1]))


    def h(q):
        return at(2 * core + q, BLOCK)

    def o(q):
        return at(2 * other + q, BLOCK)

    def flip(q):
        return lax.rem(q + core, 2)

    def flop(q):
        return lax.rem(q + other, 2)

    def pair(ref, target, k, q):
        return pltpu.make_async_remote_copy(
            src_ref=ref, dst_ref=target, send_sem=send.at[k, q], recv_sem=recv.at[k, q], device_id=partner, device_id_type=MESH
        )

    def cross_out(buf, k, q):
        ref = buf.at[o(q), h(flip(q))]
        return pair(ref, ref, k, q)

    def cross_in(buf, k, q):
        ref = buf.at[h(q), o(flop(q))]
        return pair(ref, ref, k, q)

    def square_out(buf, k, q, side):
        first = at(2 * side, BLOCK)
        second = at(2 * side + 1, BLOCK)
        ref = (buf.at[first, at(side, HALF)], buf.at[second, first], buf.at[second, second])[q]
        return pair(ref, ref, k, 2 + q)

    def stage_out(k, q):
        return pair(m.at[o(q), at(flip(q), BLOCK)], stage.at[q], 4 + k, q)

    def receive_cross(left, k):
        def step(q, _):
            cross_out(left, k, q).wait_send()
            cross_in(left, k, q).wait_recv()
            left[o(flop(q)), h(q)] = left[h(q), o(flop(q))].T
            return 0

        lax.fori_loop(0, 2, step, 0)

    def receive_square(left, k):
        for q in range(3):
            square_out(left, k, q, core).wait_send()
            square_out(left, k, q, other).wait_recv()

    def product(left, k, right, emit, after_head, after_cross, after_all):
        if k is not None:
            receive_cross(left, k)

        def head(q, _):
            emit(h(q), 0, dot(left[h(q), :], right(0)))
            return 0

        lax.fori_loop(0, 2, head, 0)
        after_head()
        if k is not None:
            receive_square(left, k)

        def cross(q, _):
            j = flip(q)
            emit(o(q), j, dot(left[o(q), :], right(j)))
            after_cross(q)
            return 0

        lax.fori_loop(0, 2, cross, 0)
        emit(h(1), 1, dot(left[h(1), :], right(1)))
        after_all()

    def square(left, k, k_out, low, high):
        def emit(where, j, value):
            value = low * left[where, h(j)].astype(jnp.float32) + high * value
            m[where, at(j, BLOCK)] = value.astype(BF)

        def after_head():
            m[h(0), at(1, BLOCK)] = m[h(1), at(0, BLOCK)].T

        def after_cross(q):
            stage_out(k_out, q).start()

        def right(j):
            return left[:, h(j)]

        product(left, k, right, emit, after_head, after_cross, lambda: None)

        def receive(q, _):
            copy = stage_out(k_out, q)
            copy.wait_send()
            copy.wait_recv()
            m[o(flop(q)), at(q, BLOCK)] = stage[q].T
            return 0

        lax.fori_loop(0, 2, receive, 0)

    def times(left, k, out, k_out, factor):
        def emit(where, j, value):
            value = COEF_ONE * left[where, h(j)].astype(jnp.float32) + value
            if factor is not None:
                value = factor * value
            out[where, h(j)] = value.astype(BF)

        def after_head():
            out[h(0), h(1)] = out[h(1), h(0)].T
            square_out(out, k_out, 0, core).start()
            square_out(out, k_out, 1, core).start()

        def after_cross(q):
            cross_out(out, k_out, q).start()
            out[h(flip(q)), o(q)] = out[o(q), h(flip(q))].T

        def after_all():
            square_out(out, k_out, 2, core).start()

        def right(j):
            return m[:, at(j, BLOCK)]

        product(left, k, right, emit, after_head, after_cross, after_all)

    square(a, None, 0, COEF_THREE * alpha, COEF_FIVE * alpha * alpha)
    times(a, None, b, 0, alpha)
    x1[:, mine] = (scale * (COEF_ONE * x0[:, mine].astype(jnp.float32) + dot(x0[...], m[...]))).astype(BF)
    turn_one = send_to(x1.at[:, mine], partner)
    times(b, 0, c, 1, None)
    square(c, 1, 1, COEF_THREE, COEF_FIVE)
    times(c, None, b, 2, None)
    turn_one.wait_recv()
    x2[:, mine] = (COEF_ONE * x1[:, mine].astype(jnp.float32) + dot(x1[...], m[...])).astype(BF)
    turn_two = send_to(x2.at[:, mine], partner)
    times(b, 2, a, 3, None)

    def some(block, low, high):
        close = spot(core * HALF + block * 256, 256, 256)

        def step(r, _):
            where = at(lax.rem(2 * core + r, 4), BLOCK)
            value = COEF_THREE * a[where, close].astype(jnp.float32) + COEF_FIVE * dot(a[where, :], a[:, close])
            m[where, at(block, 256)] = value.astype(BF)
            return 0

        lax.fori_loop(low, high, step, 0)

    def last(where, block):
        cols = at(block, 256)
        close = spot(core * HALF + block * 256, 256, 256)
        return (COEF_ONE * x2[where, close].astype(jnp.float32) + dot(x2[where, :], m[:, cols])).astype(BF)

    receive_cross(a, 3)
    some(ahead, 0, 2)
    receive_square(a, 3)
    some(ahead, 2, 4)
    turn_two.wait_recv()
    final[2] = last(pl.ds(0, rows), ahead)
    to_ahead = pltpu.make_async_remote_copy(
        src_ref=final.at[2], dst_ref=final.at[4 + core], send_sem=sems.at[COPIES], recv_sem=recvs.at[COPIES + core],
        device_id={"tp": ahead, "rep": 0}, device_id_type=MESH,
    )
    to_ahead.start()
    some(behind, 0, 4)
    final[3] = last(pl.ds(rows, rows), behind)
    to_behind = pltpu.make_async_remote_copy(
        src_ref=final.at[3], dst_ref=final.at[4 + core], send_sem=sems.at[COPIES + 1], recv_sem=recvs.at[COPIES + core],
        device_id={"tp": behind, "rep": 1}, device_id_type=MESH,
    )
    to_behind.start()
    some(place, 0, 4)
    final[6] = last(other_rows, place)
    to_partner = remote(final.at[6], final.at[core], partner)
    to_partner.start()
    final[core] = last(own_rows, place)
    to_partner.wait_recv()
    for i in range(2):
        pltpu.make_async_remote_copy(
            src_ref=final.at[2], dst_ref=final.at[4 + i], send_sem=sems.at[COPIES], recv_sem=recvs.at[COPIES + i],
            device_id=partner, device_id_type=MESH,
        ).wait_recv()
    for i in range(2):
        cols = pl.ds(i * 256, 256)
        results[kind, :, cols] = final[i]
        results[1 - kind, :, cols] = final[4 + i]
    store(results.at[0], gate_out)
    store(results.at[1], up_out)
    to_ahead.wait_send()
    to_behind.wait_send()
    for copy in used:
        copy.wait_send()
    for copy in stores:
        copy.wait()


def finish_kernel(*refs):
    ins, outs, stage, fresh, in_sem, out_sem = refs[:9], refs[9:15], refs[15:24], refs[24:27], refs[27], refs[28]
    loads = [pltpu.make_async_copy(ins[i], stage[i], in_sem.at[i]) for i in range(9)]
    for i in (3, 6, 4, 7, 5, 8, 0, 1, 2):
        loads[i].start()
    stores = []

    def store(source, target):
        copy = pltpu.make_async_copy(source, target, out_sem.at[len(stores)])
        copy.start()
        stores.append(copy)

    for i, height in enumerate((FF, FF, D)):
        loads[3 + i].wait()
        loads[6 + i].wait()
        fresh[i][...] = SHRINK * stage[6 + i][...] - RATE * math.sqrt(height) * stage[3 + i][...].astype(jnp.float32)
        store(fresh[i], outs[2 * i + 1])
    for i in range(3):
        loads[i].wait()
        store(stage[i], outs[2 * i])
    for copy in stores:
        copy.wait()


def local(*args):
    velocities = (args[1], args[4], args[7])
    shapes = [velocity.shape for velocity in velocities]
    (rows, width), (rows_b, width_b) = shapes[0], shapes[2]
    anywhere = pl.BlockSpec(memory_space=pl.ANY)
    dma = pltpu.SemaphoreType.DMA

    def buf(*shape):
        return pltpu.VMEM(shape, BF)

    def full(*shape):
        return pltpu.VMEM(shape, jnp.float32)

    outs = [jax.ShapeDtypeStruct(shape, kind) for kind in (jnp.float32, BF) for shape in shapes]
    middle = pl.pallas_call(
        kernel,
        out_shape=outs,
        in_specs=[anywhere] * 6,
        out_specs=[anywhere] * 6,
        scratch_shapes=[
            full(2, 2, rows, width), full(2, rows_b, width_b), full(2, rows, width), full(rows_b, width_b),
            buf(2, rows, width), buf(rows_b, width_b), dma((9,)), dma((6,)),
            buf(N, N), buf(N, N), buf(N, N), buf(N, HALF),
            buf(2 * rows, N), buf(2 * rows_b, NB), buf(2 * rows, N), buf(2 * rows, N), buf(7, rows, 256),
            buf(2, 2, rows, 256), buf(2, rows, 256),
            buf(2, rows, width), buf(2, rows, width), buf(rows_b, width_b), buf(rows_b, width_b),
            buf(2, 256, 1280), buf(2, 2, 3, 64, 640), buf(2, 2, 64, 640), buf(2, 2, 3, 16, 640),
            buf(2, 4, 256, 1280),
            buf(128, NB), buf(2, 3, 16, NB), buf(2, 16, NB), buf(2, 3, 16, 256), buf(8, 128, NB),
            buf(NB, NB), buf(NB, NB), buf(NB, NB),
            buf(2, BLOCK, BLOCK),
            dma((COPIES + 2,)), dma((COPIES + 2,)), dma((7, 5)), dma((7, 5)),
        ],
        compiler_params=pltpu.CompilerParams(collective_id=0, has_side_effects=True, vmem_limit_bytes=62 * 1024 * 1024),
    )(args[0], args[3], args[6], args[1], args[4], args[7])
    results = [jax.ShapeDtypeStruct(shape, jnp.float32) for shape in shapes for _ in range(2)]
    stage = [full(*shape) for shape in shapes] + [buf(*shape) for shape in shapes] + [full(*shape) for shape in shapes] * 2
    return pl.pallas_call(
        finish_kernel,
        out_shape=results,
        in_specs=[anywhere] * 9,
        out_specs=[anywhere] * 6,
        scratch_shapes=stage + [dma((9,)), dma((6,))],
    )(*middle, args[2], args[5], args[8])


def solution(mesh):
    torus = Mesh(
        mesh.devices.reshape(4, 4, mesh.shape["tp"], mesh.shape["rep"]),
        ("fs_0", "fs_1", "tp", "rep"),
    )
    grads, plain = P("rep", FS, "tp"), P(FS_REP, "tp")
    return jax.shard_map(
        local,
        mesh=torus,
        in_specs=(grads, plain, plain) * 3,
        out_specs=(plain,) * 6,
        check_vma=False,
    )
```

```python
import functools
import math

import jax
import jax.numpy as jnp
from jax import lax
from jax.experimental import pallas as pl
from jax.experimental.pallas import tpu as pltpu
from jax.sharding import Mesh
from jax.sharding import PartitionSpec as P

D = 2048
FF = 5632
FS_REP = ("fs_0", "fs_1", "rep")
FS = ("fs_0", "fs_1")

MOMENT = 0.95
COEF_ONE = 3.4445
COEF_THREE = -4.775
COEF_FIVE = 2.0315
SAFETY = 2.0
RATE = 0.5
SHRINK = 0.95
BF = jnp.bfloat16


def dot(a, b):
    return jnp.dot(a, b, preferred_element_type=jnp.float32)


N = 2048
HALF = 1024
BLOCK = 512
NB = 1024
COPIES = 160
MESH = pl.DeviceIdType.MESH


def at(index, size):
    return pl.ds(index * size if isinstance(index, int) else pl.multiple_of(index * size, size), size)


def spot(offset, size, unit):
    return pl.ds(pl.multiple_of(offset, unit), size)


def turned(a, b):
    return lax.dot_general(a, b, (((0,), (0,)), ((), ())), preferred_element_type=jnp.float32)


def kernel(
    gate_g, up_g, branch_g, gate_v, up_v, branch_v,
    gate_m, up_m, branch_m, gate_out, up_out, branch_out,
    grads, grads_b, speed, speed_b, results, results_b, in_sem, out_sem,
    a, b, c, m, x0, xb, x1, x2, final, starts, relay,
    give, take, give_b, take_b,
    part, near, kept, near2, panels,
    part_b, near_b, kept_b, near2_b, gram_b, m_b, t_b, g_b,
    stage, sems, recvs, send, recv,
):
    core = lax.axis_index("rep")
    place = lax.axis_index("tp")
    iy = lax.axis_index("fs_1")
    iz = lax.axis_index("fs_0")
    other = 1 - core
    kind = lax.rem(place, 2)
    ahead = lax.rem(place + 1, 4)
    behind = lax.rem(place + 3, 4)
    across = lax.rem(place + 2, 4)
    rows = gate_v.shape[0]
    rows_b = branch_v.shape[0]
    loads = []

    def load(source, target):
        copy = pltpu.make_async_copy(source, target, in_sem.at[len(loads)])
        copy.start()
        loads.append(copy)

    load(branch_g.at[0, at(other, rows_b)], grads_b.at[1])
    load(gate_g.at[0, at(other, rows)], grads.at[0, 1])
    load(up_g.at[0, at(other, rows)], grads.at[1, 1])
    load(branch_g.at[0, at(core, rows_b)], grads_b.at[0])
    load(branch_v, speed_b)
    load(gate_g.at[0, at(core, rows)], grads.at[0, 0])
    load(gate_v, speed.at[0])
    load(up_g.at[0, at(core, rows)], grads.at[1, 0])
    load(up_v, speed.at[1])
    mine = at(core, HALF)
    partner = {"rep": other}
    used = []

    def turn(axis, index, step):
        return {axis: lax.rem(index + step, 4)}

    def remote(src, dst, to):
        k = len(used)
        copy = pltpu.make_async_remote_copy(
            src_ref=src, dst_ref=dst, send_sem=sems.at[k], recv_sem=recvs.at[k], device_id=to, device_id_type=MESH
        )
        used.append(copy)
        return copy

    def send_to(ref, to):
        copy = remote(ref, ref, to)
        copy.start()
        return copy

    barrier = pltpu.get_barrier_semaphore()
    peers = [partner, {"tp": across}]
    peers += [{"tp": x, "rep": r} for x in (ahead, behind) for r in range(2)]
    peers += [turn(axis, index, step) for axis, index in (("fs_1", iy), ("fs_0", iz)) for step in (1, 2, 3)]
    for to in peers:
        pl.semaphore_signal(barrier, inc=1, device_id=to, device_id_type=MESH)

    own_rows, other_rows = at(core, rows), at(other, rows)
    loads[0].wait()
    give_b[...] = grads_b[1].astype(BF)
    for i in range(2):
        loads[1 + i].wait()
        give[i] = grads[i, 1].astype(BF)
    pl.semaphore_wait(barrier, len(peers))
    first_copies = [remote(give_b, take_b, partner)]
    first_copies += [remote(give.at[i], take.at[i], partner) for i in range(2)]
    for copy in first_copies:
        copy.start()
    same = lax.broadcasted_iota(jnp.int32, (128, 128), 0) == lax.broadcasted_iota(jnp.int32, (128, 128), 1)

    def columns(ref, lines, height, width):
        def block(x, part):
            return ref.at[at(core, height), spot(part * 4 * width + x * width, width, width)]

        state = {}

        def start():
            state["right"] = [send_to(block(place, p), {"tp": ahead}) for p in range(2)]
            state["left"] = [send_to(block(place, p), {"tp": behind}) for p in range(2)]
            state["own"] = [send_to(block(place, p), partner) for p in range(2)]

        def second():
            state["right"][0].wait_recv()
            far = [send_to(block(behind, 0), {"tp": ahead})]
            state["left"][1].wait_recv()
            far.append(send_to(block(ahead, 1), {"tp": behind}))
            state["far"] = far
            state["own"].append(send_to(block(behind, 0), partner))
            state["own"].append(send_to(block(ahead, 1), partner))
            state["right"][1].wait_recv()
            state["own"].append(send_to(block(behind, 1), partner))
            state["left"][0].wait_recv()
            state["own"].append(send_to(block(ahead, 0), partner))

        def finish():
            for p in range(2):
                state["far"][p].wait_recv()
                state["own"].append(send_to(block(across, p), partner))
            for copy in state["own"]:
                copy.wait_recv()

        return start, second, finish

    lines = [columns(xb, None, rows_b, 128)]
    line = {}

    def block_of(x, p):
        return x0.at[own_rows, spot(p * HALF + x * 256, 256, 256)]

    def line_start():
        line["relay"] = [
            remote(starts.at[kind, p], relay.at[p], {"tp": to}) for p, to in ((0, ahead), (1, behind))
        ]
        line["out"] = [
            [remote(starts.at[1 - kind, p], block_of(place, p), {"tp": to}) for p in range(2)] for to in (ahead, behind)
        ]
        for copy in line["relay"] + line["out"][0] + line["out"][1]:
            copy.start()
        line["own"] = [send_to(block_of(place, p), partner) for p in range(2)]

    def line_second():
        line["far"] = []
        for p, (source, to) in enumerate(((behind, ahead), (ahead, behind))):
            line["relay"][p].wait_recv()
            copy = remote(relay.at[p], block_of(source, p), {"tp": to})
            copy.start()
            line["far"].append(copy)

    def line_third():
        for side, source in ((0, behind), (1, ahead)):
            for p in range(2):
                line["out"][side][p].wait_recv()
                line["own"].append(send_to(block_of(source, p), partner))

    def line_finish():
        for p in range(2):
            line["far"][p].wait_recv()
            line["own"].append(send_to(block_of(across, p), partner))
        for copy in line["own"]:
            copy.wait_recv()

    first_copies[0].wait_recv()
    loads[3].wait()
    loads[4].wait()
    moment = MOMENT * speed_b[...] + (grads_b[0] + take_b[...].astype(jnp.float32))
    speed_b[...] = moment
    for p in range(2):
        xb[at(core, rows_b), spot(p * 512 + place * 128, 128, 128)] = moment[:, p * 128 : p * 128 + 128].astype(BF)
    lines[0][0]()
    for i in range(2):
        first_copies[1 + i].wait_recv()
        loads[5 + 2 * i].wait()
        loads[6 + 2 * i].wait()
        moment = MOMENT * speed[i] + (grads[i, 0] + take[i].astype(jnp.float32))
        speed[i] = moment
        for p in range(2):
            starts[i, p] = moment[:, p * 256 : p * 256 + 256].astype(BF)
    for p in range(2):
        x0[own_rows, spot(p * HALF + place * 256, 256, 256)] = starts[kind, p]
    line_start()
    stores = []

    def store(source, target):
        copy = pltpu.make_async_copy(source, target, out_sem.at[len(stores)])
        copy.start()
        stores.append(copy)

    axes = ((("fs_1", iy), ("fs_0", iz)), (("fs_0", iz), ("fs_1", iy)))

    def exchange(source, landing, axis, index):
        copies = []
        for step in (2, 1, 3):
            to = lax.rem(index + step, 4)
            copies.append(remote(source(to), landing.at[step - 1], {axis: to}))
            copies[-1].start()
        return copies

    def total(own, landing, copies):
        for copy in copies:
            copy.wait_recv()
        value = own.astype(jnp.float32)
        for k in range(3):
            value = value + landing[k].astype(jnp.float32)
        return value.astype(BF)

    def scatter_one(source, landings):
        return [
            exchange(functools.partial(source, p), landings[p], *axes[p][0]) for p in range(2)
        ]

    def source_of(i):
        return lambda p, t: part.at[i, at(t, 64), at(p, 640)]

    def source_b(p, t):
        return part_b.at[spot(p * 64 + t * 16, 16, 16), :]

    upper = lax.div(place, 2)

    def panel(i):
        first = core * 4 + 2 * upper + i
        own = x0[:, at(first, 256)]
        for d in range(5):
            part[i, :, at(d, 256)] = turned(own, x0[:, at(lax.rem(first + d, 8), 256)]).astype(BF)
        return scatter_one(source_of(i), [near.at[i, p] for p in range(2)])

    def gram_rows(p, i1):
        return spot(p * 64 + i1 * 16, 16, 16)

    group = at(core, 4)

    class Ring:
        def __init__(self, axis, index, block, cut):
            self.next, self.prev = turn(axis, index, 1), turn(axis, index, 3)
            self.index, self.block, self.cut = index, block, cut

        def start(self):
            ref = self.block(self.index)
            self.right = send_to(ref, self.next)
            self.left = send_to(ref, self.prev)

        def second(self):
            self.right.wait_recv()
            self.far = [send_to(self.cut(lax.rem(self.index + 3, 4), 0), self.next)]
            self.left.wait_recv()
            self.far.append(send_to(self.cut(lax.rem(self.index + 1, 4), 1), self.prev))

        def finish(self):
            for copy in self.far:
                copy.wait_recv()

    def rings(phase, block, cut):
        return [
            Ring(*axes[p][phase], functools.partial(block, p), functools.partial(cut, p)) for p in range(2)
        ]

    def b_small(p, j):
        return gram_b.at[group, gram_rows(p, axes[p][0][1]), at(j, 256)]

    def b_small_cut(p, j, h):
        return gram_b.at[at(core * 2 + h, 2), gram_rows(p, axes[p][0][1]), at(j, 256)]

    def b_large(p, j):
        return gram_b.at[group, gram_rows(p, j), :]

    def b_large_cut(p, j, h):
        return gram_b.at[at(core * 2 + h, 2), gram_rows(p, j), :]

    def g_rows(p, j):
        return spot(axes[p][0][1] * 64 + j * 16, 16, 16)

    def g_small(p, j):
        return panels.at[core, :, g_rows(p, j), at(p, 640)]

    def g_small_cut(p, j, h):
        return panels.at[core, at(h, 2), g_rows(p, j), at(p, 640)]

    def g_large(p, j):
        return panels.at[core, :, at(j, 64), at(p, 640)]

    def g_large_cut(p, j, h):
        return panels.at[core, at(h, 2), at(j, 64), at(p, 640)]

    small_b, large_b = rings(1, b_small, b_small_cut), rings(0, b_large, b_large_cut)
    small, large = rings(1, g_small, g_small_cut), rings(0, g_large, g_large_cut)
    lines[0][1]()
    line_second()
    lines[0][2]()
    part_b[...] = turned(xb[:, spot(core * 512 + place * 128, 128, 128)], xb[...]).astype(BF)
    one_b = scatter_one(source_b, [near_b.at[p] for p in range(2)])
    line_third()
    for source, target in ((speed_b, branch_m), (speed.at[0], gate_m), (speed.at[1], up_m)):
        store(source, target)
    two_b = []
    for p in range(2):
        kept_b[p] = total(part_b[spot(p * 64 + axes[p][0][1] * 16, 16, 16), :], near_b.at[p], one_b[p])
        two_b.append(exchange(lambda t, p=p: kept_b.at[p, :, at(t, 256)], near2_b.at[p], *axes[p][1]))
    line_finish()
    ones = [panel(0), panel(1)]
    swaps_b = []
    for p in range(2):
        i1, i2 = axes[p][0][1], axes[p][1][1]
        gram_b[core * 4 + place, gram_rows(p, i1), at(i2, 256)] = total(
            kept_b[p, :, at(i2, 256)], near2_b.at[p], two_b[p]
        )
        ref = gram_b.at[core * 4 + place, gram_rows(p, i1), at(i2, 256)]
        swaps_b.append([send_to(ref, {"tp": x}) for x in (across, ahead, behind)])

    def scatter_two(i):
        pair = []
        for p in range(2):
            index = axes[p][0][1]
            kept[i, p] = total(part[i, at(index, 64), at(p, 640)], near.at[i, p], ones[i][p])
            pair.append(exchange(lambda t, p=p: kept.at[i, p, at(t, 16), :], near2.at[i, p], *axes[p][1]))
        return pair

    for p in range(2):
        for copy in swaps_b[p]:
            copy.wait_recv()
        small_b[p].start()
    twos = [scatter_two(0), scatter_two(1)]
    for ring in small_b:
        ring.second()
    swaps = []
    for p in range(2):
        i2 = axes[p][1][1]
        for i in range(2):
            panels[core, 2 * upper + i, g_rows(p, i2), at(p, 640)] = total(
                kept[i, p, at(i2, 16), :], near2.at[i, p], twos[i][p]
            )
        swaps.append(send_to(panels.at[core, at(upper, 2), g_rows(p, i2), at(p, 640)], {"tp": across}))
    for ring in small_b:
        ring.finish()
    for ring in large_b:
        ring.start()
    for copy, ring in zip(swaps, small):
        copy.wait_recv()
        ring.start()
    forward_b, forward = [], []
    for p, ring in enumerate(large_b):
        ring.second()
        forward_b += [send_to(b_large(p, lax.rem(ring.index + k, 4)), partner) for k in (0, 3, 1)]
    for ring in small:
        ring.second()
    for ring in small:
        ring.finish()
    for ring in large:
        ring.start()
    for p, ring in enumerate(large_b):
        ring.finish()
        forward_b.append(send_to(b_large(p, lax.rem(ring.index + 2, 4)), partner))
    for copy in forward_b:
        copy.wait_recv()

    def coefficients(squares, diagonal):
        second = jnp.full((1, 1), squares)
        first = jnp.full((1, 1), diagonal)
        ratio = SAFETY * (second + 1.0) / (first + 1.0)
        return 1.0 / ratio, lax.rsqrt(ratio)

    def squares_b(i, sums):
        value = gram_b[i].astype(jnp.float32)
        diagonal = gram_b[i, :, at(i, 128)].astype(jnp.float32)
        return (
            sums[0] + jnp.sum((value * value).reshape(16, 8, NB), axis=0),
            sums[1] + jnp.where(same, diagonal, 0.0),
        )

    sums = lax.fori_loop(0, 8, squares_b, (jnp.zeros((8, NB), jnp.float32), jnp.zeros((128, 128), jnp.float32)))
    alpha_b, scale_b = coefficients(jnp.sum(sums[0]), jnp.sum(sums[1]))

    top, low_half = pl.ds(0, 512), pl.ds(512, 512)

    def mirrored_b(left, right, out, emit):
        out[top, top] = emit(left[top, top], dot(left[top, :], right[:, top])).astype(BF)
        out[low_half, :] = emit(left[low_half, :], dot(left[low_half, :], right[...])).astype(BF)
        out[top, low_half] = out[low_half, top].T

    def square_b(left, low, high):
        mirrored_b(left, left, m_b, lambda own, value: low * own.astype(jnp.float32) + high * value)

    def times_b(left, out, factor):
        mirrored_b(left, m_b, out, lambda own, value: factor * (COEF_ONE * own.astype(jnp.float32) + value))

    def rows_of(left, factor):
        return (factor * (COEF_ONE * left.astype(jnp.float32) + dot(left, m_b[...]))).astype(BF)

    for i in range(8):
        g_b[at(i, 128), :] = gram_b[i]
    square_b(g_b, COEF_THREE * alpha_b, COEF_FIVE * alpha_b * alpha_b)
    times_b(g_b, t_b, alpha_b)
    line_b = rows_of(xb[at(core, rows_b), :], scale_b)
    times_b(t_b, g_b, 1.0)
    square_b(g_b, COEF_THREE, COEF_FIVE)
    for p, ring in enumerate(large):
        ring.second()
        forward += [send_to(g_large(p, lax.rem(ring.index + k, 4)), partner) for k in (0, 3, 1)]
    times_b(g_b, t_b, 1.0)
    line_b = rows_of(line_b, 1.0)
    times_b(t_b, g_b, 1.0)
    for p, ring in enumerate(large):
        ring.finish()
        forward.append(send_to(g_large(p, lax.rem(ring.index + 2, 4)), partner))
    square_b(g_b, COEF_THREE, COEF_FIVE)
    t_b[0:rows_b, :] = line_b
    for p in range(2):
        cols = spot(p * 512 + place * 128, 128, 128)
        last_b = COEF_ONE * t_b[0:rows_b, cols].astype(jnp.float32) + dot(line_b, m_b[:, cols])
        results_b[:, at(p, 128)] = last_b.astype(BF)
    store(results_b, branch_out)
    for copy in forward:
        copy.wait_recv()

    def assemble(r, sums):
        value = panels[lax.div(r, 4), lax.rem(r, 4)]
        squares, diagonal = sums
        for d in range(5):
            block = value[:, d * 256 : d * 256 + 256]
            column = at(lax.rem(r + d, 8), 256)
            a[at(r, 256), column] = block
            if 0 < d < 4:
                a[column, at(r, 256)] = block.T
            wide = block.astype(jnp.float32)
            weight = 2.0 if 0 < d < 4 else 1.0
            squares = squares + weight * jnp.sum((wide * wide).reshape(32, 8, 256), axis=0)
        for k in range(2):
            corner = value[k * 128 : k * 128 + 128, k * 128 : k * 128 + 128].astype(jnp.float32)
            diagonal = diagonal + jnp.where(same, corner, 0.0)
        return squares, diagonal

    sums = lax.fori_loop(0, 8, assemble, (jnp.zeros((8, 256), jnp.float32), jnp.zeros((128, 128), jnp.float32)))
    alpha, scale = coefficients(jnp.sum(sums[0]), jnp.sum(sums[1]))


    def h(q):
        return at(2 * core + q, BLOCK)

    def o(q):
        return at(2 * other + q, BLOCK)

    def flip(q):
        return lax.rem(q + core, 2)

    def flop(q):
        return lax.rem(q + other, 2)

    def pair(ref, target, k, q):
        return pltpu.make_async_remote_copy(
            src_ref=ref, dst_ref=target, send_sem=send.at[k, q], recv_sem=recv.at[k, q], device_id=partner, device_id_type=MESH
        )

    def cross_out(buf, k, q):
        ref = buf.at[o(q), h(flip(q))]
        return pair(ref, ref, k, q)

    def cross_in(buf, k, q):
        ref = buf.at[h(q), o(flop(q))]
        return pair(ref, ref, k, q)

    def square_out(buf, k, q, side):
        first = at(2 * side, BLOCK)
        second = at(2 * side + 1, BLOCK)
        ref = (buf.at[first, at(side, HALF)], buf.at[second, first], buf.at[second, second])[q]
        return pair(ref, ref, k, 2 + q)

    def stage_out(k, q):
        return pair(m.at[o(q), at(flip(q), BLOCK)], stage.at[q], 4 + k, q)

    def receive_cross(left, k):
        def step(q, _):
            cross_out(left, k, q).wait_send()
            cross_in(left, k, q).wait_recv()
            left[o(flop(q)), h(q)] = left[h(q), o(flop(q))].T
            return 0

        lax.fori_loop(0, 2, step, 0)

    def receive_square(left, k):
        for q in range(3):
            square_out(left, k, q, core).wait_send()
            square_out(left, k, q, other).wait_recv()

    def product(left, k, right, emit, after_head, after_cross, after_all):
        if k is not None:
            receive_cross(left, k)

        def head(q, _):
            emit(h(q), 0, dot(left[h(q), :], right(0)))
            return 0

        lax.fori_loop(0, 2, head, 0)
        after_head()
        if k is not None:
            receive_square(left, k)

        def cross(q, _):
            j = flip(q)
            emit(o(q), j, dot(left[o(q), :], right(j)))
            after_cross(q)
            return 0

        lax.fori_loop(0, 2, cross, 0)
        emit(h(1), 1, dot(left[h(1), :], right(1)))
        after_all()

    def square(left, k, k_out, low, high):
        def emit(where, j, value):
            value = low * left[where, h(j)].astype(jnp.float32) + high * value
            m[where, at(j, BLOCK)] = value.astype(BF)

        def after_head():
            m[h(0), at(1, BLOCK)] = m[h(1), at(0, BLOCK)].T

        def after_cross(q):
            stage_out(k_out, q).start()

        def right(j):
            return left[:, h(j)]

        product(left, k, right, emit, after_head, after_cross, lambda: None)

        def receive(q, _):
            copy = stage_out(k_out, q)
            copy.wait_send()
            copy.wait_recv()
            m[o(flop(q)), at(q, BLOCK)] = stage[q].T
            return 0

        lax.fori_loop(0, 2, receive, 0)

    def times(left, k, out, k_out, factor):
        def emit(where, j, value):
            value = COEF_ONE * left[where, h(j)].astype(jnp.float32) + value
            if factor is not None:
                value = factor * value
            out[where, h(j)] = value.astype(BF)

        def after_head():
            out[h(0), h(1)] = out[h(1), h(0)].T
            square_out(out, k_out, 0, core).start()
            square_out(out, k_out, 1, core).start()

        def after_cross(q):
            cross_out(out, k_out, q).start()
            out[h(flip(q)), o(q)] = out[o(q), h(flip(q))].T

        def after_all():
            square_out(out, k_out, 2, core).start()

        def right(j):
            return m[:, at(j, BLOCK)]

        product(left, k, right, emit, after_head, after_cross, after_all)

    square(a, None, 0, COEF_THREE * alpha, COEF_FIVE * alpha * alpha)
    times(a, None, b, 0, alpha)
    x1[:, mine] = (scale * (COEF_ONE * x0[:, mine].astype(jnp.float32) + dot(x0[...], m[...]))).astype(BF)
    turn_one = send_to(x1.at[:, mine], partner)
    times(b, 0, c, 1, None)
    square(c, 1, 1, COEF_THREE, COEF_FIVE)
    times(c, None, b, 2, None)
    turn_one.wait_recv()
    x2[:, mine] = (COEF_ONE * x1[:, mine].astype(jnp.float32) + dot(x1[...], m[...])).astype(BF)
    turn_two = send_to(x2.at[:, mine], partner)
    times(b, 2, a, 3, None)

    def some(block, low, high):
        close = spot(core * HALF + block * 256, 256, 256)

        def step(r, _):
            where = at(lax.rem(2 * core + r, 4), BLOCK)
            value = COEF_THREE * a[where, close].astype(jnp.float32) + COEF_FIVE * dot(a[where, :], a[:, close])
            m[where, at(block, 256)] = value.astype(BF)
            return 0

        lax.fori_loop(low, high, step, 0)

    def last(where, block):
        cols = at(block, 256)
        close = spot(core * HALF + block * 256, 256, 256)
        return (COEF_ONE * x2[where, close].astype(jnp.float32) + dot(x2[where, :], m[:, cols])).astype(BF)

    receive_cross(a, 3)
    some(ahead, 0, 2)
    receive_square(a, 3)
    some(ahead, 2, 4)
    turn_two.wait_recv()
    final[2] = last(pl.ds(0, rows), ahead)
    to_ahead = pltpu.make_async_remote_copy(
        src_ref=final.at[2], dst_ref=final.at[4 + core], send_sem=sems.at[COPIES], recv_sem=recvs.at[COPIES + core],
        device_id={"tp": ahead, "rep": 0}, device_id_type=MESH,
    )
    to_ahead.start()
    some(behind, 0, 4)
    final[3] = last(pl.ds(rows, rows), behind)
    to_behind = pltpu.make_async_remote_copy(
        src_ref=final.at[3], dst_ref=final.at[4 + core], send_sem=sems.at[COPIES + 1], recv_sem=recvs.at[COPIES + core],
        device_id={"tp": behind, "rep": 1}, device_id_type=MESH,
    )
    to_behind.start()
    some(place, 0, 4)
    final[6] = last(other_rows, place)
    to_partner = remote(final.at[6], final.at[core], partner)
    to_partner.start()
    final[core] = last(own_rows, place)
    to_partner.wait_recv()
    for i in range(2):
        pltpu.make_async_remote_copy(
            src_ref=final.at[2], dst_ref=final.at[4 + i], send_sem=sems.at[COPIES], recv_sem=recvs.at[COPIES + i],
            device_id=partner, device_id_type=MESH,
        ).wait_recv()
    for i in range(2):
        cols = pl.ds(i * 256, 256)
        results[kind, :, cols] = final[i]
        results[1 - kind, :, cols] = final[4 + i]
    store(results.at[0], gate_out)
    store(results.at[1], up_out)
    to_ahead.wait_send()
    to_behind.wait_send()
    for copy in used:
        copy.wait_send()
    for copy in stores:
        copy.wait()


def finish_kernel(*refs):
    ins, outs, stage, fresh, in_sem, out_sem = refs[:9], refs[9:15], refs[15:24], refs[24:27], refs[27], refs[28]
    loads = [pltpu.make_async_copy(ins[i], stage[i], in_sem.at[i]) for i in range(9)]
    for i in (3, 6, 4, 7, 5, 8, 0, 1, 2):
        loads[i].start()
    stores = []

    def store(source, target):
        copy = pltpu.make_async_copy(source, target, out_sem.at[len(stores)])
        copy.start()
        stores.append(copy)

    for i, height in enumerate((FF, FF, D)):
        loads[3 + i].wait()
        loads[6 + i].wait()
        fresh[i][...] = SHRINK * stage[6 + i][...] - RATE * math.sqrt(height) * stage[3 + i][...].astype(jnp.float32)
        store(fresh[i], outs[2 * i + 1])
    for i in range(3):
        loads[i].wait()
        store(stage[i], outs[2 * i])
    for copy in stores:
        copy.wait()


def local(*args):
    velocities = (args[1], args[4], args[7])
    shapes = [velocity.shape for velocity in velocities]
    (rows, width), (rows_b, width_b) = shapes[0], shapes[2]
    anywhere = pl.BlockSpec(memory_space=pl.ANY)
    dma = pltpu.SemaphoreType.DMA

    def buf(*shape):
        return pltpu.VMEM(shape, BF)

    def full(*shape):
        return pltpu.VMEM(shape, jnp.float32)

    outs = [jax.ShapeDtypeStruct(shape, kind) for kind in (jnp.float32, BF) for shape in shapes]
    middle = pl.pallas_call(
        kernel,
        out_shape=outs,
        in_specs=[anywhere] * 6,
        out_specs=[anywhere] * 6,
        scratch_shapes=[
            full(2, 2, rows, width), full(2, rows_b, width_b), full(2, rows, width), full(rows_b, width_b),
            buf(2, rows, width), buf(rows_b, width_b), dma((9,)), dma((6,)),
            buf(N, N), buf(N, N), buf(N, N), buf(N, HALF),
            buf(2 * rows, N), buf(2 * rows_b, NB), buf(2 * rows, N), buf(2 * rows, N), buf(7, rows, 256),
            buf(2, 2, rows, 256), buf(2, rows, 256),
            buf(2, rows, width), buf(2, rows, width), buf(rows_b, width_b), buf(rows_b, width_b),
            buf(2, 256, 1280), buf(2, 2, 3, 64, 640), buf(2, 2, 64, 640), buf(2, 2, 3, 16, 640),
            buf(2, 4, 256, 1280),
            buf(128, NB), buf(2, 3, 16, NB), buf(2, 16, NB), buf(2, 3, 16, 256), buf(8, 128, NB),
            buf(NB, NB), buf(NB, NB), buf(NB, NB),
            buf(2, BLOCK, BLOCK),
            dma((COPIES + 2,)), dma((COPIES + 2,)), dma((7, 5)), dma((7, 5)),
        ],
        compiler_params=pltpu.CompilerParams(collective_id=0, has_side_effects=True, vmem_limit_bytes=62 * 1024 * 1024),
    )(args[0], args[3], args[6], args[1], args[4], args[7])
    results = [jax.ShapeDtypeStruct(shape, jnp.float32) for shape in shapes for _ in range(2)]
    stage = [full(*shape) for shape in shapes] + [buf(*shape) for shape in shapes] + [full(*shape) for shape in shapes] * 2
    return pl.pallas_call(
        finish_kernel,
        out_shape=results,
        in_specs=[anywhere] * 9,
        out_specs=[anywhere] * 6,
        scratch_shapes=stage + [dma((9,)), dma((6,))],
    )(*middle, args[2], args[5], args[8])


def solution(mesh):
    torus = Mesh(
        mesh.devices.reshape(4, 4, mesh.shape["tp"], mesh.shape["rep"]),
        ("fs_0", "fs_1", "tp", "rep"),
    )
    grads, plain = P("rep", FS, "tp"), P(FS_REP, "tp")
    return jax.shard_map(
        local,
        mesh=torus,
        in_specs=(grads, plain, plain) * 3,
        out_specs=(plain,) * 6,
        check_vma=False,
    )
```

```python
import functools
import math

import jax
import jax.numpy as jnp
from jax import lax
from jax.experimental import pallas as pl
from jax.experimental.pallas import tpu as pltpu
from jax.sharding import Mesh
from jax.sharding import PartitionSpec as P

D = 2048
FF = 5632
FS_REP = ("fs_0", "fs_1", "rep")
FS = ("fs_0", "fs_1")

MOMENT = 0.95
COEF_ONE = 3.4445
COEF_THREE = -4.775
COEF_FIVE = 2.0315
SAFETY = 2.0
RATE = 0.5
SHRINK = 0.95
BF = jnp.bfloat16


def dot(a, b):
    return jnp.dot(a, b, preferred_element_type=jnp.float32)


N = 2048
HALF = 1024
BLOCK = 512
NB = 1024
COPIES = 160
MESH = pl.DeviceIdType.MESH


def at(index, size):
    return pl.ds(index * size if isinstance(index, int) else pl.multiple_of(index * size, size), size)


def spot(offset, size, unit):
    return pl.ds(pl.multiple_of(offset, unit), size)


def turned(a, b):
    return lax.dot_general(a, b, (((0,), (0,)), ((), ())), preferred_element_type=jnp.float32)


def kernel(
    gate_g, up_g, branch_g, gate_v, up_v, branch_v,
    gate_m, up_m, branch_m, gate_out, up_out, branch_out,
    grads, grads_b, speed, speed_b, results, results_b, in_sem, out_sem,
    pairs, b, m, xall, xb, final, starts, relay,
    give, take, give_b, take_b,
    part, near, kept, near2, panels,
    part_b, near_b, kept_b, near2_b, gram_b, m_b, t_b, g_b,
    stage, sems, recvs, send, recv, xsend, xrecv,
):
    core = lax.axis_index("rep")
    place = lax.axis_index("tp")
    iy = lax.axis_index("fs_1")
    iz = lax.axis_index("fs_0")
    other = 1 - core
    kind = lax.rem(place, 2)
    ahead = lax.rem(place + 1, 4)
    behind = lax.rem(place + 3, 4)
    across = lax.rem(place + 2, 4)
    rows = gate_v.shape[0]
    rows_b = branch_v.shape[0]
    loads = []

    def load(source, target):
        copy = pltpu.make_async_copy(source, target, in_sem.at[len(loads)])
        copy.start()
        loads.append(copy)

    load(branch_g.at[0, at(other, rows_b)], grads_b.at[1])
    load(gate_g.at[0, at(other, rows)], grads.at[0, 1])
    load(up_g.at[0, at(other, rows)], grads.at[1, 1])
    load(branch_g.at[0, at(core, rows_b)], grads_b.at[0])
    load(branch_v, speed_b)
    load(gate_g.at[0, at(core, rows)], grads.at[0, 0])
    load(gate_v, speed.at[0])
    load(up_g.at[0, at(core, rows)], grads.at[1, 0])
    load(up_v, speed.at[1])
    mine = at(core, HALF)
    partner = {"rep": other}
    used = []
    x0 = xall.at[0]
    a = pairs.at[0]

    def turn(axis, index, step):
        return {axis: lax.rem(index + step, 4)}

    def remote(src, dst, to):
        k = len(used)
        copy = pltpu.make_async_remote_copy(
            src_ref=src, dst_ref=dst, send_sem=sems.at[k], recv_sem=recvs.at[k], device_id=to, device_id_type=MESH
        )
        used.append(copy)
        return copy

    def send_to(ref, to):
        copy = remote(ref, ref, to)
        copy.start()
        return copy

    barrier = pltpu.get_barrier_semaphore()
    peers = [partner, {"tp": across}]
    peers += [{"tp": x, "rep": r} for x in (ahead, behind) for r in range(2)]
    peers += [turn(axis, index, step) for axis, index in (("fs_1", iy), ("fs_0", iz)) for step in (1, 2, 3)]
    for to in peers:
        pl.semaphore_signal(barrier, inc=1, device_id=to, device_id_type=MESH)

    own_rows, other_rows = at(core, rows), at(other, rows)
    loads[0].wait()
    give_b[...] = grads_b[1].astype(BF)
    for i in range(2):
        loads[1 + i].wait()
        give[i] = grads[i, 1].astype(BF)
    pl.semaphore_wait(barrier, len(peers))
    first_copies = [remote(give_b, take_b, partner)]
    first_copies += [remote(give.at[i], take.at[i], partner) for i in range(2)]
    for copy in first_copies:
        copy.start()
    same = lax.broadcasted_iota(jnp.int32, (128, 128), 0) == lax.broadcasted_iota(jnp.int32, (128, 128), 1)

    def columns(ref, lines, height, width):
        def block(x, part):
            return ref.at[at(core, height), spot(part * 4 * width + x * width, width, width)]

        state = {}

        def start():
            state["right"] = [send_to(block(place, p), {"tp": ahead}) for p in range(2)]
            state["left"] = [send_to(block(place, p), {"tp": behind}) for p in range(2)]
            state["own"] = [send_to(block(place, p), partner) for p in range(2)]

        def second():
            state["right"][0].wait_recv()
            far = [send_to(block(behind, 0), {"tp": ahead})]
            state["left"][1].wait_recv()
            far.append(send_to(block(ahead, 1), {"tp": behind}))
            state["far"] = far
            state["own"].append(send_to(block(behind, 0), partner))
            state["own"].append(send_to(block(ahead, 1), partner))
            state["right"][1].wait_recv()
            state["own"].append(send_to(block(behind, 1), partner))
            state["left"][0].wait_recv()
            state["own"].append(send_to(block(ahead, 0), partner))

        def finish():
            for p in range(2):
                state["far"][p].wait_recv()
                state["own"].append(send_to(block(across, p), partner))
            for copy in state["own"]:
                copy.wait_recv()

        return start, second, finish

    lines = [columns(xb, None, rows_b, 128)]
    line = {}

    def block_of(x, p):
        return x0.at[own_rows, spot(p * HALF + x * 256, 256, 256)]

    def line_start():
        line["relay"] = [
            remote(starts.at[kind, p], relay.at[p], {"tp": to}) for p, to in ((0, ahead), (1, behind))
        ]
        line["out"] = [
            [remote(starts.at[1 - kind, p], block_of(place, p), {"tp": to}) for p in range(2)] for to in (ahead, behind)
        ]
        for copy in line["relay"] + line["out"][0] + line["out"][1]:
            copy.start()
        line["own"] = [send_to(block_of(place, p), partner) for p in range(2)]

    def line_second():
        line["far"] = []
        for p, (source, to) in enumerate(((behind, ahead), (ahead, behind))):
            line["relay"][p].wait_recv()
            copy = remote(relay.at[p], block_of(source, p), {"tp": to})
            copy.start()
            line["far"].append(copy)

    def line_third():
        for side, source in ((0, behind), (1, ahead)):
            for p in range(2):
                line["out"][side][p].wait_recv()
                line["own"].append(send_to(block_of(source, p), partner))

    def line_finish():
        for p in range(2):
            line["far"][p].wait_recv()
            line["own"].append(send_to(block_of(across, p), partner))
        for copy in line["own"]:
            copy.wait_recv()

    first_copies[0].wait_recv()
    loads[3].wait()
    loads[4].wait()
    moment = MOMENT * speed_b[...] + (grads_b[0] + take_b[...].astype(jnp.float32))
    speed_b[...] = moment
    for p in range(2):
        xb[at(core, rows_b), spot(p * 512 + place * 128, 128, 128)] = moment[:, p * 128 : p * 128 + 128].astype(BF)
    lines[0][0]()
    for i in range(2):
        first_copies[1 + i].wait_recv()
        loads[5 + 2 * i].wait()
        loads[6 + 2 * i].wait()
        moment = MOMENT * speed[i] + (grads[i, 0] + take[i].astype(jnp.float32))
        speed[i] = moment
        for p in range(2):
            starts[i, p] = moment[:, p * 256 : p * 256 + 256].astype(BF)
    for p in range(2):
        x0[own_rows, spot(p * HALF + place * 256, 256, 256)] = starts[kind, p]
    line_start()
    stores = []

    def store(source, target):
        copy = pltpu.make_async_copy(source, target, out_sem.at[len(stores)])
        copy.start()
        stores.append(copy)

    axes = ((("fs_1", iy), ("fs_0", iz)), (("fs_0", iz), ("fs_1", iy)))

    def exchange(source, landing, axis, index):
        copies = []
        for step in (2, 1, 3):
            to = lax.rem(index + step, 4)
            copies.append(remote(source(to), landing.at[step - 1], {axis: to}))
            copies[-1].start()
        return copies

    def total(own, landing, copies):
        for copy in copies:
            copy.wait_recv()
        value = own.astype(jnp.float32)
        for k in range(3):
            value = value + landing[k].astype(jnp.float32)
        return value.astype(BF)

    def scatter_one(source, landings):
        return [
            exchange(functools.partial(source, p), landings[p], *axes[p][0]) for p in range(2)
        ]

    def source_of(i):
        return lambda p, t: part.at[i, at(t, 64), at(p, 640)]

    def source_b(p, t):
        return part_b.at[spot(p * 64 + t * 16, 16, 16), :]

    upper = lax.div(place, 2)

    def panel(i):
        first = core * 4 + 2 * upper + i
        own = x0[:, at(first, 256)]
        for d in range(5):
            part[i, :, at(d, 256)] = turned(own, x0[:, at(lax.rem(first + d, 8), 256)]).astype(BF)
        return scatter_one(source_of(i), [near.at[i, p] for p in range(2)])

    def gram_rows(p, i1):
        return spot(p * 64 + i1 * 16, 16, 16)

    group = at(core, 4)

    class Ring:
        def __init__(self, axis, index, block, cut):
            self.next, self.prev = turn(axis, index, 1), turn(axis, index, 3)
            self.index, self.block, self.cut = index, block, cut

        def start(self):
            ref = self.block(self.index)
            self.right = send_to(ref, self.next)
            self.left = send_to(ref, self.prev)

        def second(self):
            self.right.wait_recv()
            self.far = [send_to(self.cut(lax.rem(self.index + 3, 4), 0), self.next)]
            self.left.wait_recv()
            self.far.append(send_to(self.cut(lax.rem(self.index + 1, 4), 1), self.prev))

        def finish(self):
            for copy in self.far:
                copy.wait_recv()

    def rings(phase, block, cut):
        return [
            Ring(*axes[p][phase], functools.partial(block, p), functools.partial(cut, p)) for p in range(2)
        ]

    def b_small(p, j):
        return gram_b.at[group, gram_rows(p, axes[p][0][1]), at(j, 256)]

    def b_small_cut(p, j, h):
        return gram_b.at[at(core * 2 + h, 2), gram_rows(p, axes[p][0][1]), at(j, 256)]

    def b_large(p, j):
        return gram_b.at[group, gram_rows(p, j), :]

    def b_large_cut(p, j, h):
        return gram_b.at[at(core * 2 + h, 2), gram_rows(p, j), :]

    def g_rows(p, j):
        return spot(axes[p][0][1] * 64 + j * 16, 16, 16)

    def g_small(p, j):
        return panels.at[core, :, g_rows(p, j), at(p, 640)]

    def g_small_cut(p, j, h):
        return panels.at[core, at(h, 2), g_rows(p, j), at(p, 640)]

    def g_large(p, j):
        return panels.at[core, :, at(j, 64), at(p, 640)]

    def g_large_cut(p, j, h):
        return panels.at[core, at(h, 2), at(j, 64), at(p, 640)]

    small_b, large_b = rings(1, b_small, b_small_cut), rings(0, b_large, b_large_cut)
    small, large = rings(1, g_small, g_small_cut), rings(0, g_large, g_large_cut)
    lines[0][1]()
    line_second()
    lines[0][2]()
    part_b[...] = turned(xb[:, spot(core * 512 + place * 128, 128, 128)], xb[...]).astype(BF)
    one_b = scatter_one(source_b, [near_b.at[p] for p in range(2)])
    line_third()
    for source, target in ((speed_b, branch_m), (speed.at[0], gate_m), (speed.at[1], up_m)):
        store(source, target)
    two_b = []
    for p in range(2):
        kept_b[p] = total(part_b[spot(p * 64 + axes[p][0][1] * 16, 16, 16), :], near_b.at[p], one_b[p])
        two_b.append(exchange(lambda t, p=p: kept_b.at[p, :, at(t, 256)], near2_b.at[p], *axes[p][1]))
    line_finish()
    ones = [panel(0), panel(1)]
    swaps_b = []
    for p in range(2):
        i1, i2 = axes[p][0][1], axes[p][1][1]
        gram_b[core * 4 + place, gram_rows(p, i1), at(i2, 256)] = total(
            kept_b[p, :, at(i2, 256)], near2_b.at[p], two_b[p]
        )
        ref = gram_b.at[core * 4 + place, gram_rows(p, i1), at(i2, 256)]
        swaps_b.append([send_to(ref, {"tp": x}) for x in (across, ahead, behind)])

    def scatter_two(i):
        pair = []
        for p in range(2):
            index = axes[p][0][1]
            kept[i, p] = total(part[i, at(index, 64), at(p, 640)], near.at[i, p], ones[i][p])
            pair.append(exchange(lambda t, p=p: kept.at[i, p, at(t, 16), :], near2.at[i, p], *axes[p][1]))
        return pair

    for p in range(2):
        for copy in swaps_b[p]:
            copy.wait_recv()
        small_b[p].start()
    twos = [scatter_two(0), scatter_two(1)]
    for ring in small_b:
        ring.second()
    swaps = []
    for p in range(2):
        i2 = axes[p][1][1]
        for i in range(2):
            panels[core, 2 * upper + i, g_rows(p, i2), at(p, 640)] = total(
                kept[i, p, at(i2, 16), :], near2.at[i, p], twos[i][p]
            )
        swaps.append(send_to(panels.at[core, at(upper, 2), g_rows(p, i2), at(p, 640)], {"tp": across}))
    for ring in small_b:
        ring.finish()
    for ring in large_b:
        ring.start()
    for copy, ring in zip(swaps, small):
        copy.wait_recv()
        ring.start()
    forward_b, forward = [], []
    for p, ring in enumerate(large_b):
        ring.second()
        forward_b += [send_to(b_large(p, lax.rem(ring.index + k, 4)), partner) for k in (0, 3, 1)]
    for ring in small:
        ring.second()
    for ring in small:
        ring.finish()
    for ring in large:
        ring.start()
    for p, ring in enumerate(large_b):
        ring.finish()
        forward_b.append(send_to(b_large(p, lax.rem(ring.index + 2, 4)), partner))
    for copy in forward_b:
        copy.wait_recv()

    def coefficients(squares, diagonal):
        second = jnp.full((1, 1), squares)
        first = jnp.full((1, 1), diagonal)
        ratio = SAFETY * (second + 1.0) / (first + 1.0)
        return 1.0 / ratio, lax.rsqrt(ratio)

    def squares_b(i, sums):
        value = gram_b[i].astype(jnp.float32)
        diagonal = gram_b[i, :, at(i, 128)].astype(jnp.float32)
        return (
            sums[0] + jnp.sum((value * value).reshape(16, 8, NB), axis=0),
            sums[1] + jnp.where(same, diagonal, 0.0),
        )

    sums = lax.fori_loop(0, 8, squares_b, (jnp.zeros((8, NB), jnp.float32), jnp.zeros((128, 128), jnp.float32)))
    alpha_b, scale_b = coefficients(jnp.sum(sums[0]), jnp.sum(sums[1]))

    top, low_half = pl.ds(0, 512), pl.ds(512, 512)

    def mirrored_b(left, right, out, emit):
        out[top, top] = emit(left[top, top], dot(left[top, :], right[:, top])).astype(BF)
        out[low_half, :] = emit(left[low_half, :], dot(left[low_half, :], right[...])).astype(BF)
        out[top, low_half] = out[low_half, top].T

    def square_b(left, low, high):
        mirrored_b(left, left, m_b, lambda own, value: low * own.astype(jnp.float32) + high * value)

    def times_b(left, out, factor):
        mirrored_b(left, m_b, out, lambda own, value: factor * (COEF_ONE * own.astype(jnp.float32) + value))

    def rows_of(left, factor):
        return (factor * (COEF_ONE * left.astype(jnp.float32) + dot(left, m_b[...]))).astype(BF)

    for i in range(8):
        g_b[at(i, 128), :] = gram_b[i]
    square_b(g_b, COEF_THREE * alpha_b, COEF_FIVE * alpha_b * alpha_b)
    times_b(g_b, t_b, alpha_b)
    line_b = rows_of(xb[at(core, rows_b), :], scale_b)
    times_b(t_b, g_b, 1.0)
    square_b(g_b, COEF_THREE, COEF_FIVE)
    for p, ring in enumerate(large):
        ring.second()
        forward += [send_to(g_large(p, lax.rem(ring.index + k, 4)), partner) for k in (0, 3, 1)]
    times_b(g_b, t_b, 1.0)
    line_b = rows_of(line_b, 1.0)
    times_b(t_b, g_b, 1.0)
    for p, ring in enumerate(large):
        ring.finish()
        forward.append(send_to(g_large(p, lax.rem(ring.index + 2, 4)), partner))
    square_b(g_b, COEF_THREE, COEF_FIVE)
    t_b[0:rows_b, :] = line_b
    for p in range(2):
        cols = spot(p * 512 + place * 128, 128, 128)
        last_b = COEF_ONE * t_b[0:rows_b, cols].astype(jnp.float32) + dot(line_b, m_b[:, cols])
        results_b[:, at(p, 128)] = last_b.astype(BF)
    store(results_b, branch_out)
    for copy in forward:
        copy.wait_recv()

    def assemble(r, sums):
        value = panels[lax.div(r, 4), lax.rem(r, 4)]
        squares, diagonal = sums
        for d in range(5):
            block = value[:, d * 256 : d * 256 + 256]
            column = at(lax.rem(r + d, 8), 256)
            a[at(r, 256), column] = block
            if 0 < d < 4:
                a[column, at(r, 256)] = block.T
            wide = block.astype(jnp.float32)
            weight = 2.0 if 0 < d < 4 else 1.0
            squares = squares + weight * jnp.sum((wide * wide).reshape(32, 8, 256), axis=0)
        for k in range(2):
            corner = value[k * 128 : k * 128 + 128, k * 128 : k * 128 + 128].astype(jnp.float32)
            diagonal = diagonal + jnp.where(same, corner, 0.0)
        return squares, diagonal

    sums = lax.fori_loop(0, 8, assemble, (jnp.zeros((8, 256), jnp.float32), jnp.zeros((128, 128), jnp.float32)))
    alpha, scale = coefficients(jnp.sum(sums[0]), jnp.sum(sums[1]))


    def h(q):
        return at(2 * core + q, BLOCK)

    def o(q):
        return at(2 * other + q, BLOCK)

    def flip(q):
        return lax.rem(q + core, 2)

    def flop(q):
        return lax.rem(q + other, 2)

    def pair(ref, target, k, q):
        return pltpu.make_async_remote_copy(
            src_ref=ref, dst_ref=target, send_sem=send.at[k, q], recv_sem=recv.at[k, q], device_id=partner, device_id_type=MESH
        )

    def cross_out(buf, k, q):
        ref = buf.at[o(q), h(flip(q))]
        return pair(ref, ref, k, q)

    def cross_in(buf, k, q):
        ref = buf.at[h(q), o(flop(q))]
        return pair(ref, ref, k, q)

    def square_out(buf, k, q, side):
        first = at(2 * side, BLOCK)
        second = at(2 * side + 1, BLOCK)
        ref = (buf.at[first, at(side, HALF)], buf.at[second, first], buf.at[second, second])[q]
        return pair(ref, ref, k, 2 + q)

    def stage_out(k, q):
        return pair(m.at[o(q), at(flip(q), BLOCK)], stage.at[q], 4 + k, q)

    def receive_cross(left, k):
        def step(q, _):
            cross_out(left, k, q).wait_send()
            cross_in(left, k, q).wait_recv()
            left[o(flop(q)), h(q)] = left[h(q), o(flop(q))].T
            return 0

        lax.fori_loop(0, 2, step, 0)

    def receive_square(left, k):
        for q in range(3):
            square_out(left, k, q, core).wait_send()
            square_out(left, k, q, other).wait_recv()

    def product(left, receive, right, emit, after_head, after_cross, after_all):
        receive(receive_cross)
        emit(at(core, HALF), 0, dot(left[at(core, HALF), :], right(0)))
        after_head()
        receive(receive_square)
        for q in range(2):
            j = flip(q)
            emit(o(q), j, dot(left[o(q), :], right(j)))
            after_cross(q)
        emit(h(1), 1, dot(left[h(1), :], right(1)))
        after_all()

    def square(left, receive, k_out, low, high):
        def emit(where, j, value):
            value = low * left[where, h(j)].astype(jnp.float32) + high * value
            m[where, at(j, BLOCK)] = value.astype(BF)

        def after_head():
            m[h(0), at(1, BLOCK)] = m[h(1), at(0, BLOCK)].T

        def after_cross(q):
            stage_out(k_out, q).start()

        def right(j):
            return left[:, h(j)]

        product(left, receive, right, emit, after_head, after_cross, lambda: None)
        for q in range(2):
            copy = stage_out(k_out, q)
            copy.wait_send()
            copy.wait_recv()
            m[o(flop(q)), at(q, BLOCK)] = stage[q].T

    def times(left, receive, out, k_out, factor):
        def emit(where, j, value):
            value = factor * (COEF_ONE * left[where, h(j)].astype(jnp.float32) + value)
            out[where, h(j)] = value.astype(BF)

        def after_head():
            out[h(0), h(1)] = out[h(1), h(0)].T
            square_out(out, k_out, 0, core).start()
            square_out(out, k_out, 1, core).start()

        def after_cross(q):
            cross_out(out, k_out, q).start()
            out[h(flip(q)), o(q)] = out[o(q), h(flip(q))].T

        def after_all():
            square_out(out, k_out, 2, core).start()

        def right(j):
            return m[:, at(j, BLOCK)]

        product(left, receive, right, emit, after_head, after_cross, after_all)

    def x_swap(i, half):
        ref = xall.at[i + 1, :, at(half, HALF)]
        return pltpu.make_async_remote_copy(
            src_ref=ref, dst_ref=ref, send_sem=xsend.at[i], recv_sem=xrecv.at[i], device_id=partner, device_id_type=MESH
        )

    def iteration(i, _):
        left, following = pairs.at[i], pairs.at[1 - i]
        opening = i == 0
        weight = jnp.where(opening, alpha, 1.0)

        def receive_later(step):
            @pl.when(i == 1)
            def _():
                step(left, 1)

        square(left, receive_later, i, COEF_THREE * weight, COEF_FIVE * weight * weight)
        times(left, lambda step: None, b, 2 * i, weight)

        @pl.when(i == 1)
        def _():
            x_swap(0, core).wait_send()
            x_swap(0, other).wait_recv()

        own = xall[i, :, mine].astype(jnp.float32)
        xall[i + 1, :, mine] = (jnp.where(opening, scale, 1.0) * (COEF_ONE * own + dot(xall[i], m[...]))).astype(BF)
        x_swap(i, core).start()
        times(b, lambda step: step(b, 2 * i), following, 2 * i + 1, 1.0)
        return 0

    lax.fori_loop(0, 2, iteration, 0)

    def some(block, low, high):
        close = spot(core * HALF + block * 256, 256, 256)

        def step(r, _):
            where = at(lax.rem(2 * core + r, 4), BLOCK)
            value = COEF_THREE * a[where, close].astype(jnp.float32) + COEF_FIVE * dot(a[where, :], a[:, close])
            m[where, at(block, 256)] = value.astype(BF)
            return 0

        lax.fori_loop(low, high, step, 0)

    def last(where, block):
        cols = at(block, 256)
        close = spot(core * HALF + block * 256, 256, 256)
        return (COEF_ONE * x2[where, close].astype(jnp.float32) + dot(x2[where, :], m[:, cols])).astype(BF)

    receive_cross(a, 3)
    some(ahead, 0, 2)
    receive_square(a, 3)
    some(ahead, 2, 4)
    x_swap(1, core).wait_send()
    x_swap(1, other).wait_recv()
    x2 = xall.at[2]
    final[2] = last(pl.ds(0, rows), ahead)
    to_ahead = pltpu.make_async_remote_copy(
        src_ref=final.at[2], dst_ref=final.at[4 + core], send_sem=sems.at[COPIES], recv_sem=recvs.at[COPIES + core],
        device_id={"tp": ahead, "rep": 0}, device_id_type=MESH,
    )
    to_ahead.start()
    some(behind, 0, 4)
    final[3] = last(pl.ds(rows, rows), behind)
    to_behind = pltpu.make_async_remote_copy(
        src_ref=final.at[3], dst_ref=final.at[4 + core], send_sem=sems.at[COPIES + 1], recv_sem=recvs.at[COPIES + core],
        device_id={"tp": behind, "rep": 1}, device_id_type=MESH,
    )
    to_behind.start()
    some(place, 0, 4)
    final[6] = last(other_rows, place)
    to_partner = remote(final.at[6], final.at[core], partner)
    to_partner.start()
    final[core] = last(own_rows, place)
    to_partner.wait_recv()
    for i in range(2):
        pltpu.make_async_remote_copy(
            src_ref=final.at[2], dst_ref=final.at[4 + i], send_sem=sems.at[COPIES], recv_sem=recvs.at[COPIES + i],
            device_id=partner, device_id_type=MESH,
        ).wait_recv()
    for i in range(2):
        cols = pl.ds(i * 256, 256)
        results[kind, :, cols] = final[i]
        results[1 - kind, :, cols] = final[4 + i]
    store(results.at[0], gate_out)
    store(results.at[1], up_out)
    to_ahead.wait_send()
    to_behind.wait_send()
    for copy in used:
        copy.wait_send()
    for copy in stores:
        copy.wait()


def finish_kernel(*refs):
    ins, outs, stage, fresh, in_sem, out_sem = refs[:9], refs[9:15], refs[15:24], refs[24:27], refs[27], refs[28]
    loads = [pltpu.make_async_copy(ins[i], stage[i], in_sem.at[i]) for i in range(9)]
    for i in (3, 6, 4, 7, 5, 8, 0, 1, 2):
        loads[i].start()
    stores = []

    def store(source, target):
        copy = pltpu.make_async_copy(source, target, out_sem.at[len(stores)])
        copy.start()
        stores.append(copy)

    for i, height in enumerate((FF, FF, D)):
        loads[3 + i].wait()
        loads[6 + i].wait()
        fresh[i][...] = SHRINK * stage[6 + i][...] - RATE * math.sqrt(height) * stage[3 + i][...].astype(jnp.float32)
        store(fresh[i], outs[2 * i + 1])
    for i in range(3):
        loads[i].wait()
        store(stage[i], outs[2 * i])
    for copy in stores:
        copy.wait()


def local(*args):
    velocities = (args[1], args[4], args[7])
    shapes = [velocity.shape for velocity in velocities]
    (rows, width), (rows_b, width_b) = shapes[0], shapes[2]
    anywhere = pl.BlockSpec(memory_space=pl.ANY)
    dma = pltpu.SemaphoreType.DMA

    def buf(*shape):
        return pltpu.VMEM(shape, BF)

    def full(*shape):
        return pltpu.VMEM(shape, jnp.float32)

    outs = [jax.ShapeDtypeStruct(shape, kind) for kind in (jnp.float32, BF) for shape in shapes]
    middle = pl.pallas_call(
        kernel,
        out_shape=outs,
        in_specs=[anywhere] * 6,
        out_specs=[anywhere] * 6,
        scratch_shapes=[
            full(2, 2, rows, width), full(2, rows_b, width_b), full(2, rows, width), full(rows_b, width_b),
            buf(2, rows, width), buf(rows_b, width_b), dma((9,)), dma((6,)),
            buf(2, N, N), buf(N, N), buf(N, HALF), buf(3, 2 * rows, N), buf(2 * rows_b, NB), buf(7, rows, 256),
            buf(2, 2, rows, 256), buf(2, rows, 256),
            buf(2, rows, width), buf(2, rows, width), buf(rows_b, width_b), buf(rows_b, width_b),
            buf(2, 256, 1280), buf(2, 2, 3, 64, 640), buf(2, 2, 64, 640), buf(2, 2, 3, 16, 640),
            buf(2, 4, 256, 1280),
            buf(128, NB), buf(2, 3, 16, NB), buf(2, 16, NB), buf(2, 3, 16, 256), buf(8, 128, NB),
            buf(NB, NB), buf(NB, NB), buf(NB, NB),
            buf(2, BLOCK, BLOCK),
            dma((COPIES + 2,)), dma((COPIES + 2,)), dma((7, 5)), dma((7, 5)), dma((2,)), dma((2,)),
        ],
        compiler_params=pltpu.CompilerParams(collective_id=0, has_side_effects=True, vmem_limit_bytes=62 * 1024 * 1024),
    )(args[0], args[3], args[6], args[1], args[4], args[7])
    results = [jax.ShapeDtypeStruct(shape, jnp.float32) for shape in shapes for _ in range(2)]
    stage = [full(*shape) for shape in shapes] + [buf(*shape) for shape in shapes] + [full(*shape) for shape in shapes] * 2
    return pl.pallas_call(
        finish_kernel,
        out_shape=results,
        in_specs=[anywhere] * 9,
        out_specs=[anywhere] * 6,
        scratch_shapes=stage + [dma((9,)), dma((6,))],
    )(*middle, args[2], args[5], args[8])


def solution(mesh):
    torus = Mesh(
        mesh.devices.reshape(4, 4, mesh.shape["tp"], mesh.shape["rep"]),
        ("fs_0", "fs_1", "tp", "rep"),
    )
    grads, plain = P("rep", FS, "tp"), P(FS_REP, "tp")
    return jax.shard_map(
        local,
        mesh=torus,
        in_specs=(grads, plain, plain) * 3,
        out_specs=(plain,) * 6,
        check_vma=False,
    )
```

```python
import functools
import math

import jax
import jax.numpy as jnp
from jax import lax
from jax.experimental import pallas as pl
from jax.experimental.pallas import tpu as pltpu
from jax.sharding import Mesh
from jax.sharding import PartitionSpec as P

D = 2048
FF = 5632
FS_REP = ("fs_0", "fs_1", "rep")
FS = ("fs_0", "fs_1")

MOMENT = 0.95
COEF_ONE = 3.4445
COEF_THREE = -4.775
COEF_FIVE = 2.0315
SAFETY = 2.0
RATE = 0.5
SHRINK = 0.95
BF = jnp.bfloat16


def dot(a, b):
    return jnp.dot(a, b, preferred_element_type=jnp.float32)


N = 2048
HALF = 1024
BLOCK = 512
NB = 1024
COPIES = 160
MESH = pl.DeviceIdType.MESH


def at(index, size):
    return pl.ds(index * size if isinstance(index, int) else pl.multiple_of(index * size, size), size)


def spot(offset, size, unit):
    return pl.ds(pl.multiple_of(offset, unit), size)


def turned(a, b):
    return lax.dot_general(a, b, (((0,), (0,)), ((), ())), preferred_element_type=jnp.float32)


def kernel(
    gate_g, up_g, branch_g, gate_v, up_v, branch_v,
    gate_m, up_m, branch_m, gate_out, up_out, branch_out,
    grads, grads_b, speed, speed_b, results, results_b, in_sem, out_sem,
    pairs, b, m, xall, xb, final, starts, relay,
    give, take, give_b, take_b,
    part, near, kept, near2, panels,
    part_b, near_b, kept_b, near2_b, gram_b, m_b, t_b, g_b,
    stage, sems, recvs, send, recv, xsend, xrecv,
):
    core = lax.axis_index("rep")
    place = lax.axis_index("tp")
    iy = lax.axis_index("fs_1")
    iz = lax.axis_index("fs_0")
    other = 1 - core
    kind = lax.rem(place, 2)
    ahead = lax.rem(place + 1, 4)
    behind = lax.rem(place + 3, 4)
    across = lax.rem(place + 2, 4)
    rows = gate_v.shape[0]
    rows_b = branch_v.shape[0]
    loads = []

    def load(source, target):
        copy = pltpu.make_async_copy(source, target, in_sem.at[len(loads)])
        copy.start()
        loads.append(copy)

    load(branch_g.at[0, at(other, rows_b)], grads_b.at[1])
    load(gate_g.at[0, at(other, rows)], grads.at[0, 1])
    load(up_g.at[0, at(other, rows)], grads.at[1, 1])
    load(branch_g.at[0, at(core, rows_b)], grads_b.at[0])
    load(branch_v, speed_b)
    load(gate_g.at[0, at(core, rows)], grads.at[0, 0])
    load(gate_v, speed.at[0])
    load(up_g.at[0, at(core, rows)], grads.at[1, 0])
    load(up_v, speed.at[1])
    mine = at(core, HALF)
    partner = {"rep": other}
    used = []
    x0 = xall.at[0]
    a = pairs.at[0]

    def turn(axis, index, step):
        return {axis: lax.rem(index + step, 4)}

    def remote(src, dst, to):
        k = len(used)
        copy = pltpu.make_async_remote_copy(
            src_ref=src, dst_ref=dst, send_sem=sems.at[k], recv_sem=recvs.at[k], device_id=to, device_id_type=MESH
        )
        used.append(copy)
        return copy

    def send_to(ref, to):
        copy = remote(ref, ref, to)
        copy.start()
        return copy

    barrier = pltpu.get_barrier_semaphore()
    peers = [partner, {"tp": across}]
    peers += [{"tp": x, "rep": r} for x in (ahead, behind) for r in range(2)]
    peers += [turn(axis, index, step) for axis, index in (("fs_1", iy), ("fs_0", iz)) for step in (1, 2, 3)]
    for to in peers:
        pl.semaphore_signal(barrier, inc=1, device_id=to, device_id_type=MESH)

    own_rows, other_rows = at(core, rows), at(other, rows)
    loads[0].wait()
    give_b[...] = grads_b[1].astype(BF)
    for i in range(2):
        loads[1 + i].wait()
        give[i] = grads[i, 1].astype(BF)
    pl.semaphore_wait(barrier, len(peers))
    first_copies = [remote(give_b, take_b, partner)]
    first_copies += [remote(give.at[i], take.at[i], partner) for i in range(2)]
    for copy in first_copies:
        copy.start()
    same = lax.broadcasted_iota(jnp.int32, (128, 128), 0) == lax.broadcasted_iota(jnp.int32, (128, 128), 1)

    def columns(ref, lines, height, width):
        def block(x, part):
            return ref.at[at(core, height), spot(part * 4 * width + x * width, width, width)]

        state = {}

        def start():
            state["right"] = [send_to(block(place, p), {"tp": ahead}) for p in range(2)]
            state["left"] = [send_to(block(place, p), {"tp": behind}) for p in range(2)]
            state["own"] = [send_to(block(place, p), partner) for p in range(2)]

        def second():
            state["right"][0].wait_recv()
            far = [send_to(block(behind, 0), {"tp": ahead})]
            state["left"][1].wait_recv()
            far.append(send_to(block(ahead, 1), {"tp": behind}))
            state["far"] = far
            state["own"].append(send_to(block(behind, 0), partner))
            state["own"].append(send_to(block(ahead, 1), partner))
            state["right"][1].wait_recv()
            state["own"].append(send_to(block(behind, 1), partner))
            state["left"][0].wait_recv()
            state["own"].append(send_to(block(ahead, 0), partner))

        def finish():
            for p in range(2):
                state["far"][p].wait_recv()
                state["own"].append(send_to(block(across, p), partner))
            for copy in state["own"]:
                copy.wait_recv()

        return start, second, finish

    lines = [columns(xb, None, rows_b, 128)]
    line = {}

    def block_of(x, p):
        return x0.at[own_rows, spot(p * HALF + x * 256, 256, 256)]

    def line_start():
        line["relay"] = [
            remote(starts.at[kind, p], relay.at[p], {"tp": to}) for p, to in ((0, ahead), (1, behind))
        ]
        line["out"] = [
            [remote(starts.at[1 - kind, p], block_of(place, p), {"tp": to}) for p in range(2)] for to in (ahead, behind)
        ]
        for copy in line["relay"] + line["out"][0] + line["out"][1]:
            copy.start()
        line["own"] = [send_to(block_of(place, p), partner) for p in range(2)]

    def line_second():
        line["far"] = []
        for p, (source, to) in enumerate(((behind, ahead), (ahead, behind))):
            line["relay"][p].wait_recv()
            copy = remote(relay.at[p], block_of(source, p), {"tp": to})
            copy.start()
            line["far"].append(copy)

    def line_third():
        for side, source in ((0, behind), (1, ahead)):
            for p in range(2):
                line["out"][side][p].wait_recv()
                line["own"].append(send_to(block_of(source, p), partner))

    def line_finish():
        for p in range(2):
            line["far"][p].wait_recv()
            line["own"].append(send_to(block_of(across, p), partner))
        for copy in line["own"]:
            copy.wait_recv()

    first_copies[0].wait_recv()
    loads[3].wait()
    loads[4].wait()
    moment = MOMENT * speed_b[...] + (grads_b[0] + take_b[...].astype(jnp.float32))
    speed_b[...] = moment
    for p in range(2):
        xb[at(core, rows_b), spot(p * 512 + place * 128, 128, 128)] = moment[:, p * 128 : p * 128 + 128].astype(BF)
    lines[0][0]()
    for i in range(2):
        first_copies[1 + i].wait_recv()
        loads[5 + 2 * i].wait()
        loads[6 + 2 * i].wait()
        moment = MOMENT * speed[i] + (grads[i, 0] + take[i].astype(jnp.float32))
        speed[i] = moment
        for p in range(2):
            starts[i, p] = moment[:, p * 256 : p * 256 + 256].astype(BF)
    for p in range(2):
        x0[own_rows, spot(p * HALF + place * 256, 256, 256)] = starts[kind, p]
    line_start()
    stores = []

    def store(source, target):
        copy = pltpu.make_async_copy(source, target, out_sem.at[len(stores)])
        copy.start()
        stores.append(copy)

    axes = ((("fs_1", iy), ("fs_0", iz)), (("fs_0", iz), ("fs_1", iy)))

    def exchange(source, landing, axis, index):
        copies = []
        for step in (2, 1, 3):
            to = lax.rem(index + step, 4)
            copies.append(remote(source(to), landing.at[step - 1], {axis: to}))
            copies[-1].start()
        return copies

    def total(own, landing, copies):
        for copy in copies:
            copy.wait_recv()
        value = own.astype(jnp.float32)
        for k in range(3):
            value = value + landing[k].astype(jnp.float32)
        return value.astype(BF)

    def scatter_one(source, landings):
        return [
            exchange(functools.partial(source, p), landings[p], *axes[p][0]) for p in range(2)
        ]

    def source_of(i):
        return lambda p, t: part.at[i, at(t, 64), at(p, 640)]

    def source_b(p, t):
        return part_b.at[spot(p * 64 + t * 16, 16, 16), :]

    upper = lax.div(place, 2)

    def panel(i):
        first = core * 4 + 2 * upper + i
        own = x0[:, at(first, 256)]
        for d in range(5):
            part[i, :, at(d, 256)] = turned(own, x0[:, at(lax.rem(first + d, 8), 256)]).astype(BF)
        return scatter_one(source_of(i), [near.at[i, p] for p in range(2)])

    def gram_rows(p, i1):
        return spot(p * 64 + i1 * 16, 16, 16)

    group = at(core, 4)

    class Ring:
        def __init__(self, axis, index, block, cut):
            self.next, self.prev = turn(axis, index, 1), turn(axis, index, 3)
            self.index, self.block, self.cut = index, block, cut

        def start(self):
            ref = self.block(self.index)
            self.right = send_to(ref, self.next)
            self.left = send_to(ref, self.prev)

        def second(self):
            self.right.wait_recv()
            self.far = [send_to(self.cut(lax.rem(self.index + 3, 4), 0), self.next)]
            self.left.wait_recv()
            self.far.append(send_to(self.cut(lax.rem(self.index + 1, 4), 1), self.prev))

        def finish(self):
            for copy in self.far:
                copy.wait_recv()

    def rings(phase, block, cut):
        return [
            Ring(*axes[p][phase], functools.partial(block, p), functools.partial(cut, p)) for p in range(2)
        ]

    def b_small(p, j):
        return gram_b.at[group, gram_rows(p, axes[p][0][1]), at(j, 256)]

    def b_small_cut(p, j, h):
        return gram_b.at[at(core * 2 + h, 2), gram_rows(p, axes[p][0][1]), at(j, 256)]

    def b_large(p, j):
        return gram_b.at[group, gram_rows(p, j), :]

    def b_large_cut(p, j, h):
        return gram_b.at[at(core * 2 + h, 2), gram_rows(p, j), :]

    def g_rows(p, j):
        return spot(axes[p][0][1] * 64 + j * 16, 16, 16)

    def g_small(p, j):
        return panels.at[core, :, g_rows(p, j), at(p, 640)]

    def g_small_cut(p, j, h):
        return panels.at[core, at(h, 2), g_rows(p, j), at(p, 640)]

    def g_large(p, j):
        return panels.at[core, :, at(j, 64), at(p, 640)]

    def g_large_cut(p, j, h):
        return panels.at[core, at(h, 2), at(j, 64), at(p, 640)]

    small_b, large_b = rings(1, b_small, b_small_cut), rings(0, b_large, b_large_cut)
    small, large = rings(1, g_small, g_small_cut), rings(0, g_large, g_large_cut)
    lines[0][1]()
    line_second()
    lines[0][2]()
    part_b[...] = turned(xb[:, spot(core * 512 + place * 128, 128, 128)], xb[...]).astype(BF)
    one_b = scatter_one(source_b, [near_b.at[p] for p in range(2)])
    line_third()
    for source, target in ((speed_b, branch_m), (speed.at[0], gate_m), (speed.at[1], up_m)):
        store(source, target)
    two_b = []
    for p in range(2):
        kept_b[p] = total(part_b[spot(p * 64 + axes[p][0][1] * 16, 16, 16), :], near_b.at[p], one_b[p])
        two_b.append(exchange(lambda t, p=p: kept_b.at[p, :, at(t, 256)], near2_b.at[p], *axes[p][1]))
    line_finish()
    ones = [panel(0), panel(1)]
    swaps_b = []
    for p in range(2):
        i1, i2 = axes[p][0][1], axes[p][1][1]
        gram_b[core * 4 + place, gram_rows(p, i1), at(i2, 256)] = total(
            kept_b[p, :, at(i2, 256)], near2_b.at[p], two_b[p]
        )
        ref = gram_b.at[core * 4 + place, gram_rows(p, i1), at(i2, 256)]
        swaps_b.append([send_to(ref, {"tp": x}) for x in (across, ahead, behind)])

    def scatter_two(i):
        pair = []
        for p in range(2):
            index = axes[p][0][1]
            kept[i, p] = total(part[i, at(index, 64), at(p, 640)], near.at[i, p], ones[i][p])
            pair.append(exchange(lambda t, p=p: kept.at[i, p, at(t, 16), :], near2.at[i, p], *axes[p][1]))
        return pair

    for p in range(2):
        for copy in swaps_b[p]:
            copy.wait_recv()
        small_b[p].start()
    twos = [scatter_two(0), scatter_two(1)]
    for ring in small_b:
        ring.second()
    swaps = []
    for p in range(2):
        i2 = axes[p][1][1]
        for i in range(2):
            panels[core, 2 * upper + i, g_rows(p, i2), at(p, 640)] = total(
                kept[i, p, at(i2, 16), :], near2.at[i, p], twos[i][p]
            )
        swaps.append(send_to(panels.at[core, at(upper, 2), g_rows(p, i2), at(p, 640)], {"tp": across}))
    for ring in small_b:
        ring.finish()
    for ring in large_b:
        ring.start()
    for copy, ring in zip(swaps, small):
        copy.wait_recv()
        ring.start()
    forward_b, forward = [], []
    for p, ring in enumerate(large_b):
        ring.second()
        forward_b += [send_to(b_large(p, lax.rem(ring.index + k, 4)), partner) for k in (0, 3, 1)]
    for ring in small:
        ring.second()
    for near_ring, wide_ring in zip(small, large):
        near_ring.finish()
        wide_ring.start()
    for p, ring in enumerate(large_b):
        ring.finish()
        forward_b.append(send_to(b_large(p, lax.rem(ring.index + 2, 4)), partner))
    for copy in forward_b:
        copy.wait_recv()

    def coefficients(squares, diagonal):
        second = jnp.full((1, 1), squares)
        first = jnp.full((1, 1), diagonal)
        ratio = SAFETY * (second + 1.0) / (first + 1.0)
        return 1.0 / ratio, lax.rsqrt(ratio)

    def squares_b(i, sums):
        value = gram_b[i].astype(jnp.float32)
        diagonal = gram_b[i, :, at(i, 128)].astype(jnp.float32)
        return (
            sums[0] + jnp.sum((value * value).reshape(16, 8, NB), axis=0),
            sums[1] + jnp.where(same, diagonal, 0.0),
        )

    sums = lax.fori_loop(0, 8, squares_b, (jnp.zeros((8, NB), jnp.float32), jnp.zeros((128, 128), jnp.float32)))
    alpha_b, scale_b = coefficients(jnp.sum(sums[0]), jnp.sum(sums[1]))

    top, low_half = pl.ds(0, 512), pl.ds(512, 512)

    def mirrored_b(left, right, out, emit):
        out[top, top] = emit(left[top, top], dot(left[top, :], right[:, top])).astype(BF)
        out[low_half, :] = emit(left[low_half, :], dot(left[low_half, :], right[...])).astype(BF)
        out[top, low_half] = out[low_half, top].T

    def square_b(left, low, high):
        mirrored_b(left, left, m_b, lambda own, value: low * own.astype(jnp.float32) + high * value)

    def times_b(left, out, factor):
        mirrored_b(left, m_b, out, lambda own, value: factor * (COEF_ONE * own.astype(jnp.float32) + value))

    def rows_of(left, factor):
        return (factor * (COEF_ONE * left.astype(jnp.float32) + dot(left, m_b[...]))).astype(BF)

    for i in range(8):
        g_b[at(i, 128), :] = gram_b[i]
    square_b(g_b, COEF_THREE * alpha_b, COEF_FIVE * alpha_b * alpha_b)
    times_b(g_b, t_b, alpha_b)
    line_b = rows_of(xb[at(core, rows_b), :], scale_b)
    times_b(t_b, g_b, 1.0)
    square_b(g_b, COEF_THREE, COEF_FIVE)
    for p, ring in enumerate(large):
        ring.second()
        forward += [send_to(g_large(p, lax.rem(ring.index + k, 4)), partner) for k in (0, 3, 1)]
    times_b(g_b, t_b, 1.0)
    line_b = rows_of(line_b, 1.0)
    times_b(t_b, g_b, 1.0)
    for p, ring in enumerate(large):
        ring.finish()
        forward.append(send_to(g_large(p, lax.rem(ring.index + 2, 4)), partner))
    square_b(g_b, COEF_THREE, COEF_FIVE)
    t_b[0:rows_b, :] = line_b
    for p in range(2):
        cols = spot(p * 512 + place * 128, 128, 128)
        last_b = COEF_ONE * t_b[0:rows_b, cols].astype(jnp.float32) + dot(line_b, m_b[:, cols])
        results_b[:, at(p, 128)] = last_b.astype(BF)
    store(results_b, branch_out)
    for copy in forward:
        copy.wait_recv()

    def assemble(r, sums):
        value = panels[lax.div(r, 4), lax.rem(r, 4)]
        squares, diagonal = sums
        for d in range(5):
            block = value[:, d * 256 : d * 256 + 256]
            column = at(lax.rem(r + d, 8), 256)
            a[at(r, 256), column] = block
            if 0 < d < 4:
                a[column, at(r, 256)] = block.T
            wide = block.astype(jnp.float32)
            weight = 2.0 if 0 < d < 4 else 1.0
            squares = squares + weight * jnp.sum((wide * wide).reshape(32, 8, 256), axis=0)
        for k in range(2):
            corner = value[k * 128 : k * 128 + 128, k * 128 : k * 128 + 128].astype(jnp.float32)
            diagonal = diagonal + jnp.where(same, corner, 0.0)
        return squares, diagonal

    sums = lax.fori_loop(0, 8, assemble, (jnp.zeros((8, 256), jnp.float32), jnp.zeros((128, 128), jnp.float32)))
    alpha, scale = coefficients(jnp.sum(sums[0]), jnp.sum(sums[1]))


    def h(q):
        return at(2 * core + q, BLOCK)

    def o(q):
        return at(2 * other + q, BLOCK)

    def flip(q):
        return lax.rem(q + core, 2)

    def flop(q):
        return lax.rem(q + other, 2)

    def pair(ref, target, k, q):
        return pltpu.make_async_remote_copy(
            src_ref=ref, dst_ref=target, send_sem=send.at[k, q], recv_sem=recv.at[k, q], device_id=partner, device_id_type=MESH
        )

    def cross_out(buf, k, q):
        ref = buf.at[o(q), h(flip(q))]
        return pair(ref, ref, k, q)

    def cross_in(buf, k, q):
        ref = buf.at[h(q), o(flop(q))]
        return pair(ref, ref, k, q)

    def square_out(buf, k, q, side):
        first = at(2 * side, BLOCK)
        second = at(2 * side + 1, BLOCK)
        ref = (buf.at[first, at(side, HALF)], buf.at[second, first], buf.at[second, second])[q]
        return pair(ref, ref, k, 2 + q)

    def stage_out(k, q):
        return pair(m.at[o(q), at(flip(q), BLOCK)], stage.at[q], 4 + k, q)

    def receive_cross(left, k):
        def step(q, _):
            cross_out(left, k, q).wait_send()
            cross_in(left, k, q).wait_recv()
            left[o(flop(q)), h(q)] = left[h(q), o(flop(q))].T
            return 0

        lax.fori_loop(0, 2, step, 0)

    def receive_square(left, k):
        for q in range(3):
            square_out(left, k, q, core).wait_send()
            square_out(left, k, q, other).wait_recv()

    def product(left, receive, right, emit, order, after_head, after_cross, after_last):
        def head():
            emit(at(core, HALF), 0, dot(left[at(core, HALF), :], right(0)))
            after_head()

        def cross():
            receive(receive_square)
            for q in range(2):
                j = flip(q)
                emit(o(q), j, dot(left[o(q), :], right(j)))
                after_cross(q)

        def corner():
            emit(h(1), 1, dot(left[h(1), :], right(1)))
            after_last()

        receive(receive_cross)
        for name in order:
            {"head": head, "cross": cross, "last": corner}[name]()

    def square(left, receive, k_out, low, high):
        def emit(where, j, value):
            value = low * left[where, h(j)].astype(jnp.float32) + high * value
            m[where, at(j, BLOCK)] = value.astype(BF)

        def after_head():
            m[h(0), at(1, BLOCK)] = m[h(1), at(0, BLOCK)].T

        def after_cross(q):
            stage_out(k_out, q).start()

        def right(j):
            return left[:, h(j)]

        product(left, receive, right, emit, ("last", "cross", "head"), after_head, after_cross, lambda: None)
        for q in range(2):
            copy = stage_out(k_out, q)
            copy.wait_send()
            copy.wait_recv()
            m[o(flop(q)), at(q, BLOCK)] = stage[q].T

    def times(left, receive, out, k_out, factor, order):
        def emit(where, j, value):
            value = factor * (COEF_ONE * left[where, h(j)].astype(jnp.float32) + value)
            out[where, h(j)] = value.astype(BF)

        def after_head():
            out[h(0), h(1)] = out[h(1), h(0)].T
            square_out(out, k_out, 0, core).start()
            square_out(out, k_out, 1, core).start()

        def after_cross(q):
            cross_out(out, k_out, q).start()
            out[h(flip(q)), o(q)] = out[o(q), h(flip(q))].T

        def after_all():
            square_out(out, k_out, 2, core).start()

        def right(j):
            return m[:, at(j, BLOCK)]

        product(left, receive, right, emit, order, after_head, after_cross, after_all)

    def x_swap(i, half):
        ref = xall.at[i + 1, :, at(half, HALF)]
        return pltpu.make_async_remote_copy(
            src_ref=ref, dst_ref=ref, send_sem=xsend.at[i], recv_sem=xrecv.at[i], device_id=partner, device_id_type=MESH
        )

    def iteration(i, _):
        left, following = pairs.at[i], pairs.at[1 - i]
        opening = i == 0
        weight = jnp.where(opening, alpha, 1.0)

        def receive_later(step):
            @pl.when(i == 1)
            def _():
                step(left, 1)

        square(left, receive_later, i, COEF_THREE * weight, COEF_FIVE * weight * weight)
        times(left, lambda step: None, b, 2 * i, weight, ("cross", "head", "last"))

        times(b, lambda step: step(b, 2 * i), following, 2 * i + 1, 1.0, ("head", "cross", "last"))

        @pl.when(i == 1)
        def _():
            x_swap(0, core).wait_send()
            x_swap(0, other).wait_recv()

        own = xall[i, :, mine].astype(jnp.float32)
        xall[i + 1, :, mine] = (jnp.where(opening, scale, 1.0) * (COEF_ONE * own + dot(xall[i], m[...]))).astype(BF)
        x_swap(i, core).start()
        return 0

    lax.fori_loop(0, 2, iteration, 0)

    def some(block, low, high):
        close = spot(core * HALF + block * 256, 256, 256)

        def step(r, _):
            where = at(lax.rem(2 * core + r, 4), BLOCK)
            value = COEF_THREE * a[where, close].astype(jnp.float32) + COEF_FIVE * dot(a[where, :], a[:, close])
            m[where, at(block, 256)] = value.astype(BF)
            return 0

        lax.fori_loop(low, high, step, 0)

    def last(where, block):
        cols = at(block, 256)
        close = spot(core * HALF + block * 256, 256, 256)
        return (COEF_ONE * x2[where, close].astype(jnp.float32) + dot(x2[where, :], m[:, cols])).astype(BF)

    receive_cross(a, 3)
    some(ahead, 0, 2)
    receive_square(a, 3)
    some(ahead, 2, 4)
    x_swap(1, core).wait_send()
    x_swap(1, other).wait_recv()
    x2 = xall.at[2]
    final[2] = last(pl.ds(0, rows), ahead)
    to_ahead = pltpu.make_async_remote_copy(
        src_ref=final.at[2], dst_ref=final.at[4 + core], send_sem=sems.at[COPIES], recv_sem=recvs.at[COPIES + core],
        device_id={"tp": ahead, "rep": 0}, device_id_type=MESH,
    )
    to_ahead.start()
    some(behind, 0, 4)
    final[3] = last(pl.ds(rows, rows), behind)
    to_behind = pltpu.make_async_remote_copy(
        src_ref=final.at[3], dst_ref=final.at[4 + core], send_sem=sems.at[COPIES + 1], recv_sem=recvs.at[COPIES + core],
        device_id={"tp": behind, "rep": 1}, device_id_type=MESH,
    )
    to_behind.start()
    some(place, 0, 4)
    final[6] = last(other_rows, place)
    to_partner = remote(final.at[6], final.at[core], partner)
    to_partner.start()
    final[core] = last(own_rows, place)
    to_partner.wait_recv()
    for i in range(2):
        pltpu.make_async_remote_copy(
            src_ref=final.at[2], dst_ref=final.at[4 + i], send_sem=sems.at[COPIES], recv_sem=recvs.at[COPIES + i],
            device_id=partner, device_id_type=MESH,
        ).wait_recv()
    for i in range(2):
        cols = pl.ds(i * 256, 256)
        results[kind, :, cols] = final[i]
        results[1 - kind, :, cols] = final[4 + i]
    store(results.at[0], gate_out)
    store(results.at[1], up_out)
    to_ahead.wait_send()
    to_behind.wait_send()
    for copy in used:
        copy.wait_send()
    for copy in stores:
        copy.wait()


def finish_kernel(*refs):
    ins, outs, stage, fresh, in_sem, out_sem = refs[:9], refs[9:15], refs[15:24], refs[24:27], refs[27], refs[28]
    loads = [pltpu.make_async_copy(ins[i], stage[i], in_sem.at[i]) for i in range(9)]
    for i in (3, 6, 4, 7, 5, 8, 0, 1, 2):
        loads[i].start()
    stores = []

    def store(source, target):
        copy = pltpu.make_async_copy(source, target, out_sem.at[len(stores)])
        copy.start()
        stores.append(copy)

    for i, height in enumerate((FF, FF, D)):
        loads[3 + i].wait()
        loads[6 + i].wait()
        fresh[i][...] = SHRINK * stage[6 + i][...] - RATE * math.sqrt(height) * stage[3 + i][...].astype(jnp.float32)
        store(fresh[i], outs[2 * i + 1])
    for i in range(3):
        loads[i].wait()
        store(stage[i], outs[2 * i])
    for copy in stores:
        copy.wait()


def local(*args):
    velocities = (args[1], args[4], args[7])
    shapes = [velocity.shape for velocity in velocities]
    (rows, width), (rows_b, width_b) = shapes[0], shapes[2]
    anywhere = pl.BlockSpec(memory_space=pl.ANY)
    dma = pltpu.SemaphoreType.DMA

    def buf(*shape):
        return pltpu.VMEM(shape, BF)

    def full(*shape):
        return pltpu.VMEM(shape, jnp.float32)

    outs = [jax.ShapeDtypeStruct(shape, kind) for kind in (jnp.float32, BF) for shape in shapes]
    middle = pl.pallas_call(
        kernel,
        out_shape=outs,
        in_specs=[anywhere] * 6,
        out_specs=[anywhere] * 6,
        scratch_shapes=[
            full(2, 2, rows, width), full(2, rows_b, width_b), full(2, rows, width), full(rows_b, width_b),
            buf(2, rows, width), buf(rows_b, width_b), dma((9,)), dma((6,)),
            buf(2, N, N), buf(N, N), buf(N, HALF), buf(3, 2 * rows, N), buf(2 * rows_b, NB), buf(7, rows, 256),
            buf(2, 2, rows, 256), buf(2, rows, 256),
            buf(2, rows, width), buf(2, rows, width), buf(rows_b, width_b), buf(rows_b, width_b),
            buf(2, 256, 1280), buf(2, 2, 3, 64, 640), buf(2, 2, 64, 640), buf(2, 2, 3, 16, 640),
            buf(2, 4, 256, 1280),
            buf(128, NB), buf(2, 3, 16, NB), buf(2, 16, NB), buf(2, 3, 16, 256), buf(8, 128, NB),
            buf(NB, NB), buf(NB, NB), buf(NB, NB),
            buf(2, BLOCK, BLOCK),
            dma((COPIES + 2,)), dma((COPIES + 2,)), dma((7, 5)), dma((7, 5)), dma((2,)), dma((2,)),
        ],
        compiler_params=pltpu.CompilerParams(collective_id=0, has_side_effects=True, vmem_limit_bytes=62 * 1024 * 1024),
    )(args[0], args[3], args[6], args[1], args[4], args[7])
    results = [jax.ShapeDtypeStruct(shape, jnp.float32) for shape in shapes for _ in range(2)]
    stage = [full(*shape) for shape in shapes] + [buf(*shape) for shape in shapes] + [full(*shape) for shape in shapes] * 2
    return pl.pallas_call(
        finish_kernel,
        out_shape=results,
        in_specs=[anywhere] * 9,
        out_specs=[anywhere] * 6,
        scratch_shapes=stage + [dma((9,)), dma((6,))],
    )(*middle, args[2], args[5], args[8])


def solution(mesh):
    torus = Mesh(
        mesh.devices.reshape(4, 4, mesh.shape["tp"], mesh.shape["rep"]),
        ("fs_0", "fs_1", "tp", "rep"),
    )
    grads, plain = P("rep", FS, "tp"), P(FS_REP, "tp")
    return jax.shard_map(
        local,
        mesh=torus,
        in_specs=(grads, plain, plain) * 3,
        out_specs=(plain,) * 6,
        check_vma=False,
    )
```

```python
import functools
import math

import jax
import jax.numpy as jnp
from jax import lax
from jax.experimental import pallas as pl
from jax.experimental.pallas import tpu as pltpu
from jax.sharding import Mesh
from jax.sharding import PartitionSpec as P

D = 2048
FF = 5632
FS_REP = ("fs_0", "fs_1", "rep")
FS = ("fs_0", "fs_1")

MOMENT = 0.95
COEF_ONE = 3.4445
COEF_THREE = -4.775
COEF_FIVE = 2.0315
SAFETY = 2.0
RATE = 0.5
SHRINK = 0.95
BF = jnp.bfloat16


def dot(a, b):
    return jnp.dot(a, b, preferred_element_type=jnp.float32)


N = 2048
HALF = 1024
BLOCK = 512
NB = 1024
COPIES = 160
MESH = pl.DeviceIdType.MESH


def at(index, size):
    return pl.ds(index * size if isinstance(index, int) else pl.multiple_of(index * size, size), size)


def spot(offset, size, unit):
    return pl.ds(pl.multiple_of(offset, unit), size)


def turned(a, b):
    return lax.dot_general(a, b, (((0,), (0,)), ((), ())), preferred_element_type=jnp.float32)


def kernel(
    gate_g, up_g, branch_g, gate_v, up_v, branch_v,
    gate_m, up_m, branch_m, gate_out, up_out, branch_out,
    grads, grads_b, speed, speed_b, results, results_b, in_sem, out_sem,
    pairs, b, m, xall, xb, final, starts, relay,
    give, take, give_b, take_b,
    part, near, kept, near2, panels,
    part_b, near_b, kept_b, near2_b, gram_b, m_b, t_b, g_b,
    stage, sems, recvs, send, recv, xsend, xrecv,
):
    core = lax.axis_index("rep")
    place = lax.axis_index("tp")
    iy = lax.axis_index("fs_1")
    iz = lax.axis_index("fs_0")
    other = 1 - core
    kind = lax.rem(place, 2)
    ahead = lax.rem(place + 1, 4)
    behind = lax.rem(place + 3, 4)
    across = lax.rem(place + 2, 4)
    rows = gate_v.shape[0]
    rows_b = branch_v.shape[0]
    loads = []

    def load(source, target):
        copy = pltpu.make_async_copy(source, target, in_sem.at[len(loads)])
        copy.start()
        loads.append(copy)

    load(branch_g.at[0, at(other, rows_b)], grads_b.at[1])
    load(gate_g.at[0, at(other, rows)], grads.at[0, 1])
    load(up_g.at[0, at(other, rows)], grads.at[1, 1])
    load(branch_g.at[0, at(core, rows_b)], grads_b.at[0])
    load(branch_v, speed_b)
    load(gate_g.at[0, at(core, rows)], grads.at[0, 0])
    load(gate_v, speed.at[0])
    load(up_g.at[0, at(core, rows)], grads.at[1, 0])
    load(up_v, speed.at[1])
    mine = at(core, HALF)
    partner = {"rep": other}
    used = []
    x0 = xall.at[0]
    a = pairs.at[0]

    def turn(axis, index, step):
        return {axis: lax.rem(index + step, 4)}

    def remote(src, dst, to):
        k = len(used)
        copy = pltpu.make_async_remote_copy(
            src_ref=src, dst_ref=dst, send_sem=sems.at[k], recv_sem=recvs.at[k], device_id=to, device_id_type=MESH
        )
        used.append(copy)
        return copy

    def send_to(ref, to):
        copy = remote(ref, ref, to)
        copy.start()
        return copy

    barrier = pltpu.get_barrier_semaphore()
    peers = [partner, {"tp": across}]
    peers += [{"tp": x, "rep": r} for x in (ahead, behind) for r in range(2)]
    peers += [turn(axis, index, step) for axis, index in (("fs_1", iy), ("fs_0", iz)) for step in (1, 2, 3)]
    for to in peers:
        pl.semaphore_signal(barrier, inc=1, device_id=to, device_id_type=MESH)

    own_rows, other_rows = at(core, rows), at(other, rows)
    loads[0].wait()
    give_b[...] = grads_b[1].astype(BF)
    for i in range(2):
        loads[1 + i].wait()
        give[i] = grads[i, 1].astype(BF)
    pl.semaphore_wait(barrier, len(peers))
    first_copies = [remote(give_b, take_b, partner)]
    first_copies += [remote(give.at[i], take.at[i], partner) for i in range(2)]
    for copy in first_copies:
        copy.start()
    same = lax.broadcasted_iota(jnp.int32, (128, 128), 0) == lax.broadcasted_iota(jnp.int32, (128, 128), 1)

    def columns(ref, lines, height, width):
        def block(x, part):
            return ref.at[at(core, height), spot(part * 4 * width + x * width, width, width)]

        state = {}

        def start():
            state["right"] = [send_to(block(place, p), {"tp": ahead}) for p in range(2)]
            state["left"] = [send_to(block(place, p), {"tp": behind}) for p in range(2)]
            state["own"] = [send_to(block(place, p), partner) for p in range(2)]

        def second():
            state["right"][0].wait_recv()
            far = [send_to(block(behind, 0), {"tp": ahead})]
            state["left"][1].wait_recv()
            far.append(send_to(block(ahead, 1), {"tp": behind}))
            state["far"] = far
            state["own"].append(send_to(block(behind, 0), partner))
            state["own"].append(send_to(block(ahead, 1), partner))
            state["right"][1].wait_recv()
            state["own"].append(send_to(block(behind, 1), partner))
            state["left"][0].wait_recv()
            state["own"].append(send_to(block(ahead, 0), partner))

        def finish():
            for p in range(2):
                state["far"][p].wait_recv()
                state["own"].append(send_to(block(across, p), partner))
            for copy in state["own"]:
                copy.wait_recv()

        return start, second, finish

    lines = [columns(xb, None, rows_b, 128)]
    line = {}

    def block_of(x, p):
        return x0.at[own_rows, spot(p * HALF + x * 256, 256, 256)]

    def line_start():
        line["relay"] = [
            remote(starts.at[kind, p], relay.at[p], {"tp": to}) for p, to in ((0, ahead), (1, behind))
        ]
        line["out"] = [
            [remote(starts.at[1 - kind, p], block_of(place, p), {"tp": to}) for p in range(2)] for to in (ahead, behind)
        ]
        for copy in line["relay"] + line["out"][0] + line["out"][1]:
            copy.start()
        line["own"] = [send_to(block_of(place, p), partner) for p in range(2)]

    def line_second():
        line["far"] = []
        for p, (source, to) in enumerate(((behind, ahead), (ahead, behind))):
            line["relay"][p].wait_recv()
            copy = remote(relay.at[p], block_of(source, p), {"tp": to})
            copy.start()
            line["far"].append(copy)

    def line_third():
        for side, source in ((0, behind), (1, ahead)):
            for p in range(2):
                line["out"][side][p].wait_recv()
                line["own"].append(send_to(block_of(source, p), partner))

    def line_finish():
        for p in range(2):
            line["far"][p].wait_recv()
            line["own"].append(send_to(block_of(across, p), partner))
        for copy in line["own"]:
            copy.wait_recv()

    first_copies[0].wait_recv()
    loads[3].wait()
    loads[4].wait()
    moment = MOMENT * speed_b[...] + (grads_b[0] + take_b[...].astype(jnp.float32))
    speed_b[...] = moment
    for p in range(2):
        xb[at(core, rows_b), spot(p * 512 + place * 128, 128, 128)] = moment[:, p * 128 : p * 128 + 128].astype(BF)
    lines[0][0]()
    for i in range(2):
        first_copies[1 + i].wait_recv()
        loads[5 + 2 * i].wait()
        loads[6 + 2 * i].wait()
        moment = MOMENT * speed[i] + (grads[i, 0] + take[i].astype(jnp.float32))
        speed[i] = moment
        for p in range(2):
            starts[i, p] = moment[:, p * 256 : p * 256 + 256].astype(BF)
    for p in range(2):
        x0[own_rows, spot(p * HALF + place * 256, 256, 256)] = starts[kind, p]
    line_start()
    stores = []

    def store(source, target):
        copy = pltpu.make_async_copy(source, target, out_sem.at[len(stores)])
        copy.start()
        stores.append(copy)

    axes = ((("fs_1", iy), ("fs_0", iz)), (("fs_0", iz), ("fs_1", iy)))

    def exchange(source, landing, axis, index):
        copies = []
        for step in (2, 1, 3):
            to = lax.rem(index + step, 4)
            copies.append(remote(source(to), landing.at[step - 1], {axis: to}))
            copies[-1].start()
        return copies

    def total(own, landing, copies):
        for copy in copies:
            copy.wait_recv()
        value = own.astype(jnp.float32)
        for k in range(3):
            value = value + landing[k].astype(jnp.float32)
        return value.astype(BF)

    def scatter_one(source, landings):
        return [
            exchange(functools.partial(source, p), landings[p], *axes[p][0]) for p in range(2)
        ]

    def source_of(i):
        return lambda p, t: part.at[i, at(t, 64), at(p, 640)]

    def source_b(p, t):
        return part_b.at[spot(p * 64 + t * 16, 16, 16), :]

    upper = lax.div(place, 2)

    def panel(i):
        first = core * 4 + 2 * upper + i
        own = x0[:, at(first, 256)]
        for d in range(5):
            part[i, :, at(d, 256)] = turned(own, x0[:, at(lax.rem(first + d, 8), 256)]).astype(BF)
        return scatter_one(source_of(i), [near.at[i, p] for p in range(2)])

    def gram_rows(p, i1):
        return spot(p * 64 + i1 * 16, 16, 16)

    group = at(core, 4)

    class Ring:
        def __init__(self, axis, index, block, cut):
            self.next, self.prev = turn(axis, index, 1), turn(axis, index, 3)
            self.index, self.block, self.cut = index, block, cut

        def start(self):
            self.right = [send_to(self.cut(self.index, half), self.next) for half in (0, 1)]
            self.left = [send_to(self.cut(self.index, half), self.prev) for half in (1, 0)]

        def second(self):
            self.right[0].wait_recv()
            self.far = [send_to(self.cut(lax.rem(self.index + 3, 4), 0), self.next)]
            self.left[0].wait_recv()
            self.far.append(send_to(self.cut(lax.rem(self.index + 1, 4), 1), self.prev))

        def third(self):
            self.right[1].wait_recv()
            self.left[1].wait_recv()

        def finish(self):
            for copy in self.far:
                copy.wait_recv()

    def rings(phase, block, cut):
        return [
            Ring(*axes[p][phase], functools.partial(block, p), functools.partial(cut, p)) for p in range(2)
        ]

    def b_small(p, j):
        return gram_b.at[group, gram_rows(p, axes[p][0][1]), at(j, 256)]

    def b_small_cut(p, j, h):
        return gram_b.at[at(core * 2 + h, 2), gram_rows(p, axes[p][0][1]), at(j, 256)]

    def b_large(p, j):
        return gram_b.at[group, gram_rows(p, j), :]

    def b_large_cut(p, j, h):
        return gram_b.at[at(core * 2 + h, 2), gram_rows(p, j), :]

    def g_rows(p, j):
        return spot(axes[p][0][1] * 64 + j * 16, 16, 16)

    def g_small(p, j):
        return panels.at[core, :, g_rows(p, j), at(p, 640)]

    def g_small_cut(p, j, h):
        return panels.at[core, at(h, 2), g_rows(p, j), at(p, 640)]

    def g_large(p, j):
        return panels.at[core, :, at(j, 64), at(p, 640)]

    def g_large_cut(p, j, h):
        return panels.at[core, at(h, 2), at(j, 64), at(p, 640)]

    small_b, large_b = rings(1, b_small, b_small_cut), rings(0, b_large, b_large_cut)
    small, large = rings(1, g_small, g_small_cut), rings(0, g_large, g_large_cut)
    lines[0][1]()
    line_second()
    lines[0][2]()
    part_b[...] = turned(xb[:, spot(core * 512 + place * 128, 128, 128)], xb[...]).astype(BF)
    one_b = scatter_one(source_b, [near_b.at[p] for p in range(2)])
    line_third()
    for source, target in ((speed_b, branch_m), (speed.at[0], gate_m), (speed.at[1], up_m)):
        store(source, target)
    two_b = []
    for p in range(2):
        kept_b[p] = total(part_b[spot(p * 64 + axes[p][0][1] * 16, 16, 16), :], near_b.at[p], one_b[p])
        two_b.append(exchange(lambda t, p=p: kept_b.at[p, :, at(t, 256)], near2_b.at[p], *axes[p][1]))
    line_finish()
    ones = [panel(0), panel(1)]
    swaps_b = []
    for p in range(2):
        i1, i2 = axes[p][0][1], axes[p][1][1]
        gram_b[core * 4 + place, gram_rows(p, i1), at(i2, 256)] = total(
            kept_b[p, :, at(i2, 256)], near2_b.at[p], two_b[p]
        )
        ref = gram_b.at[core * 4 + place, gram_rows(p, i1), at(i2, 256)]
        swaps_b.append([send_to(ref, {"tp": x}) for x in (across, ahead, behind)])

    def scatter_two(i):
        pair = []
        for p in range(2):
            index = axes[p][0][1]
            kept[i, p] = total(part[i, at(index, 64), at(p, 640)], near.at[i, p], ones[i][p])
            pair.append(exchange(lambda t, p=p: kept.at[i, p, at(t, 16), :], near2.at[i, p], *axes[p][1]))
        return pair

    for p in range(2):
        for copy in swaps_b[p]:
            copy.wait_recv()
        small_b[p].start()
    twos = [scatter_two(0), scatter_two(1)]
    for ring in small_b:
        ring.second()
        ring.third()
    swaps = []
    for p in range(2):
        i2 = axes[p][1][1]
        for i in range(2):
            panels[core, 2 * upper + i, g_rows(p, i2), at(p, 640)] = total(
                kept[i, p, at(i2, 16), :], near2.at[i, p], twos[i][p]
            )
        swaps.append(send_to(panels.at[core, at(upper, 2), g_rows(p, i2), at(p, 640)], {"tp": across}))
    for ring in small_b:
        ring.finish()
    for ring in large_b:
        ring.start()
    for copy, ring in zip(swaps, small):
        copy.wait_recv()
        ring.start()
    forward_b, forward = [], []
    for ring in large_b:
        ring.second()
    for p, ring in enumerate(large_b):
        ring.third()
        forward_b += [send_to(b_large(p, lax.rem(ring.index + k, 4)), partner) for k in (0, 3, 1)]
    for ring in small:
        ring.second()
        ring.third()
    for near_ring, wide_ring in zip(small, large):
        near_ring.finish()
        wide_ring.start()
    for p, ring in enumerate(large_b):
        ring.finish()
        forward_b.append(send_to(b_large(p, lax.rem(ring.index + 2, 4)), partner))
    for copy in forward_b:
        copy.wait_recv()

    def coefficients(squares, diagonal):
        second = jnp.full((1, 1), squares)
        first = jnp.full((1, 1), diagonal)
        ratio = SAFETY * (second + 1.0) / (first + 1.0)
        return 1.0 / ratio, lax.rsqrt(ratio)

    def squares_b(i, sums):
        value = gram_b[i].astype(jnp.float32)
        diagonal = gram_b[i, :, at(i, 128)].astype(jnp.float32)
        return (
            sums[0] + jnp.sum((value * value).reshape(16, 8, NB), axis=0),
            sums[1] + jnp.where(same, diagonal, 0.0),
        )

    sums = lax.fori_loop(0, 8, squares_b, (jnp.zeros((8, NB), jnp.float32), jnp.zeros((128, 128), jnp.float32)))
    alpha_b, scale_b = coefficients(jnp.sum(sums[0]), jnp.sum(sums[1]))

    top, low_half = pl.ds(0, 512), pl.ds(512, 512)

    def mirrored_b(left, right, out, emit):
        out[top, top] = emit(left[top, top], dot(left[top, :], right[:, top])).astype(BF)
        out[low_half, :] = emit(left[low_half, :], dot(left[low_half, :], right[...])).astype(BF)
        out[top, low_half] = out[low_half, top].T

    def square_b(left, low, high):
        mirrored_b(left, left, m_b, lambda own, value: low * own.astype(jnp.float32) + high * value)

    def times_b(left, out, factor):
        mirrored_b(left, m_b, out, lambda own, value: factor * (COEF_ONE * own.astype(jnp.float32) + value))

    def rows_of(left, factor):
        return (factor * (COEF_ONE * left.astype(jnp.float32) + dot(left, m_b[...]))).astype(BF)

    for i in range(8):
        g_b[at(i, 128), :] = gram_b[i]
    square_b(g_b, COEF_THREE * alpha_b, COEF_FIVE * alpha_b * alpha_b)
    times_b(g_b, t_b, alpha_b)
    for p, ring in enumerate(large):
        ring.second()
        forward.append(send_to(g_large(p, ring.index), partner))
    line_b = rows_of(xb[at(core, rows_b), :], scale_b)
    times_b(t_b, g_b, 1.0)
    square_b(g_b, COEF_THREE, COEF_FIVE)
    for p, ring in enumerate(large):
        ring.third()
        forward += [send_to(g_large(p, lax.rem(ring.index + k, 4)), partner) for k in (3, 1)]
    times_b(g_b, t_b, 1.0)
    line_b = rows_of(line_b, 1.0)
    times_b(t_b, g_b, 1.0)
    for p, ring in enumerate(large):
        ring.finish()
        forward.append(send_to(g_large(p, lax.rem(ring.index + 2, 4)), partner))
    square_b(g_b, COEF_THREE, COEF_FIVE)
    t_b[0:rows_b, :] = line_b
    for p in range(2):
        cols = spot(p * 512 + place * 128, 128, 128)
        last_b = COEF_ONE * t_b[0:rows_b, cols].astype(jnp.float32) + dot(line_b, m_b[:, cols])
        results_b[:, at(p, 128)] = last_b.astype(BF)
    store(results_b, branch_out)
    for copy in forward:
        copy.wait_recv()

    def assemble(r, sums):
        value = panels[lax.div(r, 4), lax.rem(r, 4)]
        squares, diagonal = sums
        for d in range(5):
            block = value[:, d * 256 : d * 256 + 256]
            column = at(lax.rem(r + d, 8), 256)
            a[at(r, 256), column] = block
            if 0 < d < 4:
                a[column, at(r, 256)] = block.T
            wide = block.astype(jnp.float32)
            weight = 2.0 if 0 < d < 4 else 1.0
            squares = squares + weight * jnp.sum((wide * wide).reshape(32, 8, 256), axis=0)
        for k in range(2):
            corner = value[k * 128 : k * 128 + 128, k * 128 : k * 128 + 128].astype(jnp.float32)
            diagonal = diagonal + jnp.where(same, corner, 0.0)
        return squares, diagonal

    sums = lax.fori_loop(0, 8, assemble, (jnp.zeros((8, 256), jnp.float32), jnp.zeros((128, 128), jnp.float32)))
    alpha, scale = coefficients(jnp.sum(sums[0]), jnp.sum(sums[1]))


    def h(q):
        return at(2 * core + q, BLOCK)

    def o(q):
        return at(2 * other + q, BLOCK)

    def flip(q):
        return lax.rem(q + core, 2)

    def flop(q):
        return lax.rem(q + other, 2)

    def pair(ref, target, k, q):
        return pltpu.make_async_remote_copy(
            src_ref=ref, dst_ref=target, send_sem=send.at[k, q], recv_sem=recv.at[k, q], device_id=partner, device_id_type=MESH
        )

    def cross_out(buf, k, q):
        ref = buf.at[o(q), h(flip(q))]
        return pair(ref, ref, k, q)

    def cross_in(buf, k, q):
        ref = buf.at[h(q), o(flop(q))]
        return pair(ref, ref, k, q)

    def square_out(buf, k, q, side):
        first = at(2 * side, BLOCK)
        second = at(2 * side + 1, BLOCK)
        ref = (buf.at[first, at(side, HALF)], buf.at[second, first], buf.at[second, second])[q]
        return pair(ref, ref, k, 2 + q)

    def stage_out(k, q):
        return pair(m.at[o(q), at(flip(q), BLOCK)], stage.at[q], 4 + k, q)

    def receive_cross(left, k):
        def step(q, _):
            cross_out(left, k, q).wait_send()
            cross_in(left, k, q).wait_recv()
            left[o(flop(q)), h(q)] = left[h(q), o(flop(q))].T
            return 0

        lax.fori_loop(0, 2, step, 0)

    def receive_square(left, k):
        for q in range(3):
            square_out(left, k, q, core).wait_send()
            square_out(left, k, q, other).wait_recv()

    def product(left, receive, right, emit, order, after_head, after_cross, after_last):
        def head():
            emit(at(core, HALF), 0, dot(left[at(core, HALF), :], right(0)))
            after_head()

        def cross():
            receive(receive_square)
            for q in range(2):
                j = flip(q)
                emit(o(q), j, dot(left[o(q), :], right(j)))
                after_cross(q)

        def corner():
            emit(h(1), 1, dot(left[h(1), :], right(1)))
            after_last()

        receive(receive_cross)
        for name in order:
            {"head": head, "cross": cross, "last": corner}[name]()

    def square(left, receive, k_out, low, high):
        def emit(where, j, value):
            value = low * left[where, h(j)].astype(jnp.float32) + high * value
            m[where, at(j, BLOCK)] = value.astype(BF)

        def after_head():
            m[h(0), at(1, BLOCK)] = m[h(1), at(0, BLOCK)].T

        def after_cross(q):
            stage_out(k_out, q).start()

        def right(j):
            return left[:, h(j)]

        product(left, receive, right, emit, ("last", "cross", "head"), after_head, after_cross, lambda: None)
        for q in range(2):
            copy = stage_out(k_out, q)
            copy.wait_send()
            copy.wait_recv()
            m[o(flop(q)), at(q, BLOCK)] = stage[q].T

    def times(left, receive, out, k_out, factor, order):
        def emit(where, j, value):
            value = factor * (COEF_ONE * left[where, h(j)].astype(jnp.float32) + value)
            out[where, h(j)] = value.astype(BF)

        def after_head():
            out[h(0), h(1)] = out[h(1), h(0)].T
            square_out(out, k_out, 0, core).start()
            square_out(out, k_out, 1, core).start()

        def after_cross(q):
            cross_out(out, k_out, q).start()
            out[h(flip(q)), o(q)] = out[o(q), h(flip(q))].T

        def after_all():
            square_out(out, k_out, 2, core).start()

        def right(j):
            return m[:, at(j, BLOCK)]

        product(left, receive, right, emit, order, after_head, after_cross, after_all)

    def x_swap(i, half):
        ref = xall.at[i + 1, :, at(half, HALF)]
        return pltpu.make_async_remote_copy(
            src_ref=ref, dst_ref=ref, send_sem=xsend.at[i], recv_sem=xrecv.at[i], device_id=partner, device_id_type=MESH
        )

    def iteration(i, _):
        left, following = pairs.at[i], pairs.at[1 - i]
        opening = i == 0
        weight = jnp.where(opening, alpha, 1.0)

        def receive_later(step):
            @pl.when(i == 1)
            def _():
                step(left, 1)

        square(left, receive_later, i, COEF_THREE * weight, COEF_FIVE * weight * weight)
        times(left, lambda step: None, b, 2 * i, weight, ("cross", "head", "last"))

        times(b, lambda step: step(b, 2 * i), following, 2 * i + 1, 1.0, ("head", "cross", "last"))

        @pl.when(i == 1)
        def _():
            x_swap(0, core).wait_send()
            x_swap(0, other).wait_recv()

        own = xall[i, :, mine].astype(jnp.float32)
        xall[i + 1, :, mine] = (jnp.where(opening, scale, 1.0) * (COEF_ONE * own + dot(xall[i], m[...]))).astype(BF)
        x_swap(i, core).start()
        return 0

    lax.fori_loop(0, 2, iteration, 0)

    def some(block, low, high):
        close = spot(core * HALF + block * 256, 256, 256)

        def step(r, _):
            where = at(lax.rem(2 * core + r, 4), BLOCK)
            value = COEF_THREE * a[where, close].astype(jnp.float32) + COEF_FIVE * dot(a[where, :], a[:, close])
            m[where, at(block, 256)] = value.astype(BF)
            return 0

        lax.fori_loop(low, high, step, 0)

    def last(where, block):
        cols = at(block, 256)
        close = spot(core * HALF + block * 256, 256, 256)
        return (COEF_ONE * x2[where, close].astype(jnp.float32) + dot(x2[where, :], m[:, cols])).astype(BF)

    receive_cross(a, 3)
    some(ahead, 0, 2)
    receive_square(a, 3)
    some(ahead, 2, 4)
    x_swap(1, core).wait_send()
    x_swap(1, other).wait_recv()
    x2 = xall.at[2]
    final[2] = last(pl.ds(0, rows), ahead)
    to_ahead = pltpu.make_async_remote_copy(
        src_ref=final.at[2], dst_ref=final.at[4 + core], send_sem=sems.at[COPIES], recv_sem=recvs.at[COPIES + core],
        device_id={"tp": ahead, "rep": 0}, device_id_type=MESH,
    )
    to_ahead.start()
    some(behind, 0, 4)
    final[3] = last(pl.ds(rows, rows), behind)
    to_behind = pltpu.make_async_remote_copy(
        src_ref=final.at[3], dst_ref=final.at[4 + core], send_sem=sems.at[COPIES + 1], recv_sem=recvs.at[COPIES + core],
        device_id={"tp": behind, "rep": 1}, device_id_type=MESH,
    )
    to_behind.start()
    some(place, 0, 4)
    final[6] = last(other_rows, place)
    to_partner = remote(final.at[6], final.at[core], partner)
    to_partner.start()
    final[core] = last(own_rows, place)
    to_partner.wait_recv()
    for i in range(2):
        pltpu.make_async_remote_copy(
            src_ref=final.at[2], dst_ref=final.at[4 + i], send_sem=sems.at[COPIES], recv_sem=recvs.at[COPIES + i],
            device_id=partner, device_id_type=MESH,
        ).wait_recv()
    for i in range(2):
        cols = pl.ds(i * 256, 256)
        results[kind, :, cols] = final[i]
        results[1 - kind, :, cols] = final[4 + i]
    store(results.at[0], gate_out)
    store(results.at[1], up_out)
    to_ahead.wait_send()
    to_behind.wait_send()
    for copy in used:
        copy.wait_send()
    for copy in stores:
        copy.wait()


def finish_kernel(*refs):
    ins, outs, stage, fresh, in_sem, out_sem = refs[:9], refs[9:15], refs[15:24], refs[24:27], refs[27], refs[28]
    loads = [pltpu.make_async_copy(ins[i], stage[i], in_sem.at[i]) for i in range(9)]
    for i in (3, 6, 4, 7, 5, 8, 0, 1, 2):
        loads[i].start()
    stores = []

    def store(source, target):
        copy = pltpu.make_async_copy(source, target, out_sem.at[len(stores)])
        copy.start()
        stores.append(copy)

    for i, height in enumerate((FF, FF, D)):
        loads[3 + i].wait()
        loads[6 + i].wait()
        fresh[i][...] = SHRINK * stage[6 + i][...] - RATE * math.sqrt(height) * stage[3 + i][...].astype(jnp.float32)
        store(fresh[i], outs[2 * i + 1])
    for i in range(3):
        loads[i].wait()
        store(stage[i], outs[2 * i])
    for copy in stores:
        copy.wait()


def local(*args):
    velocities = (args[1], args[4], args[7])
    shapes = [velocity.shape for velocity in velocities]
    (rows, width), (rows_b, width_b) = shapes[0], shapes[2]
    anywhere = pl.BlockSpec(memory_space=pl.ANY)
    dma = pltpu.SemaphoreType.DMA

    def buf(*shape):
        return pltpu.VMEM(shape, BF)

    def full(*shape):
        return pltpu.VMEM(shape, jnp.float32)

    outs = [jax.ShapeDtypeStruct(shape, kind) for kind in (jnp.float32, BF) for shape in shapes]
    middle = pl.pallas_call(
        kernel,
        out_shape=outs,
        in_specs=[anywhere] * 6,
        out_specs=[anywhere] * 6,
        scratch_shapes=[
            full(2, 2, rows, width), full(2, rows_b, width_b), full(2, rows, width), full(rows_b, width_b),
            buf(2, rows, width), buf(rows_b, width_b), dma((9,)), dma((6,)),
            buf(2, N, N), buf(N, N), buf(N, HALF), buf(3, 2 * rows, N), buf(2 * rows_b, NB), buf(7, rows, 256),
            buf(2, 2, rows, 256), buf(2, rows, 256),
            buf(2, rows, width), buf(2, rows, width), buf(rows_b, width_b), buf(rows_b, width_b),
            buf(2, 256, 1280), buf(2, 2, 3, 64, 640), buf(2, 2, 64, 640), buf(2, 2, 3, 16, 640),
            buf(2, 4, 256, 1280),
            buf(128, NB), buf(2, 3, 16, NB), buf(2, 16, NB), buf(2, 3, 16, 256), buf(8, 128, NB),
            buf(NB, NB), buf(NB, NB), buf(NB, NB),
            buf(2, BLOCK, BLOCK),
            dma((COPIES + 2,)), dma((COPIES + 2,)), dma((7, 5)), dma((7, 5)), dma((2,)), dma((2,)),
        ],
        compiler_params=pltpu.CompilerParams(collective_id=0, has_side_effects=True, vmem_limit_bytes=62 * 1024 * 1024),
    )(args[0], args[3], args[6], args[1], args[4], args[7])
    results = [jax.ShapeDtypeStruct(shape, jnp.float32) for shape in shapes for _ in range(2)]
    stage = [full(*shape) for shape in shapes] + [buf(*shape) for shape in shapes] + [full(*shape) for shape in shapes] * 2
    return pl.pallas_call(
        finish_kernel,
        out_shape=results,
        in_specs=[anywhere] * 9,
        out_specs=[anywhere] * 6,
        scratch_shapes=stage + [dma((9,)), dma((6,))],
    )(*middle, args[2], args[5], args[8])


def solution(mesh):
    torus = Mesh(
        mesh.devices.reshape(4, 4, mesh.shape["tp"], mesh.shape["rep"]),
        ("fs_0", "fs_1", "tp", "rep"),
    )
    grads, plain = P("rep", FS, "tp"), P(FS_REP, "tp")
    return jax.shard_map(
        local,
        mesh=torus,
        in_specs=(grads, plain, plain) * 3,
        out_specs=(plain,) * 6,
        check_vma=False,
    )
```
